256 devices in a mesh: grp: 2 (over y), fs: 32 (over z, core), tp: 4 (over x).
Axes of the slice: x: 4, y: 2, z: 16, core: 2. Of those that a mesh axis runs over, the one named last changes fastest.
The devices are a block of a 4x16x16 slice.
Arguments:
- tokens: bfloat16 [4096, 2048], P(('grp', 'fs')), parts along dimension 0, may hold values from -6 to 6
- routes: int32 [4096, 2], P(('grp', 'fs')), parts along dimension 0, may hold values from 0 to 3, as said below
- route_logits: float32 [4096, 2], P(('grp', 'fs')), parts along dimension 0, may hold values from -8 to 8
- gain: float32 [2048], P('fs'), may hold values from 0.1 to 1.9
- w_gate: float32 [4, 2048, 7168], P(None, 'fs', 'tp'), may hold values from -0.125 to 0.125
- w_up: float32 [4, 2048, 7168], P(None, 'fs', 'tp'), may hold values from -0.125 to 0.125
- w_down: float32 [4, 7168, 2048], P(None, 'fs', 'tp'), may hold values from -0.0625 to 0.0625
Outputs:
- gate_served: bfloat16 [8, 2048, 7168], P(('grp', 'tp'), None, 'fs'), parts along dimension 0
- up_served: bfloat16 [8, 2048, 7168], P(('grp', 'tp'), None, 'fs'), parts along dimension 0
- down_served: bfloat16 [8, 7168, 2048], P(('grp', 'tp'), 'fs'), parts along dimension 0
- mixed: bfloat16 [4096, 2048], P(('grp', 'fs'), 'tp'), parts along dimension 0
The draws below stay inside these ranges and needn't reach their ends.
There are 2 independent parts, one for each index of `grp`. The reference program is written for one: setup_inputs(seed, part) draws one part's arguments, and reference() takes and returns one part's arrays. A program takes and returns all parts, laid end to end along the dimension named above; an argument that names none is the same for every part. Nothing has to cross between parts.
Inputs may be any that keep to these rules, and one draw needn't show every extreme that they name: `routes`: each row names 2 different experts; every expert is named by some row.
All inputs are finite; a program needn't handle non-finite values.
Results may differ from the reference program's by a relative error of at most 0.0085.
Values may be sent and summed in bfloat16 or wider, within the bound.
A program may use at most 128 MiB of HBM per device.

```python
import jax
import jax.numpy as jnp
from jax import lax

D = 2048
FF = 7168
EXPERTS = 4
TOP = 2
TOKENS = 2048


def draw_routes(key, part):
    key_hot = jax.random.fold_in(key, 101)
    key_pick = jax.random.fold_in(key, 102)
    key_other = jax.random.fold_in(key, 103)
    key_second = jax.random.fold_in(key, 104)
    hot_expert = jax.random.randint(key_hot, (), 0, EXPERTS, dtype=jnp.int32)
    chooser = jax.random.randint(key_pick, (TOKENS,), 0, 8, dtype=jnp.int32)
    other_offset = jax.random.randint(key_other, (TOKENS,), 0, EXPERTS - 1, dtype=jnp.int32)
    other_expert = (hot_expert + 1 + other_offset) % EXPERTS
    first_col = jnp.where(chooser < 7, hot_expert, other_expert).astype(jnp.int32)
    second_offset = jax.random.randint(key_second, (TOKENS,), 0, EXPERTS - 1, dtype=jnp.int32)
    second_col = ((first_col + 1 + second_offset) % EXPERTS).astype(jnp.int32)
    row_index = jnp.arange(TOKENS, dtype=jnp.int32)
    first_col = jnp.where(row_index < EXPERTS, row_index, first_col)
    second_col = jnp.where(row_index < EXPERTS, (row_index + 1) % EXPERTS, second_col)
    return jnp.stack([first_col, second_col], axis=1).astype(jnp.int32)


def steps_of(stream_key, extent, pieces, low, largest):
    def one(axis_at, shards_of):
        draws = jax.random.uniform(jax.random.fold_in(jax.random.fold_in(stream_key, 6), axis_at), (shards_of,), jnp.float32, low / len(pieces), largest / len(pieces))
        return jnp.repeat(jnp.exp(draws), extent[axis_at] // shards_of).reshape((-1,) + (1,) * (len(extent) - axis_at - 1))

    level = one(*pieces[0])
    for cut in pieces[1:]:
        level = level * one(*cut)
    return level


def gaussian(stream_key, dims, width, reach, split=(), held_as=jnp.bfloat16):
    array = jax.random.normal(stream_key, dims, jnp.float32) * width
    if len(split) > 0:
        array = steps_of(stream_key, dims, split, -0.22, 0.18) * array
    return jnp.clip(array, min=-reach, max=reach).astype(held_as)


def setup_inputs(seed: int = 0, part: int = 0) -> dict:
    splits = jax.random.split(jax.random.key(seed), 8)
    own_keys = jax.random.split(jax.random.fold_in(splits[7], part), 8)
    tokens = gaussian(own_keys[0], (TOKENS, D), 1.0, 6.0, ((0, 32),))
    routes = draw_routes(jax.random.fold_in(jax.random.fold_in(splits[7], part), 71), part)
    route_logits = gaussian(own_keys[2], (TOKENS, TOP), 1.5, 8.0, ((0, 32),), jnp.float32)
    gain = jnp.clip(1.0 + 0.18 * jax.random.normal(splits[3], (D,), jnp.float32), 0.1, 1.9)
    w_gate = gaussian(splits[4], (EXPERTS, D, FF), D ** -0.5, 0.125, ((1, 32), (2, 4)), jnp.float32)
    w_up = gaussian(splits[5], (EXPERTS, D, FF), D ** -0.5, 0.125, ((1, 32), (2, 4)), jnp.float32)
    w_down = gaussian(splits[6], (EXPERTS, FF, D), FF ** -0.5, 0.0625, ((1, 32), (2, 4)), jnp.float32)
    return {"tokens": tokens, "routes": routes, "route_logits": route_logits, "gain": gain, "w_gate": w_gate, "w_up": w_up, "w_down": w_down}


def reference(tokens, routes, route_logits, gain, w_gate, w_up, w_down):
    values = tokens.astype(jnp.float32)
    mean_square = lax.optimization_barrier(jnp.mean(values * values, axis=-1, keepdims=True))
    normed = (values * lax.rsqrt(mean_square + 1e-06)).astype(jnp.bfloat16)
    first = jax.nn.sigmoid(route_logits[:, 0] - route_logits[:, 1])
    second = jax.nn.sigmoid(route_logits[:, 1] - route_logits[:, 0])
    gate_cast = (w_gate * gain[None, :, None]).astype(jnp.bfloat16)
    up_cast = (w_up * gain[None, :, None]).astype(jnp.bfloat16)
    down_cast = w_down.astype(jnp.bfloat16)
    total = jnp.zeros((tokens.shape[0], w_down.shape[2]), jnp.float32)
    for expert in range(EXPERTS):
        weight_col = first * (routes[:, 0] == expert).astype(jnp.float32)
        weight_col = weight_col + second * (routes[:, 1] == expert).astype(jnp.float32)
        weight_col = weight_col.astype(jnp.bfloat16)
        gate_act = jnp.dot(normed, gate_cast[expert], preferred_element_type=jnp.float32)
        up_act = jnp.dot(normed, up_cast[expert], preferred_element_type=jnp.float32)
        hidden = (jax.nn.silu(gate_act) * up_act * weight_col[:, None].astype(jnp.float32)).astype(jnp.bfloat16)
        total = total + jnp.dot(hidden, down_cast[expert], preferred_element_type=jnp.float32)
    return (gate_cast, up_cast, down_cast, total.astype(jnp.bfloat16))
```

```python
import functools

import jax
import jax.numpy as jnp
from jax import lax
from jax.experimental import pallas as pl
from jax.experimental.pallas import tpu as pltpu
from jax.sharding import PartitionSpec as P

MESH = pl.DeviceIdType.MESH
DMA = pltpu.SemaphoreType.DMA
LANES = 128


def remote(src, dst, send, recv, **where):
    return pltpu.make_async_remote_copy(
        src_ref=src, dst_ref=dst, send_sem=send, recv_sem=recv, device_id=where, device_id_type=MESH
    )


def hand_over(
    FS, TP, wp, dn, nt, wt, gu, ds, tok, wall, xr,
    xw_s, xw_r, xd_s, xd_r, loc, wt_s, wt_r, rs, rr, xt_s, xt_r, xo_s, xo_r,
    cc_s, cc_r, za_s, za_r, y_s, y_r, yd_s, yd_r,
):
    Z = FS // 2
    H = Z // 2
    x, f, g = lax.axis_index("tp"), lax.axis_index("fs"), lax.axis_index("grp")
    z, c = f // 2, f % 2
    p = g % 2
    mate = g + 1 - 2 * p
    slices = wp.shape[1]
    fb = nt.shape[1] // TP
    half = nt.shape[0] // 2
    db = dn.shape[2]

    def cols(i):
        return pl.ds(pl.multiple_of(i * fb, LANES), fb)

    def dcols(i):
        return pl.ds(pl.multiple_of(i * db, LANES), db)

    barrier = pltpu.get_barrier_semaphore()

    def greet(r, _):
        pl.semaphore_signal(barrier, inc=1, device_id={"fs": (f + r) % FS}, device_id_type=MESH)
        return 0

    lax.fori_loop(1, FS, greet, 0)
    for k in range(1, TP):
        pl.semaphore_signal(barrier, inc=1, device_id={"tp": (x + k) % TP}, device_id_type=MESH)
    pl.semaphore_signal(barrier, inc=1, device_id={"grp": mate}, device_id_type=MESH)
    pl.semaphore_wait(barrier, FS - 1 + TP - 1 + 1)

    def ring(i, fo, side):
        to = ((z + 1) % Z if side == 0 else (z + Z - 1) % Z) * 2 + c
        return remote(tok.at[fo, :, cols(x)], tok.at[fo, :, cols(x)], rs.at[side, i], rr.at[side, i], fs=to)

    def ring_first(side):
        to = ((z + 1) % Z if side == 0 else (z + Z - 1) % Z) * 2 + c
        return remote(nt.at[:, cols(x)], tok.at[f, :, cols(x)], rs.at[side, 0], rr.at[side, 0], fs=to)

    ring_first(0).start()
    ring_first(1).start()
    other = f + 1 - 2 * c
    own_cross = remote(nt, tok.at[f], cc_s.at[Z - 1], cc_r.at[Z - 1], fs=other)
    own_cross.start()

    def xw(k):
        return remote(wp.at[(x + k) % TP], xr.at[x], xw_s.at[k - 1], xw_r.at[k - 1], tp=(x + k) % TP)

    def xd(k):
        return remote(dn.at[(x + k) % TP], ds.at[p, :, dcols(x)], xd_s.at[k - 1], xd_r.at[k - 1], tp=(x + k) % TP)

    for k in (2, 1, 3):
        xw(k).start()
    for k in (2, 1, 3):
        xd(k).start()
    local = [
        pltpu.make_async_copy(wp.at[x], xr.at[x], loc.at[0]),
        pltpu.make_async_copy(dn.at[x], ds.at[p, :, dcols(x)], loc.at[1]),
        pltpu.make_async_copy(nt, tok.at[f], loc.at[2]),
        pltpu.make_async_copy(wt, wall.at[f], loc.at[3]),
    ]
    for copy in local:
        copy.start()

    def tell(r, _):
        remote(wt, wall.at[f], wt_s, wt_r, fs=(f + r) % FS).start()
        return 0

    lax.fori_loop(1, FS, tell, 0)

    def across(i, fo, side):
        to = (x + 1) % TP if side == 0 else (x + TP - 1) % TP
        return remote(tok.at[fo, :, cols(x)], tok.at[fo, :, cols(x)], xt_s.at[side, i], xt_r.at[side, i], tp=to)

    def from_left(s):
        return ((z + Z - s) % Z) * 2 + c

    def from_right(s):
        return ((z + s) % Z) * 2 + c

    def ring_step(s, _):
        fo = from_left(s)
        ring(s - 1, fo, 0).wait_recv()
        ring(s, fo, 0).start()
        fo2 = from_right(s)
        ring(s - 1, fo2, 1).wait_recv()

        @pl.when(s < H - 1)
        def _():
            ring(s, fo2, 1).start()

        for side in (0, 1):
            across(2 * s - 2, fo, side).start()
            across(2 * s - 1, fo2, side).start()
        return 0

    lax.fori_loop(1, H, ring_step, 0)
    last = from_left(H)
    ring(H - 1, last, 0).wait_recv()
    for side in (0, 1):
        across(2 * H - 2, last, side).start()

    for copy in local:
        copy.wait()
    for k in (2, 1, 3):
        xw(k).wait_recv()

    def apart(i):
        m = H - 1 - (i - 1) // 2
        return jnp.where(i == 0, H, jnp.where(i % 2 == 1, m, Z - m))

    def za(d, cd):
        to = ((z + d) % Z) * 2 + cd
        return remote(
            xr.at[to // slices, to % slices], gu.at[:, f, p], za_s.at[d, cd], za_r.at[d, c], fs=to
        )

    def za_recv(d, cs):
        fo = ((z + Z - d) % Z) * 2 + cs
        return remote(xr.at[0, 0], gu.at[:, fo, p], za_s.at[d, cs], za_r.at[d, cs], fs=other)

    def za_start(i, _):
        d = apart(i)
        za(d, 0).start()
        za(d, 1).start()
        return 0

    lax.fori_loop(0, Z - 1, za_start, 0)
    za(0, 1 - c).start()
    own = pltpu.make_async_copy(xr.at[f // slices, f % slices], gu.at[:, f, p], loc.at[4])
    own.start()

    for k in (2, 1, 3):
        xd(k).wait_recv()
    yd = remote(ds.at[p], ds.at[p], yd_s, yd_r, grp=mate)
    yd.start()

    def y_hand(d):
        zo = (z + Z - d) % Z
        part = gu.at[:, pl.ds(2 * zo, 2), p]
        return remote(part, part, y_s.at[d], y_r.at[d], grp=mate)

    def origin(i):
        s = i // 2 + 1
        return jnp.where(i % 2 == 0, from_left(s), from_right(s))

    def onward(i, fo, side):
        to = (x + 1) % TP if side == 0 else (x + TP - 1) % TP
        held = (x + TP - 1) % TP if side == 0 else (x + 1) % TP
        part = tok.at[fo, pl.ds(side * half, half), cols(held)]
        return remote(part, part, xo_s.at[side, i], xo_r.at[side, i], tp=to)

    def cross(i, fo):
        return remote(tok.at[fo], tok.at[fo], cc_s.at[i], cc_r.at[i], fs=other)

    def finish(i):
        fo = origin(i)
        for side in (0, 1):
            onward(i, fo, side).wait_recv()
        cross(i, fo).start()

    def flow(i, _):
        fo = origin(i)
        for side in (0, 1):
            across(i, fo, side).wait_recv()
            onward(i, fo, side).start()
        d = apart(i)
        za_recv(d, 0).wait_recv()
        za_recv(d, 1).wait_recv()
        y_hand(d).start()

        @pl.when(i > 0)
        def _():
            finish(i - 1)

        return 0

    lax.fori_loop(0, Z - 1, flow, 0)
    own.wait()
    za_recv(0, 1 - c).wait_recv()
    y_hand(0).start()
    finish(Z - 2)

    def drain(i, _):
        fo = origin(i)
        for side in (0, 1):
            across(i, fo, side).wait_send()
            onward(i, fo, side).wait_send()
        cross(i, fo).wait()
        d = apart(i)
        za(d, 0).wait_send()
        za(d, 1).wait_send()
        y_hand(d).wait()
        return 0

    lax.fori_loop(0, Z - 1, drain, 0)

    def ring_drain(s, _):
        ring(s, f, 0).wait_send()

        @pl.when(s < H - 1)
        def _():
            ring(s, f, 1).wait_send()

        return 0

    lax.fori_loop(0, H, ring_drain, 0)
    own_cross.wait()
    za(0, 1 - c).wait_send()
    y_hand(0).wait()
    yd.wait()
    for k in (1, 2, 3):
        xw(k).wait_send()
        xd(k).wait_send()
    tiles = remote(wall.at[pl.ds(0, FS - 1)], wall.at[pl.ds(0, FS - 1)], wt_s, wt_r, fs=other)
    tiles.wait_send()
    tiles.wait_recv()


def run_hand_over(FS, TP, wp, dn, nt, wt):
    Z = FS // 2
    _, slices, two, half, ff = wp.shape
    vmem = pl.BlockSpec(memory_space=pltpu.VMEM)
    hbm = pl.BlockSpec(memory_space=pl.ANY)
    return pl.pallas_call(
        functools.partial(hand_over, FS, TP),
        out_shape=(
            jax.ShapeDtypeStruct((two, FS, 2, half, ff), jnp.bfloat16),
            jax.ShapeDtypeStruct((2, dn.shape[1], TP * dn.shape[2]), jnp.bfloat16),
            jax.ShapeDtypeStruct((FS,) + nt.shape, jnp.bfloat16),
            jax.ShapeDtypeStruct((FS,) + wt.shape, jnp.bfloat16),
        ),
        in_specs=[vmem] * 4,
        out_specs=(hbm, hbm, hbm, vmem),
        scratch_shapes=[
            pltpu.VMEM(wp.shape, jnp.bfloat16),
            DMA((TP - 1,)), DMA((TP - 1,)), DMA((TP - 1,)), DMA((TP - 1,)),
            DMA((5,)), DMA, DMA,
            DMA((2, Z // 2)), DMA((2, Z // 2)),
            DMA((2, Z - 1)), DMA((2, Z - 1)), DMA((2, Z - 1)), DMA((2, Z - 1)),
            DMA((Z,)), DMA((Z,)),
            DMA((Z, 2)), DMA((Z, 2)),
            DMA((Z,)), DMA((Z,)), DMA, DMA,
        ],
        compiler_params=pltpu.CompilerParams(collective_id=0, has_side_effects=True, vmem_limit_bytes=32 << 20),
        cost_estimate=pl.CostEstimate(flops=10**9, bytes_accessed=30 << 20, transcendentals=0),
        name="hand_over",
    )(wp, dn, nt, wt)


def body(FS, TP, tokens, routes, route_logits, gain, w_gate, w_up, w_down):
    p = lax.axis_index("grp") % 2
    e = lax.axis_index("tp")
    rows, ff = w_gate.shape[1:]
    slices = FS // TP
    half = rows // 2

    def mine(w):
        part = lax.dynamic_slice_in_dim(w, p * half, half, 1)
        scale = lax.dynamic_slice_in_dim(gain, p * half, half, 0)
        part = (part * scale[None, :, None]).astype(jnp.bfloat16)
        return part.reshape(TP, half, slices, ff // slices).transpose(0, 2, 1, 3)

    wp = jnp.stack([mine(w_gate), mine(w_up)], axis=2)
    hrows = w_down.shape[1] // 2
    dn = lax.dynamic_slice_in_dim(w_down, p * hrows, hrows, 1).astype(jnp.bfloat16)

    values = tokens.astype(jnp.float32)
    mean_square = jnp.mean(values * values, axis=-1, keepdims=True)
    nt = (values * lax.rsqrt(mean_square + 1e-06)).astype(jnp.bfloat16)
    first = jax.nn.sigmoid(route_logits[:, 0] - route_logits[:, 1])
    second = jax.nn.sigmoid(route_logits[:, 1] - route_logits[:, 0])
    weight = first * (routes[:, 0] == e).astype(jnp.float32)
    weight = (weight + second * (routes[:, 1] == e).astype(jnp.float32)).astype(jnp.bfloat16)
    count = weight.shape[0]
    wt = jnp.broadcast_to(jnp.pad(weight, (0, LANES - count))[None], (16, LANES))

    gu, ds, tok, wall = run_hand_over(FS, TP, wp, dn, nt, wt)
    gate_served = gu[0].reshape(1, FS * rows, ff // slices)
    up_served = gu[1].reshape(1, FS * rows, ff // slices)
    down_served = ds.reshape(1, 2 * hrows, TP * dn.shape[2])
    x_all = tok.reshape(FS * count, -1)
    w_all = wall[:, 0, :count].reshape(FS * count)

    contract = (((0,), (1,)), ((), ()))
    gate_act = lax.dot_general(gate_served[0], x_all, contract, preferred_element_type=jnp.float32)
    up_act = lax.dot_general(up_served[0], x_all, contract, preferred_element_type=jnp.float32)
    hidden = (jax.nn.silu(gate_act) * up_act * w_all[None, :].astype(jnp.float32)).astype(jnp.bfloat16)
    every = lax.all_gather(hidden, "tp", axis=0, tiled=True)
    down = w_down.astype(jnp.bfloat16).reshape(-1, w_down.shape[2])
    part = lax.dot_general(every, down, (((0,), (0,)), ((), ())), preferred_element_type=jnp.float32)
    mixed = lax.psum_scatter(part, "fs", scatter_dimension=0, tiled=True)
    return (gate_served, up_served, down_served, mixed.astype(jnp.bfloat16))


def solution(mesh):
    return jax.shard_map(
        functools.partial(body, mesh.shape["fs"], mesh.shape["tp"]),
        mesh=mesh,
        in_specs=(
            P(("grp", "fs"), None),
            P(("grp", "fs"), None),
            P(("grp", "fs"), None),
            P("fs"),
            P(None, "fs", "tp"),
            P(None, "fs", "tp"),
            P(None, "fs", "tp"),
        ),
        out_specs=(
            P(("grp", "tp"), None, "fs"),
            P(("grp", "tp"), None, "fs"),
            P(("grp", "tp"), "fs", None),
            P(("grp", "fs"), "tp"),
        ),
        check_vma=False,
    )
```

```python
import functools

import jax
import jax.numpy as jnp
from jax import lax
from jax.experimental import pallas as pl
from jax.experimental.pallas import tpu as pltpu
from jax.sharding import PartitionSpec as P

MESH = pl.DeviceIdType.MESH
DMA = pltpu.SemaphoreType.DMA
LANES = 128


def remote(src, dst, send, recv, **where):
    return pltpu.make_async_remote_copy(
        src_ref=src, dst_ref=dst, send_sem=send, recv_sem=recv, device_id=where, device_id_type=MESH
    )


def hand_over(
    FS, TP, wp, dn, nt, wt, gu, ds, tok, wall, xr,
    xw_s, xw_r, xd_s, xd_r, loc, wt_s, wt_r, rs, rr, xt_s, xt_r, xo_s, xo_r,
    cc_s, cc_r, za_s, za_r, y_s, y_r, yd_s, yd_r,
):
    Z = FS // 2
    H = Z // 2
    x, f, g = lax.axis_index("tp"), lax.axis_index("fs"), lax.axis_index("grp")
    z, c = f // 2, f % 2
    p = g % 2
    mate = g + 1 - 2 * p
    slices = wp.shape[1]
    fb = nt.shape[1] // TP
    half = nt.shape[0] // 2
    db = dn.shape[2]

    def cols(i):
        return pl.ds(pl.multiple_of(i * fb, LANES), fb)

    def dcols(i):
        return pl.ds(pl.multiple_of(i * db, LANES), db)

    barrier = pltpu.get_barrier_semaphore()

    def greet(r, _):
        pl.semaphore_signal(barrier, inc=1, device_id={"fs": (f + r) % FS}, device_id_type=MESH)
        return 0

    lax.fori_loop(1, FS, greet, 0)
    for k in range(1, TP):
        pl.semaphore_signal(barrier, inc=1, device_id={"tp": (x + k) % TP}, device_id_type=MESH)
    pl.semaphore_signal(barrier, inc=1, device_id={"grp": mate}, device_id_type=MESH)
    pl.semaphore_wait(barrier, FS - 1 + TP - 1 + 1)

    def ring(i, fo, side):
        to = ((z + 1) % Z if side == 0 else (z + Z - 1) % Z) * 2 + c
        return remote(tok.at[fo, :, cols(x)], tok.at[fo, :, cols(x)], rs.at[side, i], rr.at[side, i], fs=to)

    def ring_first(side):
        to = ((z + 1) % Z if side == 0 else (z + Z - 1) % Z) * 2 + c
        return remote(nt.at[:, cols(x)], tok.at[f, :, cols(x)], rs.at[side, 0], rr.at[side, 0], fs=to)

    ring_first(0).start()
    ring_first(1).start()
    other = f + 1 - 2 * c
    own_cross = remote(nt, tok.at[f], cc_s.at[Z - 1], cc_r.at[Z - 1], fs=other)
    own_cross.start()

    def xw(k):
        return remote(wp.at[(x + k) % TP], xr.at[x], xw_s.at[k - 1], xw_r.at[k - 1], tp=(x + k) % TP)

    def xd(k):
        return remote(dn.at[(x + k) % TP], ds.at[p, :, dcols(x)], xd_s.at[k - 1], xd_r.at[k - 1], tp=(x + k) % TP)

    for k in (2, 1, 3):
        xw(k).start()
    for k in (2, 1, 3):
        xd(k).start()
    local = [
        pltpu.make_async_copy(wp.at[x], xr.at[x], loc.at[0]),
        pltpu.make_async_copy(dn.at[x], ds.at[p, :, dcols(x)], loc.at[1]),
        pltpu.make_async_copy(nt, tok.at[f], loc.at[2]),
        pltpu.make_async_copy(wt, wall.at[f], loc.at[3]),
    ]
    for copy in local:
        copy.start()

    def tell(r, _):
        remote(wt, wall.at[f], wt_s, wt_r, fs=(f + r) % FS).start()
        return 0

    lax.fori_loop(1, FS, tell, 0)

    def across(i, fo, side):
        to = (x + 1) % TP if side == 0 else (x + TP - 1) % TP
        return remote(tok.at[fo, :, cols(x)], tok.at[fo, :, cols(x)], xt_s.at[side, i], xt_r.at[side, i], tp=to)

    def from_left(s):
        return ((z + Z - s) % Z) * 2 + c

    def from_right(s):
        return ((z + s) % Z) * 2 + c

    def ring_step(s, _):
        fo = from_left(s)
        ring(s - 1, fo, 0).wait_recv()
        ring(s, fo, 0).start()
        fo2 = from_right(s)
        ring(s - 1, fo2, 1).wait_recv()

        @pl.when(s < H - 1)
        def _():
            ring(s, fo2, 1).start()

        for side in (0, 1):
            across(2 * s - 2, fo, side).start()
            across(2 * s - 1, fo2, side).start()
        return 0

    lax.fori_loop(1, H, ring_step, 0)
    last = from_left(H)
    ring(H - 1, last, 0).wait_recv()
    for side in (0, 1):
        across(2 * H - 2, last, side).start()

    for copy in local:
        copy.wait()
    for k in (2, 1, 3):
        xw(k).wait_recv()

    def apart(i):
        m = H - 1 - (i - 1) // 2
        return jnp.where(i == 0, H, jnp.where(i % 2 == 1, m, Z - m))

    def za(d, cd):
        to = ((z + d) % Z) * 2 + cd
        return remote(
            xr.at[to // slices, to % slices], gu.at[:, f, p], za_s.at[d, cd], za_r.at[d, c], fs=to
        )

    def za_recv(d, cs):
        fo = ((z + Z - d) % Z) * 2 + cs
        return remote(xr.at[0, 0], gu.at[:, fo, p], za_s.at[d, cs], za_r.at[d, cs], fs=other)

    def za_start(i, _):
        d = apart(i)
        za(d, 0).start()
        za(d, 1).start()
        return 0

    lax.fori_loop(0, Z - 1, za_start, 0)
    za(0, 1 - c).start()
    own = pltpu.make_async_copy(xr.at[f // slices, f % slices], gu.at[:, f, p], loc.at[4])
    own.start()

    for k in (2, 1, 3):
        xd(k).wait_recv()
    yd = remote(ds.at[p], ds.at[p], yd_s, yd_r, grp=mate)
    yd.start()

    def y_hand(d):
        zo = (z + Z - d) % Z
        part = gu.at[:, pl.ds(2 * zo, 2), p]
        return remote(part, part, y_s.at[d], y_r.at[d], grp=mate)

    def origin(i):
        s = i // 2 + 1
        return jnp.where(i % 2 == 0, from_left(s), from_right(s))

    def onward(i, fo, side):
        to = (x + 1) % TP if side == 0 else (x + TP - 1) % TP
        held = (x + TP - 1) % TP if side == 0 else (x + 1) % TP
        part = tok.at[fo, pl.ds(side * half, half), cols(held)]
        return remote(part, part, xo_s.at[side, i], xo_r.at[side, i], tp=to)

    def cross(i, fo):
        return remote(tok.at[fo], tok.at[fo], cc_s.at[i], cc_r.at[i], fs=other)

    def finish(i):
        fo = origin(i)
        for side in (0, 1):
            onward(i, fo, side).wait_recv()
        cross(i, fo).start()

    def flow(i, _):
        fo = origin(i)
        for side in (0, 1):
            across(i, fo, side).wait_recv()
            onward(i, fo, side).start()
        d = apart(i)
        za_recv(d, 0).wait_recv()
        za_recv(d, 1).wait_recv()
        y_hand(d).start()

        @pl.when(i > 0)
        def _():
            finish(i - 1)

        return 0

    lax.fori_loop(0, Z - 1, flow, 0)
    own.wait()
    za_recv(0, 1 - c).wait_recv()
    y_hand(0).start()
    finish(Z - 2)

    def drain(i, _):
        fo = origin(i)
        for side in (0, 1):
            across(i, fo, side).wait_send()
            onward(i, fo, side).wait_send()
        cross(i, fo).wait()
        d = apart(i)
        za(d, 0).wait_send()
        za(d, 1).wait_send()
        y_hand(d).wait()
        return 0

    lax.fori_loop(0, Z - 1, drain, 0)

    def ring_drain(s, _):
        ring(s, f, 0).wait_send()

        @pl.when(s < H - 1)
        def _():
            ring(s, f, 1).wait_send()

        return 0

    lax.fori_loop(0, H, ring_drain, 0)
    own_cross.wait()
    za(0, 1 - c).wait_send()
    y_hand(0).wait()
    yd.wait()
    for k in (1, 2, 3):
        xw(k).wait_send()
        xd(k).wait_send()
    tiles = remote(wall.at[pl.ds(0, FS - 1)], wall.at[pl.ds(0, FS - 1)], wt_s, wt_r, fs=other)
    tiles.wait_send()
    tiles.wait_recv()


def run_hand_over(FS, TP, wp, dn, nt, wt):
    Z = FS // 2
    _, slices, two, half, ff = wp.shape
    vmem = pl.BlockSpec(memory_space=pltpu.VMEM)
    hbm = pl.BlockSpec(memory_space=pl.ANY)
    return pl.pallas_call(
        functools.partial(hand_over, FS, TP),
        out_shape=(
            jax.ShapeDtypeStruct((two, FS, 2, half, ff), jnp.bfloat16),
            jax.ShapeDtypeStruct((2, dn.shape[1], TP * dn.shape[2]), jnp.bfloat16),
            jax.ShapeDtypeStruct((FS,) + nt.shape, jnp.bfloat16),
            jax.ShapeDtypeStruct((FS,) + wt.shape, jnp.bfloat16),
        ),
        in_specs=[vmem] * 4,
        out_specs=(hbm, hbm, hbm, vmem),
        scratch_shapes=[
            pltpu.VMEM(wp.shape, jnp.bfloat16),
            DMA((TP - 1,)), DMA((TP - 1,)), DMA((TP - 1,)), DMA((TP - 1,)),
            DMA((5,)), DMA, DMA,
            DMA((2, Z // 2)), DMA((2, Z // 2)),
            DMA((2, Z - 1)), DMA((2, Z - 1)), DMA((2, Z - 1)), DMA((2, Z - 1)),
            DMA((Z,)), DMA((Z,)),
            DMA((Z, 2)), DMA((Z, 2)),
            DMA((Z,)), DMA((Z,)), DMA, DMA,
        ],
        compiler_params=pltpu.CompilerParams(collective_id=0, has_side_effects=True, vmem_limit_bytes=32 << 20),
        cost_estimate=pl.CostEstimate(flops=10**9, bytes_accessed=30 << 20, transcendentals=0),
        name="hand_over",
    )(wp, dn, nt, wt)


def combine(FS, TP, W, ht, wdt, out, hs, part, prec, zs, zr, outt, turned, loc, xd_s, xd_r, xo_s, xo_r, cc_s, cc_r, z_s, z_r, fin_s, fin_r):
    Z = FS // 2
    H = Z // 2
    x, f = lax.axis_index("tp"), lax.axis_index("fs")
    z, c = f // 2, f % 2
    other = f + 1 - 2 * c
    ff, block = hs.shape[2], hs.shape[3]
    half = ff // 2
    keep = part.shape[1] // 2
    xside = ((x + 1) % TP, (x + TP - 1) % TP)
    zside = (((z + 1) % Z) * 2 + c, ((z + Z - 1) % Z) * 2 + c)

    barrier = pltpu.get_barrier_semaphore()
    for k in xside:
        pl.semaphore_signal(barrier, inc=1, device_id={"tp": k}, device_id_type=MESH)
    for k in zside + (other,):
        pl.semaphore_signal(barrier, inc=1, device_id={"fs": k}, device_id_type=MESH)
    pl.semaphore_wait(barrier, 5)

    def away(i):
        return H - (i + 1) // 2

    def chip(i):
        return jnp.where(i % 2 == 0, (z + away(i)) % Z, (z + Z - away(i)) % Z)

    def mine(i):
        return ht.at[:, pl.ds(pl.multiple_of(chip(i) * block, LANES), block)]

    def keep_own(i):
        return pltpu.make_async_copy(mine(i), hs.at[i, x], loc.at[i])

    def direct(i, side):
        return remote(mine(i), hs.at[i, x], xd_s.at[side, i], xd_r.at[side, i], tp=xside[side])

    def onward(i, side):
        held = hs.at[i, xside[1 - side], pl.ds(side * half, half)]
        return remote(held, held, xo_s.at[side, i], xo_r.at[side, i], tp=xside[side])

    def cross(j):
        return remote(part.at[j, pl.ds((1 - c) * keep, keep)], prec.at[j], cc_s.at[j], cc_r.at[j], fs=other)

    def walk(m, side):
        k = away(m) - 1
        return remote(zs.at[m], zr.at[side, k], z_s.at[m], z_r.at[side, k], fs=zside[side])

    def arrival(side, k):
        return remote(zs.at[0], zr.at[side, k], z_s.at[0], z_r.at[side, k], fs=zside[side])

    def own_first(i, _):
        keep_own(i).start()
        return 0

    lax.fori_loop(0, Z, own_first, 0)
    for i in range(W):
        for side in (0, 1):
            direct(i, side).start()

    def step(i, _):
        @pl.when(i + W < Z)
        def _():
            for side in (0, 1):
                direct(i + W, side).start()

        @pl.when(i < Z)
        def _():
            for side in (0, 1):
                direct(i, side).wait_recv()
                onward(i, side).start()

        @pl.when((i >= 1) & (i <= Z))
        def _():
            j = i - 1
            keep_own(j).wait()
            for side in (0, 1):
                onward(j, side).wait_recv()
            rhs = hs[j].reshape(TP * ff, block)
            part[j] = jnp.dot(wdt[...], rhs, preferred_element_type=jnp.float32)
            cross(j).start()

        @pl.when(i >= 2)
        def _():
            m = i - 2
            k = away(m)
            cross(m).wait_recv()
            total = part[m, pl.ds(c * keep, keep)] + prec[m]

            @pl.when(m == 0)
            def _():
                zs[m] = total.astype(jnp.bfloat16)

            @pl.when(m == 1)
            def _():
                zs[m] = total.astype(jnp.bfloat16)

            for side in (0, 1):
                @pl.when((m >= 2) & (m < Z - 1) & (m % 2 == side))
                def _():
                    arrival(side, k).wait_recv()
                    zs[m] = (total + zr[side, k].astype(jnp.float32)).astype(jnp.bfloat16)

                @pl.when((m < Z - 1) & (m % 2 == side))
                def _():
                    walk(m, side).start()

            @pl.when(m == Z - 1)
            def _():
                arrival(0, 0).wait_recv()
                arrival(1, 0).wait_recv()
                both = zr[0, 0].astype(jnp.float32) + zr[1, 0].astype(jnp.float32)
                outt[pl.ds(c * keep, keep)] = (total + both).astype(jnp.bfloat16)

        return 0

    lax.fori_loop(0, Z + 2, step, 0)
    last = remote(outt.at[pl.ds(c * keep, keep)], outt.at[pl.ds(c * keep, keep)], fin_s, fin_r, fs=other)
    last.start()

    def drain(i, _):
        for side in (0, 1):
            direct(i, side).wait_send()
            onward(i, side).wait_send()
        cross(i).wait_send()

        @pl.when(i < Z - 1)
        def _():
            arrival_of = remote(zs.at[i], zr.at[0, 0], z_s.at[i], z_r.at[0, 0], fs=other)
            arrival_of.wait_send()

        return 0

    lax.fori_loop(0, Z, drain, 0)
    last.wait()
    turned[...] = outt[...].astype(jnp.float32).T
    rows = block // 2
    out[...] = turned[pl.ds(c * rows, rows)].astype(jnp.bfloat16)


def run_combine(FS, TP, ht, wdt):
    Z = FS // 2
    ff, tokens = ht.shape
    block = tokens // Z
    feats = wdt.shape[0]
    vmem = pl.BlockSpec(memory_space=pltpu.VMEM)
    return pl.pallas_call(
        functools.partial(combine, FS, TP, 3),
        out_shape=jax.ShapeDtypeStruct((block // 2, feats), jnp.bfloat16),
        in_specs=[vmem] * 2,
        out_specs=vmem,
        scratch_shapes=[
            pltpu.VMEM((Z, TP, ff, block), jnp.bfloat16),
            pltpu.VMEM((Z, feats, block), jnp.float32),
            pltpu.VMEM((Z, feats // 2, block), jnp.float32),
            pltpu.VMEM((Z - 1, feats // 2, block), jnp.bfloat16),
            pltpu.VMEM((2, Z // 2, feats // 2, block), jnp.bfloat16),
            pltpu.VMEM((feats, block), jnp.bfloat16),
            pltpu.VMEM((block, feats), jnp.float32),
            DMA((Z,)), DMA((2, Z)), DMA((2, Z)), DMA((2, Z)), DMA((2, Z)),
            DMA((Z,)), DMA((Z,)), DMA((Z - 1,)), DMA((2, Z // 2)), DMA, DMA,
        ],
        compiler_params=pltpu.CompilerParams(collective_id=1, has_side_effects=True, vmem_limit_bytes=32 << 20),
        cost_estimate=pl.CostEstimate(flops=10**9, bytes_accessed=30 << 20, transcendentals=0),
        name="combine",
    )(ht, wdt)


def body(FS, TP, tokens, routes, route_logits, gain, w_gate, w_up, w_down):
    p = lax.axis_index("grp") % 2
    e = lax.axis_index("tp")
    rows, ff = w_gate.shape[1:]
    slices = FS // TP
    half = rows // 2

    def mine(w):
        part = lax.dynamic_slice_in_dim(w, p * half, half, 1)
        scale = lax.dynamic_slice_in_dim(gain, p * half, half, 0)
        part = (part * scale[None, :, None]).astype(jnp.bfloat16)
        return part.reshape(TP, half, slices, ff // slices).transpose(0, 2, 1, 3)

    wp = jnp.stack([mine(w_gate), mine(w_up)], axis=2)
    hrows = w_down.shape[1] // 2
    dn = lax.dynamic_slice_in_dim(w_down, p * hrows, hrows, 1).astype(jnp.bfloat16)

    values = tokens.astype(jnp.float32)
    mean_square = jnp.mean(values * values, axis=-1, keepdims=True)
    nt = (values * lax.rsqrt(mean_square + 1e-06)).astype(jnp.bfloat16)
    first = jax.nn.sigmoid(route_logits[:, 0] - route_logits[:, 1])
    second = jax.nn.sigmoid(route_logits[:, 1] - route_logits[:, 0])
    weight = first * (routes[:, 0] == e).astype(jnp.float32)
    weight = (weight + second * (routes[:, 1] == e).astype(jnp.float32)).astype(jnp.bfloat16)
    count = weight.shape[0]
    wt = jnp.broadcast_to(jnp.pad(weight, (0, LANES - count))[None], (16, LANES))

    gu, ds, tok, wall = run_hand_over(FS, TP, wp, dn, nt, wt)
    gate_served = gu[0].reshape(1, FS * rows, ff // slices)
    up_served = gu[1].reshape(1, FS * rows, ff // slices)
    down_served = ds.reshape(1, 2 * hrows, TP * dn.shape[2])
    x_all = tok.reshape(FS * count, -1)
    w_all = wall[:, 0, :count].reshape(FS * count)

    contract = (((0,), (1,)), ((), ()))
    gate_act = lax.dot_general(gate_served[0], x_all, contract, preferred_element_type=jnp.float32)
    up_act = lax.dot_general(up_served[0], x_all, contract, preferred_element_type=jnp.float32)
    hidden = (jax.nn.silu(gate_act) * up_act * w_all[None, :].astype(jnp.float32)).astype(jnp.bfloat16)
    wdt = w_down.astype(jnp.bfloat16).reshape(-1, w_down.shape[2]).T
    mixed = run_combine(FS, TP, hidden, wdt)
    return (gate_served, up_served, down_served, mixed)


def solution(mesh):
    return jax.shard_map(
        functools.partial(body, mesh.shape["fs"], mesh.shape["tp"]),
        mesh=mesh,
        in_specs=(
            P(("grp", "fs"), None),
            P(("grp", "fs"), None),
            P(("grp", "fs"), None),
            P("fs"),
            P(None, "fs", "tp"),
            P(None, "fs", "tp"),
            P(None, "fs", "tp"),
        ),
        out_specs=(
            P(("grp", "tp"), None, "fs"),
            P(("grp", "tp"), None, "fs"),
            P(("grp", "tp"), "fs", None),
            P(("grp", "fs"), "tp"),
        ),
        check_vma=False,
    )
```

```python
import functools

import jax
import jax.numpy as jnp
from jax import lax
from jax.experimental import pallas as pl
from jax.experimental.pallas import tpu as pltpu
from jax.sharding import PartitionSpec as P

MESH = pl.DeviceIdType.MESH
DMA = pltpu.SemaphoreType.DMA
LANES = 128


def remote(src, dst, send, recv, **where):
    return pltpu.make_async_remote_copy(
        src_ref=src, dst_ref=dst, send_sem=send, recv_sem=recv, device_id=where, device_id_type=MESH
    )


def hand_over(
    FS, TP, START, wp, dn, nt, wt, gu, ds, tok, wall, xr, stage,
    xw_s, xw_r, st_s, st_r, sf_s, sf_r, xd_s, xd_r, loc, wt_s, wt_r, rs, rr, xt_s, xt_r, xo_s, xo_r,
    cc_s, cc_r, za_s, za_r, y_s, y_r, yd_s, yd_r,
):
    Z = FS // 2
    H = Z // 2
    N = H - START + 1
    B = (Z - 1) // N
    assert B * N == Z - 1
    x, f, g = lax.axis_index("tp"), lax.axis_index("fs"), lax.axis_index("grp")
    z, c = f // 2, f % 2
    p = g % 2
    mate = g + 1 - 2 * p
    slices = wp.shape[1]
    hs = slices // 2
    fb = nt.shape[1] // TP
    half = nt.shape[0] // 2
    db = dn.shape[2]
    other = f + 1 - 2 * c
    xside = ((x + 1) % TP, (x + TP - 1) % TP)
    zside = (((z + 1) % Z) * 2 + c, ((z + Z - 1) % Z) * 2 + c)
    opposite = (x + 2) % TP

    def cols(i):
        return pl.ds(pl.multiple_of(i * fb, LANES), fb)

    def dcols(i):
        return pl.ds(pl.multiple_of(i * db, LANES), db)

    barrier = pltpu.get_barrier_semaphore()

    def greet(r, _):
        pl.semaphore_signal(barrier, inc=1, device_id={"fs": (f + r) % FS}, device_id_type=MESH)
        return 0

    lax.fori_loop(1, FS, greet, 0)
    for k in range(1, TP):
        pl.semaphore_signal(barrier, inc=1, device_id={"tp": (x + k) % TP}, device_id_type=MESH)
    pl.semaphore_signal(barrier, inc=1, device_id={"grp": mate}, device_id_type=MESH)
    pl.semaphore_wait(barrier, FS - 1 + TP - 1 + 1)

    def ring(i, fo, side):
        return remote(tok.at[fo, :, cols(x)], tok.at[fo, :, cols(x)], rs.at[side, i], rr.at[side, i], fs=zside[side])

    def ring_first(side):
        return remote(nt.at[:, cols(x)], tok.at[f, :, cols(x)], rs.at[side, 0], rr.at[side, 0], fs=zside[side])

    ring_first(0).start()
    ring_first(1).start()

    def first_leg(side):
        return remote(
            wp.at[opposite, pl.ds(side * hs, hs)], stage.at[side], st_s.at[side], st_r.at[side], tp=xside[side]
        )

    def second_leg(side):
        held = xside[1 - side]
        return remote(
            stage.at[side], xr.at[held, pl.ds(side * hs, hs)], sf_s.at[side], sf_r.at[side], tp=xside[side]
        )

    def second_leg_recv(side):
        return remote(
            stage.at[side], xr.at[opposite, pl.ds(side * hs, hs)], sf_s.at[side], sf_r.at[side], tp=xside[side]
        )

    def xw(side):
        return remote(wp.at[xside[side]], xr.at[x], xw_s.at[side], xw_r.at[side], tp=xside[side])

    def xw_recv(side):
        return remote(wp.at[x], xr.at[xside[1 - side]], xw_s.at[side], xw_r.at[side], tp=xside[side])

    def xd(k):
        return remote(dn.at[(x + k) % TP], ds.at[p, :, dcols(x)], xd_s.at[k - 1], xd_r.at[k - 1], tp=(x + k) % TP)

    def xd_recv(k):
        return remote(
            dn.at[x], ds.at[p, :, dcols((x + TP - k) % TP)], xd_s.at[k - 1], xd_r.at[k - 1], tp=(x + k) % TP
        )

    for side in (0, 1):
        first_leg(side).start()
    for side in (0, 1):
        xw(side).start()
    own_cross = remote(nt, tok.at[f], cc_s.at[Z - 1], cc_r.at[Z - 1], fs=other)
    own_cross.start()
    local = [
        pltpu.make_async_copy(wp.at[x], xr.at[x], loc.at[0]),
        pltpu.make_async_copy(dn.at[x], ds.at[p, :, dcols(x)], loc.at[1]),
        pltpu.make_async_copy(nt, tok.at[f], loc.at[2]),
        pltpu.make_async_copy(wt, wall.at[f], loc.at[3]),
    ]
    for copy in local:
        copy.start()

    def tell(r, _):
        remote(wt, wall.at[f], wt_s, wt_r, fs=(f + r) % FS).start()
        return 0

    lax.fori_loop(1, FS, tell, 0)

    def across(i, fo, side):
        return remote(
            tok.at[fo, :, cols(x)], tok.at[fo, :, cols(x)], xt_s.at[side, i], xt_r.at[side, i], tp=xside[side]
        )

    def across_recv(i, fo, side):
        held = tok.at[fo, :, cols(xside[1 - side])]
        return remote(held, held, xt_s.at[side, i], xt_r.at[side, i], tp=xside[side])

    def from_left(s):
        return ((z + Z - s) % Z) * 2 + c

    def from_right(s):
        return ((z + s) % Z) * 2 + c

    def origin(i):
        s = i // 2 + 1
        return jnp.where(i % 2 == 0, from_left(s), from_right(s))

    def ring_step(s):
        fo = from_left(s)
        ring(s - 1, fo, 0).wait_recv()

        @pl.when(s < H)
        def _():
            ring(s, fo, 0).start()

        for side in (0, 1):
            across(2 * s - 2, fo, side).start()

        @pl.when(s < H)
        def _():
            fo2 = from_right(s)
            ring(s - 1, fo2, 1).wait_recv()

            @pl.when(s < H - 1)
            def _():
                ring(s, fo2, 1).start()

            for side in (0, 1):
                across(2 * s - 1, fo2, side).start()

    ring_step(1)
    for side in (0, 1):
        first_leg(side).wait_recv()
        second_leg(side).start()
    for k in (2, 1, 3):
        xd(k).start()

    def early(s, _):
        ring_step(s)
        return 0

    lax.fori_loop(2, START, early, 0)
    local[0].wait()
    for side in (0, 1):
        xw_recv(side).wait_recv()
        second_leg_recv(side).wait_recv()

    def apart(i):
        m = H - 1 - (i - 1) // 2
        return jnp.where(i == 0, H, jnp.where(i % 2 == 1, m, Z - m))

    def za(d, cd):
        to = ((z + d) % Z) * 2 + cd
        return remote(xr.at[to // slices, to % slices], gu.at[:, f, p], za_s.at[d, cd], za_r.at[d, c], fs=to)

    def za_recv(d, cs):
        fo = ((z + Z - d) % Z) * 2 + cs
        return remote(xr.at[0, 0], gu.at[:, fo, p], za_s.at[d, cs], za_r.at[d, cs], fs=other)

    def y_hand(d):
        zo = (z + Z - d) % Z
        part = gu.at[:, pl.ds(2 * zo, 2), p]
        return remote(part, part, y_s.at[d], y_r.at[d], grp=mate)

    def y_recv(d):
        zo = (z + Z - d) % Z
        part = gu.at[:, pl.ds(2 * zo, 2), 1 - p]
        return remote(part, part, y_s.at[d], y_r.at[d], grp=mate)

    def onward(i, fo, side):
        part = tok.at[fo, pl.ds(side * half, half), cols(xside[1 - side])]
        return remote(part, part, xo_s.at[side, i], xo_r.at[side, i], tp=xside[side])

    def onward_recv(i, fo, side):
        part = tok.at[fo, pl.ds(side * half, half), cols(opposite)]
        return remote(part, part, xo_s.at[side, i], xo_r.at[side, i], tp=xside[side])

    def cross(i, fo):
        return remote(tok.at[fo], tok.at[fo], cc_s.at[i], cc_r.at[i], fs=other)

    def cross_recv(i, fo):
        return remote(tok.at[fo + 1 - 2 * c], tok.at[fo + 1 - 2 * c], cc_s.at[i], cc_r.at[i], fs=other)

    own = pltpu.make_async_copy(xr.at[f // slices, f % slices], gu.at[:, f, p], loc.at[4])
    own.start()
    yd = remote(ds.at[p], ds.at[p], yd_s, yd_r, grp=mate)

    def taken(t):
        for n in range(B):
            i = t * B + n
            fo = origin(i)
            for side in (0, 1):
                onward_recv(i, fo, side).wait_recv()
            cross(i, fo).start()
        for n in range(B):
            d = apart(t * B + n)
            za_recv(d, 0).wait_recv()
            za_recv(d, 1).wait_recv()
            y_hand(d).start()

    def flow(t, _):
        ring_step(START + t)
        for n in range(B):
            d = apart(t * B + n)
            za(d, 0).start()
            za(d, 1).start()
        for n in range(B):
            i = t * B + n
            fo = origin(i)
            for side in (0, 1):
                across_recv(i, fo, side).wait_recv()
                onward(i, fo, side).start()

        @pl.when(t == 0)
        def _():
            za(0, 1 - c).start()
            local[1].wait()
            for k in (2, 1, 3):
                xd_recv(k).wait_recv()
            yd.start()

        @pl.when(t > 0)
        def _():
            taken(t - 1)

        return 0

    lax.fori_loop(0, N, flow, 0)
    own.wait()
    za_recv(0, 1 - c).wait_recv()
    y_hand(0).start()
    taken(N - 1)

    own_fo = f + 1 - 2 * c
    remote(nt, tok.at[own_fo], cc_s.at[Z - 1], cc_r.at[Z - 1], fs=other).wait_recv()

    def drain(i, _):
        fo = origin(i)
        for side in (0, 1):
            across(i, fo, side).wait_send()
            onward(i, fo, side).wait_send()
        cross(i, fo).wait_send()
        cross_recv(i, fo).wait_recv()
        d = apart(i)
        za(d, 0).wait_send()
        za(d, 1).wait_send()
        y_hand(d).wait_send()
        y_recv(d).wait_recv()
        return 0

    lax.fori_loop(0, Z - 1, drain, 0)

    def ring_drain(s, _):
        ring(s, f, 0).wait_send()

        @pl.when(s < H - 1)
        def _():
            ring(s, f, 1).wait_send()

        return 0

    lax.fori_loop(0, H, ring_drain, 0)
    own_cross.wait_send()
    za(0, 1 - c).wait_send()
    y_hand(0).wait_send()
    y_recv(0).wait_recv()
    yd.wait_send()
    remote(ds.at[1 - p], ds.at[1 - p], yd_s, yd_r, grp=mate).wait_recv()
    for side in (0, 1):
        first_leg(side).wait_send()
        second_leg(side).wait_send()
        xw(side).wait_send()
    for k in range(1, TP):
        xd(k).wait_send()
    local[2].wait()
    local[3].wait()
    tiles = remote(wall.at[pl.ds(0, FS - 1)], wall.at[pl.ds(0, FS - 1)], wt_s, wt_r, fs=other)
    tiles.wait_send()
    tiles.wait_recv()


def run_hand_over(FS, TP, wp, dn, nt, wt):
    Z = FS // 2
    _, slices, two, half, ff = wp.shape
    vmem = pl.BlockSpec(memory_space=pltpu.VMEM)
    return pl.pallas_call(
        functools.partial(hand_over, FS, TP, Z // 4),
        out_shape=(
            jax.ShapeDtypeStruct((two, FS, 2, half, ff), jnp.bfloat16),
            jax.ShapeDtypeStruct((2, dn.shape[1], TP * dn.shape[2]), jnp.bfloat16),
            jax.ShapeDtypeStruct((FS,) + nt.shape, jnp.bfloat16),
            jax.ShapeDtypeStruct((FS,) + wt.shape, jnp.bfloat16),
        ),
        in_specs=[vmem] * 4,
        out_specs=(vmem,) * 4,
        scratch_shapes=[
            pltpu.VMEM(wp.shape, jnp.bfloat16),
            pltpu.VMEM((2, slices // 2) + wp.shape[2:], jnp.bfloat16),
            DMA((2,)), DMA((2,)), DMA((2,)), DMA((2,)), DMA((2,)), DMA((2,)),
            DMA((TP - 1,)), DMA((TP - 1,)),
            DMA((5,)), DMA, DMA,
            DMA((2, Z // 2)), DMA((2, Z // 2)),
            DMA((2, Z - 1)), DMA((2, Z - 1)), DMA((2, Z - 1)), DMA((2, Z - 1)),
            DMA((Z,)), DMA((Z,)),
            DMA((Z, 2)), DMA((Z, 2)),
            DMA((Z,)), DMA((Z,)), DMA, DMA,
        ],
        compiler_params=pltpu.CompilerParams(collective_id=0, has_side_effects=True, vmem_limit_bytes=8 << 20),
        cost_estimate=pl.CostEstimate(flops=10**9, bytes_accessed=30 << 20, transcendentals=0),
        name="hand_over",
    )(wp, dn, nt, wt)


def expert(block, gu, x, w, ht, gate_out, up_out):
    features = x.shape[2]
    count = block // x.shape[1]

    def step(i, _):
        span = pl.ds(pl.multiple_of(i * block, block), block)
        part = pl.ds(i * count, count)
        rows = x[part].reshape(block, features)
        gate = jnp.dot(rows, gu[0].reshape(features, -1), preferred_element_type=jnp.float32)
        up = jnp.dot(rows, gu[1].reshape(features, -1), preferred_element_type=jnp.float32)
        scale = jnp.concatenate([w[i * count + n, 0:1, : x.shape[1]] for n in range(count)], axis=1)
        ht[:, span] = ((jax.nn.silu(gate) * up).T * scale.astype(jnp.float32)).astype(jnp.bfloat16)
        for n, served in ((0, gate_out), (1, up_out)):
            served[:, span] = gu[n, part].reshape(block, -1).astype(jnp.float32).T.astype(jnp.bfloat16)
        return 0

    lax.fori_loop(0, features // block, step, 0)


def run_expert(gu, x, w):
    tokens, features = x.shape[0] * x.shape[1], x.shape[2]
    assert tokens == features
    ff = gu.shape[-1]
    vmem = pl.BlockSpec(memory_space=pltpu.VMEM)
    return pl.pallas_call(
        functools.partial(expert, 256),
        out_shape=(
            jax.ShapeDtypeStruct((ff, tokens), jnp.bfloat16),
            jax.ShapeDtypeStruct((ff, features), jnp.bfloat16),
            jax.ShapeDtypeStruct((ff, features), jnp.bfloat16),
        ),
        in_specs=[vmem] * 3,
        out_specs=(vmem,) * 3,
        compiler_params=pltpu.CompilerParams(vmem_limit_bytes=12 << 20),
        cost_estimate=pl.CostEstimate(flops=4 * 10**9, bytes_accessed=16 << 20, transcendentals=0),
        name="expert",
    )(gu, x, w)


def combine(FS, TP, W, ht, wd, out, wdt, hs, part, prec, zs, zr, outt, turned, loc, xd_s, xd_r, xo_s, xo_r, cc_s, cc_r, z_s, z_r, fin_s, fin_r):
    Z = FS // 2
    H = Z // 2
    x, f = lax.axis_index("tp"), lax.axis_index("fs")
    z, c = f // 2, f % 2
    other = f + 1 - 2 * c
    ff, block = hs.shape[2], hs.shape[3]
    half = ff // 2
    keep = part.shape[1] // 2
    xside = ((x + 1) % TP, (x + TP - 1) % TP)
    zside = (((z + 1) % Z) * 2 + c, ((z + Z - 1) % Z) * 2 + c)

    barrier = pltpu.get_barrier_semaphore()
    for k in xside:
        pl.semaphore_signal(barrier, inc=1, device_id={"tp": k}, device_id_type=MESH)
    for k in zside + (other,):
        pl.semaphore_signal(barrier, inc=1, device_id={"fs": k}, device_id_type=MESH)
    pl.semaphore_wait(barrier, 5)

    def away(i):
        return H - (i + 1) // 2

    def chip(i):
        return jnp.where(i % 2 == 0, (z + away(i)) % Z, (z + Z - away(i)) % Z)

    def mine(i):
        return ht.at[:, pl.ds(pl.multiple_of(chip(i) * block, LANES), block)]

    def keep_own(i):
        return pltpu.make_async_copy(mine(i), hs.at[i, x], loc.at[i])

    def direct(i, side):
        return remote(mine(i), hs.at[i, x], xd_s.at[side, i], xd_r.at[side, i], tp=xside[side])

    def onward(i, side):
        held = hs.at[i, xside[1 - side], pl.ds(side * half, half)]
        return remote(held, held, xo_s.at[side, i], xo_r.at[side, i], tp=xside[side])

    def cross(j):
        return remote(part.at[j, pl.ds((1 - c) * keep, keep)], prec.at[j], cc_s.at[j], cc_r.at[j], fs=other)

    def walk(m, side):
        k = away(m) - 1
        return remote(zs.at[m], zr.at[side, k], z_s.at[m], z_r.at[side, k], fs=zside[side])

    def arrival(side, k):
        return remote(zs.at[0], zr.at[side, k], z_s.at[0], z_r.at[side, k], fs=zside[side])

    def own_first(i, _):
        keep_own(i).start()
        return 0

    lax.fori_loop(0, Z, own_first, 0)
    for i in range(W):
        for side in (0, 1):
            direct(i, side).start()
    for e in range(TP):
        wdt[:, e * ff : (e + 1) * ff] = wd[e].T.astype(jnp.bfloat16)

    def step(i, _):
        @pl.when(i + W < Z)
        def _():
            for side in (0, 1):
                direct(i + W, side).start()

        @pl.when(i < Z)
        def _():
            for side in (0, 1):
                direct(i, side).wait_recv()
                onward(i, side).start()

        @pl.when((i >= 1) & (i <= Z))
        def _():
            j = i - 1
            keep_own(j).wait()
            for side in (0, 1):
                onward(j, side).wait_recv()
            rhs = hs[j].reshape(TP * ff, block)
            part[j] = jnp.dot(wdt[...], rhs, preferred_element_type=jnp.float32)
            cross(j).start()

        @pl.when(i >= 2)
        def _():
            m = i - 2
            k = away(m)
            cross(m).wait_recv()
            total = part[m, pl.ds(c * keep, keep)] + prec[m]

            @pl.when(m == 0)
            def _():
                zs[m] = total.astype(jnp.bfloat16)

            @pl.when(m == 1)
            def _():
                zs[m] = total.astype(jnp.bfloat16)

            for side in (0, 1):
                @pl.when((m >= 2) & (m < Z - 1) & (m % 2 == side))
                def _():
                    arrival(side, k).wait_recv()
                    zs[m] = (total + zr[side, k].astype(jnp.float32)).astype(jnp.bfloat16)

                @pl.when((m < Z - 1) & (m % 2 == side))
                def _():
                    walk(m, side).start()

            @pl.when(m == Z - 1)
            def _():
                arrival(0, 0).wait_recv()
                arrival(1, 0).wait_recv()
                both = zr[0, 0].astype(jnp.float32) + zr[1, 0].astype(jnp.float32)
                outt[pl.ds(c * keep, keep)] = (total + both).astype(jnp.bfloat16)

        return 0

    lax.fori_loop(0, Z + 2, step, 0)
    last = remote(outt.at[pl.ds(c * keep, keep)], outt.at[pl.ds(c * keep, keep)], fin_s, fin_r, fs=other)
    last.start()

    def drain(i, _):
        for side in (0, 1):
            direct(i, side).wait_send()
            onward(i, side).wait_send()
        cross(i).wait_send()

        @pl.when(i < Z - 1)
        def _():
            arrival_of = remote(zs.at[i], zr.at[0, 0], z_s.at[i], z_r.at[0, 0], fs=other)
            arrival_of.wait_send()

        return 0

    lax.fori_loop(0, Z, drain, 0)
    last.wait()
    turned[...] = outt[...].astype(jnp.float32).T
    rows = block // 2
    out[...] = turned[pl.ds(c * rows, rows)].astype(jnp.bfloat16)


def run_combine(FS, TP, ht, wd):
    Z = FS // 2
    ff, tokens = ht.shape
    block = tokens // Z
    feats = wd.shape[2]
    vmem = pl.BlockSpec(memory_space=pltpu.VMEM)
    return pl.pallas_call(
        functools.partial(combine, FS, TP, 3),
        out_shape=jax.ShapeDtypeStruct((block // 2, feats), jnp.bfloat16),
        in_specs=[vmem] * 2,
        out_specs=vmem,
        scratch_shapes=[
            pltpu.VMEM((feats, TP * ff), jnp.bfloat16),
            pltpu.VMEM((Z, TP, ff, block), jnp.bfloat16),
            pltpu.VMEM((Z, feats, block), jnp.float32),
            pltpu.VMEM((Z, feats // 2, block), jnp.float32),
            pltpu.VMEM((Z - 1, feats // 2, block), jnp.bfloat16),
            pltpu.VMEM((2, Z // 2, feats // 2, block), jnp.bfloat16),
            pltpu.VMEM((feats, block), jnp.bfloat16),
            pltpu.VMEM((block, feats), jnp.float32),
            DMA((Z,)), DMA((2, Z)), DMA((2, Z)), DMA((2, Z)), DMA((2, Z)),
            DMA((Z,)), DMA((Z,)), DMA((Z - 1,)), DMA((2, Z // 2)), DMA, DMA,
        ],
        compiler_params=pltpu.CompilerParams(collective_id=1, has_side_effects=True, vmem_limit_bytes=20 << 20),
        cost_estimate=pl.CostEstimate(flops=10**9, bytes_accessed=30 << 20, transcendentals=0),
        name="combine",
    )(ht, wd)


def body(FS, TP, tokens, routes, route_logits, gain, w_gate, w_up, w_down):
    p = lax.axis_index("grp") % 2
    e = lax.axis_index("tp")
    rows, ff = w_gate.shape[1:]
    slices = FS // TP
    half = rows // 2

    def mine(w):
        part = lax.dynamic_slice_in_dim(w, p * half, half, 1)
        scale = lax.dynamic_slice_in_dim(gain, p * half, half, 0)
        part = (part * scale[None, :, None]).astype(jnp.bfloat16)
        return part.reshape(TP, half, slices, ff // slices).transpose(0, 2, 1, 3)

    wp = jnp.stack([mine(w_gate), mine(w_up)], axis=2)
    hrows = w_down.shape[1] // 2
    dn = lax.dynamic_slice_in_dim(w_down, p * hrows, hrows, 1).astype(jnp.bfloat16)

    values = tokens.astype(jnp.float32)
    mean_square = jnp.mean(values * values, axis=-1, keepdims=True)
    nt = (values * lax.rsqrt(mean_square + 1e-06)).astype(jnp.bfloat16)
    first = jax.nn.sigmoid(route_logits[:, 0] - route_logits[:, 1])
    second = jax.nn.sigmoid(route_logits[:, 1] - route_logits[:, 0])
    weight = first * (routes[:, 0] == e).astype(jnp.float32)
    weight = (weight + second * (routes[:, 1] == e).astype(jnp.float32)).astype(jnp.bfloat16)
    count = weight.shape[0]
    wt = jnp.broadcast_to(jnp.pad(weight, (0, LANES - count))[None], (16, LANES))

    gu, ds, tok, wall = run_hand_over(FS, TP, wp, dn, nt, wt)
    hidden, gate_t, up_t = run_expert(gu, tok, wall)
    mixed = run_combine(FS, TP, hidden, w_down)
    return (gate_t.T[None], up_t.T[None], ds.reshape(1, 2 * hrows, -1), mixed)


def solution(mesh):
    return jax.shard_map(
        functools.partial(body, mesh.shape["fs"], mesh.shape["tp"]),
        mesh=mesh,
        in_specs=(
            P(("grp", "fs"), None),
            P(("grp", "fs"), None),
            P(("grp", "fs"), None),
            P("fs"),
            P(None, "fs", "tp"),
            P(None, "fs", "tp"),
            P(None, "fs", "tp"),
        ),
        out_specs=(
            P(("grp", "tp"), None, "fs"),
            P(("grp", "tp"), None, "fs"),
            P(("grp", "tp"), "fs", None),
            P(("grp", "fs"), "tp"),
        ),
        check_vma=False,
    )
```

```python
import functools

import jax
import jax.numpy as jnp
from jax import lax
from jax.experimental import pallas as pl
from jax.experimental.pallas import tpu as pltpu
from jax.sharding import PartitionSpec as P

MESH = pl.DeviceIdType.MESH
DMA = pltpu.SemaphoreType.DMA
LANES = 128


def remote(src, dst, send, recv, **where):
    return pltpu.make_async_remote_copy(
        src_ref=src, dst_ref=dst, send_sem=send, recv_sem=recv, device_id=where, device_id_type=MESH
    )


def hand_over(
    FS, TP, x_in, routes, logits, gain, w_gate, w_up, w_down, gu, ds, tok, wall,
    raw_gate, raw_up, raw_down, scale, wp, dn, nt, wt, xr, stage,
    in_s, loc, xw_s, xw_r, st_s, st_r, sf_s, sf_r, xd_s, xd_r, rs, rr, ws, wr, xt_s, xt_r, xo_s, xo_r,
    cc_s, cc_r, cw_s, cw_r, za_s, za_r, y_s, y_r, yd_s, yd_r,
):
    Z = FS // 2
    H = Z // 2
    Q = Z // TP
    assert TP == 4 and Q * TP == Z and H == 2 * Q
    x, f, g = lax.axis_index("tp"), lax.axis_index("fs"), lax.axis_index("grp")
    z, c = f // 2, f % 2
    zone, seat = z // Q, z % Q
    p = g % 2
    mate = g + 1 - 2 * p
    fb = nt.shape[1] // TP
    half = nt.shape[0] // 2
    db = dn.shape[2]
    rows = raw_gate.shape[1]
    drows = raw_down.shape[1]
    other = f + 1 - 2 * c
    xside = ((x + 1) % TP, (x + TP - 1) % TP)
    zside = (((z + 1) % Z) * 2 + c, ((z + Z - 1) % Z) * 2 + c)
    opposite = (x + 2) % TP

    fetch = (
        pltpu.make_async_copy(w_gate.at[:, pl.ds(p * rows, rows)], raw_gate, in_s.at[0]),
        pltpu.make_async_copy(w_up.at[:, pl.ds(p * rows, rows)], raw_up, in_s.at[1]),
        pltpu.make_async_copy(w_down.at[:, pl.ds(p * drows, drows)], raw_down, in_s.at[2]),
    )
    for copy in fetch:
        copy.start()

    barrier = pltpu.get_barrier_semaphore()

    def greet(r, _):
        pl.semaphore_signal(barrier, inc=1, device_id={"fs": (f + r) % FS}, device_id_type=MESH)
        return 0

    lax.fori_loop(1, FS, greet, 0)
    for k in range(1, TP):
        pl.semaphore_signal(barrier, inc=1, device_id={"tp": (x + k) % TP}, device_id_type=MESH)
    pl.semaphore_signal(barrier, inc=1, device_id={"grp": mate}, device_id_type=MESH)

    values = x_in[...].astype(jnp.float32)
    mean_square = jnp.mean(values * values, axis=-1, keepdims=True)
    nt[...] = (values * lax.rsqrt(mean_square + 1e-06)).astype(jnp.bfloat16)
    count = routes.shape[1]
    first = jax.nn.sigmoid(logits[0:1] - logits[1:2])
    second = jax.nn.sigmoid(logits[1:2] - logits[0:1])
    weight = first * (routes[0:1] == x).astype(jnp.float32) + second * (routes[1:2] == x).astype(jnp.float32)
    wt[...] = jnp.zeros_like(wt)
    wt[:, :count] = jnp.broadcast_to(weight, (wt.shape[0], count)).astype(jnp.bfloat16)
    scale[...] = jnp.broadcast_to(gain[...], (LANES, gain.shape[1])).T
    factor = scale[pl.ds(p * rows, rows), :][:, :1]
    ff = wp.shape[4] // 4
    part = rows // 2
    fetch[0].wait()
    fetch[1].wait()

    def pack(e, _):
        gate = raw_gate[e] * factor
        up = raw_up[e] * factor
        for j in range(2 * Q):
            span = slice(j * ff, (j + 1) * ff)
            quarters = [gate[:part, span], up[:part, span], gate[part:, span], up[part:, span]]
            wp[e, j // 2, j % 2] = jnp.concatenate(quarters, axis=1).astype(jnp.bfloat16)
        return 0

    lax.fori_loop(0, TP, pack, 0)
    fetch[2].wait()
    dn[...] = raw_down[...].astype(jnp.bfloat16)

    pl.semaphore_wait(barrier, FS - 1 + TP - 1 + 1)

    def cols(i):
        return pl.ds(pl.multiple_of(i * fb, LANES), fb)

    def dcols(i):
        return pl.ds(pl.multiple_of(i * db, LANES), db)

    def ring(i, fo, side):
        return remote(tok.at[fo, :, cols(x)], tok.at[fo, :, cols(x)], rs.at[side, i], rr.at[side, i], fs=zside[side])

    def ring_w(i, fo, side):
        return remote(wall.at[fo], wall.at[fo], ws.at[side, i], wr.at[side, i], fs=zside[side])

    for side in (0, 1):
        remote(nt.at[:, cols(x)], tok.at[f, :, cols(x)], rs.at[side, 0], rr.at[side, 0], fs=zside[side]).start()
        remote(wt, wall.at[f], ws.at[side, 0], wr.at[side, 0], fs=zside[side]).start()

    def spot(n):
        return (seat + n) % Q

    def xw(n, side):
        return remote(wp.at[xside[side], spot(n)], xr.at[x, spot(n)], xw_s.at[side, n], xw_r.at[side, n], tp=xside[side])

    def xw_recv(n, side):
        held = xr.at[xside[1 - side], spot(n)]
        return remote(held, held, xw_s.at[side, n], xw_r.at[side, n], tp=xside[side])

    def first_leg(n):
        return remote(wp.at[opposite, spot(n)], stage.at[n], st_s.at[n], st_r.at[n], tp=xside[n % 2])

    def second_leg(n):
        return remote(stage.at[n], xr.at[xside[1 - n % 2], spot(n)], sf_s.at[n], sf_r.at[n], tp=xside[n % 2])

    def second_leg_recv(n):
        return remote(stage.at[n], xr.at[opposite, spot(n)], sf_s.at[n], sf_r.at[n], tp=xside[n % 2])

    def xd(k):
        return remote(dn.at[(x + k) % TP], ds.at[p, :, dcols(x)], xd_s.at[k - 1], xd_r.at[k - 1], tp=(x + k) % TP)

    def xd_recv(k):
        held = ds.at[p, :, dcols((x + TP - k) % TP)]
        return remote(held, held, xd_s.at[k - 1], xd_r.at[k - 1], tp=(x + k) % TP)

    for n in range(Q):
        first_leg(n).start()
        for side in (0, 1):
            xw(n, side).start()
    own_cross = remote(nt, tok.at[f], cc_s.at[Z - 1], cc_r.at[Z - 1], fs=other)
    own_cross.start()
    own_cross_w = remote(wt, wall.at[f], cw_s.at[Z - 1], cw_r.at[Z - 1], fs=other)
    own_cross_w.start()
    local = [
        pltpu.make_async_copy(wp.at[x], xr.at[x], loc.at[0]),
        pltpu.make_async_copy(dn.at[x], ds.at[p, :, dcols(x)], loc.at[1]),
        pltpu.make_async_copy(nt, tok.at[f], loc.at[2]),
        pltpu.make_async_copy(wt, wall.at[f], loc.at[3]),
    ]
    for copy in local:
        copy.start()

    def across(i, fo, side):
        return remote(
            tok.at[fo, :, cols(x)], tok.at[fo, :, cols(x)], xt_s.at[side, i], xt_r.at[side, i], tp=xside[side]
        )

    def across_recv(i, fo, side):
        held = tok.at[fo, :, cols(xside[1 - side])]
        return remote(held, held, xt_s.at[side, i], xt_r.at[side, i], tp=xside[side])

    def from_left(s):
        return ((z + Z - s) % Z) * 2 + c

    def from_right(s):
        return ((z + s) % Z) * 2 + c

    def origin(i):
        s = i // 2 + 1
        return jnp.where(i % 2 == 0, from_left(s), from_right(s))

    def ring_step(s):
        for side in (0, 1):
            if s < H or side == 0:
                fo = from_left(s) if side == 0 else from_right(s)
                ring(s - 1, fo, side).wait_recv()
                ring_w(s - 1, fo, side).wait_recv()
                if s < H - side:
                    ring(s, fo, side).start()
                    ring_w(s, fo, side).start()
                for way in (0, 1):
                    across(2 * s - 2 + side, fo, way).start()

    turns = ((1, 3), (2, 0))

    def za(n, u, cd):
        zc = ((zone + u) % TP) * Q + spot(n)
        return remote(
            xr.at[zc // Q, spot(n), cd], gu.at[f, p], za_s.at[n * TP + u, cd], za_r.at[n * TP + u, c], fs=zc * 2 + cd
        )

    def source(n, u):
        return ((zone + TP - u) % TP) * Q + (seat + Q - n) % Q

    def za_recv(n, u, cs):
        held = gu.at[2 * source(n, u) + cs, p]
        return remote(held, held, za_s.at[n * TP + u, cs], za_r.at[n * TP + u, cs], fs=other)

    def y_hand(n, u):
        held = gu.at[pl.ds(2 * source(n, u), 2), p]
        return remote(held, held, y_s.at[n * TP + u], y_r.at[n * TP + u], grp=mate)

    def y_recv(n, u):
        held = gu.at[pl.ds(2 * source(n, u), 2), 1 - p]
        return remote(held, held, y_s.at[n * TP + u], y_r.at[n * TP + u], grp=mate)

    own = pltpu.make_async_copy(xr.at[zone, seat, c], gu.at[f, p], loc.at[4])

    def issue(b):
        n = b // 2
        if b % 2 == 0:
            for side in (0, 1):
                xw_recv(n, side).wait_recv()
            second_leg_recv(n).wait_recv()
        for u in turns[b % 2]:
            if n == 0 and u == 0:
                za(0, 0, 1 - c).start()
                own.start()
            else:
                za(n, u, 0).start()
                za(n, u, 1).start()

    def accept(b):
        n = b // 2
        for u in turns[b % 2]:
            if n == 0 and u == 0:
                own.wait()
                za_recv(0, 0, 1 - c).wait_recv()
            else:
                za_recv(n, u, 0).wait_recv()
                za_recv(n, u, 1).wait_recv()
            y_hand(n, u).start()

    def onward(i, fo, side):
        held = tok.at[fo, pl.ds(side * half, half), cols(xside[1 - side])]
        return remote(held, held, xo_s.at[side, i], xo_r.at[side, i], tp=xside[side])

    def onward_recv(i, fo, side):
        held = tok.at[fo, pl.ds(side * half, half), cols(opposite)]
        return remote(held, held, xo_s.at[side, i], xo_r.at[side, i], tp=xside[side])

    def cross(i, fo):
        return remote(tok.at[fo], tok.at[fo], cc_s.at[i], cc_r.at[i], fs=other)

    def cross_w(i, fo):
        return remote(wall.at[fo], wall.at[fo], cw_s.at[i], cw_r.at[i], fs=other)

    def cross_recv(i, fo):
        return remote(tok.at[fo + 1 - 2 * c], tok.at[fo + 1 - 2 * c], cc_s.at[i], cc_r.at[i], fs=other)

    def cross_w_recv(i, fo):
        return remote(wall.at[fo + 1 - 2 * c], wall.at[fo + 1 - 2 * c], cw_s.at[i], cw_r.at[i], fs=other)

    def pass_on(i):
        fo = origin(i)
        for side in (0, 1):
            across_recv(i, fo, side).wait_recv()
            onward(i, fo, side).start()

    def finish(i):
        fo = origin(i)
        for side in (0, 1):
            onward_recv(i, fo, side).wait_recv()
        cross(i, fo).start()
        cross_w(i, fo).start()

    yd = remote(ds.at[p], ds.at[p], yd_s, yd_r, grp=mate)
    ring_step(1)
    for n in (0, 1):
        first_leg(n).wait_recv()
        second_leg(n).start()
    for n in range(2, Q):
        first_leg(n).wait_recv()
        second_leg(n).start()
    for k in (2, 1, 3):
        xd(k).start()
    ring_step(2)
    local[0].wait()
    issue(0)
    for s in range(3, H + 1):
        ring_step(s)
        issue(s - 2)
        if s == H:
            issue(s - 1)
        for i in (2 * s - 6, 2 * s - 5):
            pass_on(i)
        if s == 4:
            local[1].wait()
            for k in (2, 1, 3):
                xd_recv(k).wait_recv()
            yd.start()
        if s > 3:
            for i in (2 * s - 8, 2 * s - 7):
                finish(i)
            accept(s - 4)
    pass_on(2 * H - 4)
    pass_on(2 * H - 3)
    finish(2 * H - 6)
    finish(2 * H - 5)
    accept(H - 3)
    pass_on(2 * H - 2)
    finish(2 * H - 4)
    finish(2 * H - 3)
    accept(H - 2)
    finish(2 * H - 2)
    accept(H - 1)

    local[2].wait()
    local[3].wait()
    own_fo = f + 1 - 2 * c
    remote(nt, tok.at[own_fo], cc_s.at[Z - 1], cc_r.at[Z - 1], fs=other).wait_recv()
    remote(wt, wall.at[own_fo], cw_s.at[Z - 1], cw_r.at[Z - 1], fs=other).wait_recv()
    own_cross.wait_send()
    own_cross_w.wait_send()

    def drain(i, _):
        fo = origin(i)
        for side in (0, 1):
            across(i, fo, side).wait_send()
            onward(i, fo, side).wait_send()
        cross(i, fo).wait_send()
        cross_w(i, fo).wait_send()
        cross_recv(i, fo).wait_recv()
        cross_w_recv(i, fo).wait_recv()
        return 0

    lax.fori_loop(0, Z - 1, drain, 0)

    def ring_drain(s, _):
        ring(s, f, 0).wait_send()
        ring_w(s, f, 0).wait_send()

        @pl.when(s < H - 1)
        def _():
            ring(s, f, 1).wait_send()
            ring_w(s, f, 1).wait_send()

        return 0

    lax.fori_loop(0, H, ring_drain, 0)
    za(0, 0, 1 - c).wait_send()
    y_hand(0, 0).wait_send()
    y_recv(0, 0).wait_recv()

    def exchange_drain(v, _):
        n, u = v // TP, v % TP
        za(n, u, 0).wait_send()
        za(n, u, 1).wait_send()
        y_hand(n, u).wait_send()
        y_recv(n, u).wait_recv()
        return 0

    lax.fori_loop(1, Z, exchange_drain, 0)
    yd.wait_send()
    remote(ds.at[1 - p], ds.at[1 - p], yd_s, yd_r, grp=mate).wait_recv()
    for n in range(Q):
        first_leg(n).wait_send()
        second_leg(n).wait_send()
        for side in (0, 1):
            xw(n, side).wait_send()
    for k in range(1, TP):
        xd(k).wait_send()


def run_hand_over(FS, TP, tokens, routes, logits, gain, w_gate, w_up, w_down):
    Z = FS // 2
    Q = Z // TP
    _, rows, ff = w_gate.shape
    ff = ff // (2 * Q)
    half = rows // 2
    drows, db = w_down.shape[1] // 2, w_down.shape[2]
    vmem = pl.BlockSpec(memory_space=pltpu.VMEM)
    hbm = pl.BlockSpec(memory_space=pl.ANY)
    tile = (16, LANES)
    piece = (half // 2, 4 * ff)
    bf16 = jnp.bfloat16
    return pl.pallas_call(
        functools.partial(hand_over, FS, TP),
        out_shape=(
            jax.ShapeDtypeStruct((FS, 2) + piece, bf16),
            jax.ShapeDtypeStruct((2, drows, TP * db), bf16),
            jax.ShapeDtypeStruct((FS,) + tokens.shape, bf16),
            jax.ShapeDtypeStruct((FS,) + tile, bf16),
        ),
        in_specs=[vmem] * 4 + [hbm] * 3,
        out_specs=(vmem,) * 4,
        scratch_shapes=[
            pltpu.VMEM((TP, half, w_gate.shape[2]), jnp.float32),
            pltpu.VMEM((TP, half, w_gate.shape[2]), jnp.float32),
            pltpu.VMEM((TP, drows, db), jnp.float32),
            pltpu.VMEM((rows, LANES), jnp.float32),
            pltpu.VMEM((TP, Q, 2) + piece, bf16),
            pltpu.VMEM((TP, drows, db), bf16),
            pltpu.VMEM(tokens.shape, bf16),
            pltpu.VMEM(tile, bf16),
            pltpu.VMEM((TP, Q, 2) + piece, bf16),
            pltpu.VMEM((Q, 2) + piece, bf16),
            DMA((3,)), DMA((5,)),
            DMA((2, Q)), DMA((2, Q)), DMA((Q,)), DMA((Q,)), DMA((Q,)), DMA((Q,)),
            DMA((TP - 1,)), DMA((TP - 1,)),
            DMA((2, Z // 2)), DMA((2, Z // 2)), DMA((2, Z // 2)), DMA((2, Z // 2)),
            DMA((2, Z - 1)), DMA((2, Z - 1)), DMA((2, Z - 1)), DMA((2, Z - 1)),
            DMA((Z,)), DMA((Z,)), DMA((Z,)), DMA((Z,)),
            DMA((Z, 2)), DMA((Z, 2)),
            DMA((Z,)), DMA((Z,)), DMA, DMA,
        ],
        compiler_params=pltpu.CompilerParams(collective_id=0, has_side_effects=True, vmem_limit_bytes=16 << 20),
        cost_estimate=pl.CostEstimate(flops=10**9, bytes_accessed=30 << 20, transcendentals=0),
        name="hand_over",
    )(tokens, routes, logits, gain, w_gate, w_up, w_down)


def expert(block, gu, x, w, ht, gate_out, up_out, wg, wu):
    features = x.shape[2]
    count = block // x.shape[1]
    part, ff = gu.shape[2], gu.shape[3] // 4
    pieces = block // (2 * part)

    def unpack(i, _):
        span = pl.ds(pl.multiple_of(i * block, block), block)
        for v in range(pieces):
            k = i * pieces + v
            piece = gu[k // 2, k % 2].astype(jnp.float32)
            for hh in (0, 1):
                at = pl.ds(pl.multiple_of(k * 2 * part + hh * part, part), part)
                wg[at, :] = piece[:, 2 * hh * ff : (2 * hh + 1) * ff].astype(jnp.bfloat16)
                wu[at, :] = piece[:, (2 * hh + 1) * ff : (2 * hh + 2) * ff].astype(jnp.bfloat16)
        for own, served in ((wg, gate_out), (wu, up_out)):
            served[:, span] = own[span, :].astype(jnp.float32).T.astype(jnp.bfloat16)
        return 0

    lax.fori_loop(0, features // block, unpack, 0)

    def step(i, _):
        span = pl.ds(pl.multiple_of(i * block, block), block)
        rows = x[pl.ds(i * count, count)].reshape(block, features)
        gate = jnp.dot(rows, wg[...], preferred_element_type=jnp.float32)
        up = jnp.dot(rows, wu[...], preferred_element_type=jnp.float32)
        scale = jnp.concatenate([w[i * count + n, 0:1, : x.shape[1]] for n in range(count)], axis=1)
        ht[:, span] = ((jax.nn.silu(gate) * up).T * scale.astype(jnp.float32)).astype(jnp.bfloat16)
        return 0

    lax.fori_loop(0, x.shape[0] // count, step, 0)


def run_expert(gu, x, w):
    tokens, features = x.shape[0] * x.shape[1], x.shape[2]
    ff = gu.shape[3] // 4
    vmem = pl.BlockSpec(memory_space=pltpu.VMEM)
    bf16 = jnp.bfloat16
    return pl.pallas_call(
        functools.partial(expert, 256),
        out_shape=(
            jax.ShapeDtypeStruct((ff, tokens), bf16),
            jax.ShapeDtypeStruct((ff, features), bf16),
            jax.ShapeDtypeStruct((ff, features), bf16),
        ),
        in_specs=[vmem] * 3,
        out_specs=(vmem,) * 3,
        scratch_shapes=[pltpu.VMEM((features, ff), bf16), pltpu.VMEM((features, ff), bf16)],
        compiler_params=pltpu.CompilerParams(vmem_limit_bytes=12 << 20),
        cost_estimate=pl.CostEstimate(flops=4 * 10**9, bytes_accessed=16 << 20, transcendentals=0),
        name="expert",
    )(gu, x, w)


def combine(FS, TP, W, L, ht, wd, out, wdt, hs, part, prec, zs, zr, outt, turned, loc, xd_s, xd_r, xo_s, xo_r, cc_s, cc_r, z_s, z_r, fin_s, fin_r):
    Z = FS // 2
    H = Z // 2
    x, f = lax.axis_index("tp"), lax.axis_index("fs")
    z, c = f // 2, f % 2
    other = f + 1 - 2 * c
    ff, block = hs.shape[2], hs.shape[3]
    half = ff // 2
    keep = part.shape[1] // 2
    xside = ((x + 1) % TP, (x + TP - 1) % TP)
    zside = (((z + 1) % Z) * 2 + c, ((z + Z - 1) % Z) * 2 + c)

    barrier = pltpu.get_barrier_semaphore()
    for k in xside:
        pl.semaphore_signal(barrier, inc=1, device_id={"tp": k}, device_id_type=MESH)
    for k in zside + (other,):
        pl.semaphore_signal(barrier, inc=1, device_id={"fs": k}, device_id_type=MESH)
    pl.semaphore_wait(barrier, 5)

    def away(i):
        return H - (i + 1) // 2

    def chip(i):
        return jnp.where(i % 2 == 0, (z + away(i)) % Z, (z + Z - away(i)) % Z)

    def mine(i):
        return ht.at[:, pl.ds(pl.multiple_of(chip(i) * block, LANES), block)]

    def keep_own(i):
        return pltpu.make_async_copy(mine(i), hs.at[i, x], loc.at[i])

    def direct(i, side):
        return remote(mine(i), hs.at[i, x], xd_s.at[side, i], xd_r.at[side, i], tp=xside[side])

    def onward(i, side):
        held = hs.at[i, xside[1 - side], pl.ds(side * half, half)]
        return remote(held, held, xo_s.at[side, i], xo_r.at[side, i], tp=xside[side])

    def cross(j):
        return remote(part.at[j, pl.ds((1 - c) * keep, keep)], prec.at[j], cc_s.at[j], cc_r.at[j], fs=other)

    def walk(m, side):
        k = away(m) - 1
        return remote(zs.at[m], zr.at[side, k], z_s.at[m], z_r.at[side, k], fs=zside[side])

    def arrival(side, k):
        return remote(zs.at[0], zr.at[side, k], z_s.at[0], z_r.at[side, k], fs=zside[side])

    def own_first(i, _):
        keep_own(i).start()
        return 0

    lax.fori_loop(0, Z, own_first, 0)
    for i in range(W):
        for side in (0, 1):
            direct(i, side).start()
    for e in range(TP):
        wdt[:, e * ff : (e + 1) * ff] = wd[e].T.astype(jnp.bfloat16)

    def step(i, _):
        @pl.when(i + W < Z)
        def _():
            for side in (0, 1):
                direct(i + W, side).start()

        @pl.when(i < Z)
        def _():
            for side in (0, 1):
                direct(i, side).wait_recv()
                onward(i, side).start()

        @pl.when((i >= L) & (i < Z + L))
        def _():
            j = i - L
            keep_own(j).wait()
            for side in (0, 1):
                onward(j, side).wait_recv()
            rhs = hs[j].reshape(TP * ff, block)
            part[j] = jnp.dot(wdt[...], rhs, preferred_element_type=jnp.float32)
            cross(j).start()

        @pl.when(i > L)
        def _():
            m = i - L - 1
            k = away(m)
            cross(m).wait_recv()
            total = part[m, pl.ds(c * keep, keep)] + prec[m]

            @pl.when(m == 0)
            def _():
                zs[m] = total.astype(jnp.bfloat16)

            @pl.when(m == 1)
            def _():
                zs[m] = total.astype(jnp.bfloat16)

            for side in (0, 1):
                @pl.when((m >= 2) & (m < Z - 1) & (m % 2 == side))
                def _():
                    arrival(side, k).wait_recv()
                    zs[m] = (total + zr[side, k].astype(jnp.float32)).astype(jnp.bfloat16)

                @pl.when((m < Z - 1) & (m % 2 == side))
                def _():
                    walk(m, side).start()

            @pl.when(m == Z - 1)
            def _():
                arrival(0, 0).wait_recv()
                arrival(1, 0).wait_recv()
                both = zr[0, 0].astype(jnp.float32) + zr[1, 0].astype(jnp.float32)
                outt[pl.ds(c * keep, keep)] = (total + both).astype(jnp.bfloat16)

        return 0

    lax.fori_loop(0, Z + L + 1, step, 0)
    last = remote(outt.at[pl.ds(c * keep, keep)], outt.at[pl.ds(c * keep, keep)], fin_s, fin_r, fs=other)
    last.start()

    def drain(i, _):
        for side in (0, 1):
            direct(i, side).wait_send()
            onward(i, side).wait_send()
        cross(i).wait_send()

        @pl.when(i < Z - 1)
        def _():
            arrival_of = remote(zs.at[i], zr.at[0, 0], z_s.at[i], z_r.at[0, 0], fs=other)
            arrival_of.wait_send()

        return 0

    lax.fori_loop(0, Z, drain, 0)
    last.wait()
    turned[...] = outt[...].astype(jnp.float32).T
    rows = block // 2
    out[...] = turned[pl.ds(c * rows, rows)].astype(jnp.bfloat16)


def run_combine(FS, TP, ht, wd):
    Z = FS // 2
    ff, tokens = ht.shape
    block = tokens // Z
    feats = wd.shape[2]
    vmem = pl.BlockSpec(memory_space=pltpu.VMEM)
    return pl.pallas_call(
        functools.partial(combine, FS, TP, 4, 2),
        out_shape=jax.ShapeDtypeStruct((block // 2, feats), jnp.bfloat16),
        in_specs=[vmem] * 2,
        out_specs=vmem,
        scratch_shapes=[
            pltpu.VMEM((feats, TP * ff), jnp.bfloat16),
            pltpu.VMEM((Z, TP, ff, block), jnp.bfloat16),
            pltpu.VMEM((Z, feats, block), jnp.float32),
            pltpu.VMEM((Z, feats // 2, block), jnp.float32),
            pltpu.VMEM((Z - 1, feats // 2, block), jnp.bfloat16),
            pltpu.VMEM((2, Z // 2, feats // 2, block), jnp.bfloat16),
            pltpu.VMEM((feats, block), jnp.bfloat16),
            pltpu.VMEM((block, feats), jnp.float32),
            DMA((Z,)), DMA((2, Z)), DMA((2, Z)), DMA((2, Z)), DMA((2, Z)),
            DMA((Z,)), DMA((Z,)), DMA((Z - 1,)), DMA((2, Z // 2)), DMA, DMA,
        ],
        compiler_params=pltpu.CompilerParams(collective_id=1, has_side_effects=True, vmem_limit_bytes=20 << 20),
        cost_estimate=pl.CostEstimate(flops=10**9, bytes_accessed=30 << 20, transcendentals=0),
        name="combine",
    )(ht, wd)


def body(FS, TP, tokens, routes, route_logits, gain, w_gate, w_up, w_down):
    gu, ds, tok, wall = run_hand_over(
        FS, TP, tokens, routes.T, route_logits.T, gain[None], w_gate, w_up, w_down
    )
    hidden, gate_t, up_t = run_expert(gu, tok, wall)
    mixed = run_combine(FS, TP, hidden, w_down)
    return (gate_t.T[None], up_t.T[None], ds.reshape(1, 2 * ds.shape[1], -1), mixed)


def solution(mesh):
    return jax.shard_map(
        functools.partial(body, mesh.shape["fs"], mesh.shape["tp"]),
        mesh=mesh,
        in_specs=(
            P(("grp", "fs"), None),
            P(("grp", "fs"), None),
            P(("grp", "fs"), None),
            P("fs"),
            P(None, "fs", "tp"),
            P(None, "fs", "tp"),
            P(None, "fs", "tp"),
        ),
        out_specs=(
            P(("grp", "tp"), None, "fs"),
            P(("grp", "tp"), None, "fs"),
            P(("grp", "tp"), "fs", None),
            P(("grp", "fs"), "tp"),
        ),
        check_vma=False,
    )
```

```python
import functools

import jax
import jax.numpy as jnp
from jax import lax
from jax.experimental import pallas as pl
from jax.experimental.pallas import tpu as pltpu
from jax.sharding import PartitionSpec as P

MESH = pl.DeviceIdType.MESH
DMA = pltpu.SemaphoreType.DMA
LANES = 128


def remote(src, dst, send, recv, **where):
    return pltpu.make_async_remote_copy(
        src_ref=src, dst_ref=dst, send_sem=send, recv_sem=recv, device_id=where, device_id_type=MESH
    )


def hand_over(
    FS, TP, x_hbm, routes_hbm, logits_hbm, gain_hbm, w_gate, w_up, w_down, gu, ds, tok, wall,
    x_in, routes, logits, gain, raw_gate, raw_up, raw_down, scale, wp, dn, nt, wt, xr, stage,
    in_s, loc, xw_s, xw_r, st_s, st_r, sf_s, sf_r, xd_s, xd_r, rs, rr, ws, wr, xt_s, xt_r, xo_s, xo_r,
    cc_s, cc_r, cw_s, cw_r, za_s, za_r, y_s, y_r, yd_s, yd_r,
):
    Z = FS // 2
    H = Z // 2
    Q = Z // TP
    assert TP == 4 and Q * TP == Z and H == 2 * Q
    x, f, g = lax.axis_index("tp"), lax.axis_index("fs"), lax.axis_index("grp")
    z, c = f // 2, f % 2
    zone, seat = z // Q, z % Q
    p = g % 2
    mate = g + 1 - 2 * p
    fb = nt.shape[1] // TP
    half = nt.shape[0] // 2
    db = dn.shape[2]
    rows = raw_gate.shape[1]
    drows = raw_down.shape[1]
    other = f + 1 - 2 * c
    xside = ((x + 1) % TP, (x + TP - 1) % TP)
    zside = (((z + 1) % Z) * 2 + c, ((z + Z - 1) % Z) * 2 + c)
    opposite = (x + 2) % TP

    fetch = (
        pltpu.make_async_copy(x_hbm, x_in, in_s.at[3]),
        pltpu.make_async_copy(routes_hbm, routes, in_s.at[4]),
        pltpu.make_async_copy(logits_hbm, logits, in_s.at[5]),
        pltpu.make_async_copy(gain_hbm, gain, in_s.at[6]),
        pltpu.make_async_copy(w_gate.at[:, pl.ds(p * rows, rows)], raw_gate, in_s.at[0]),
        pltpu.make_async_copy(w_up.at[:, pl.ds(p * rows, rows)], raw_up, in_s.at[1]),
        pltpu.make_async_copy(w_down.at[:, pl.ds(p * drows, drows)], raw_down, in_s.at[2]),
    )
    for copy in fetch:
        copy.start()

    barrier = pltpu.get_barrier_semaphore()

    def greet(r, _):
        pl.semaphore_signal(barrier, inc=1, device_id={"fs": (f + r) % FS}, device_id_type=MESH)
        return 0

    lax.fori_loop(1, FS, greet, 0)
    for k in range(1, TP):
        pl.semaphore_signal(barrier, inc=1, device_id={"tp": (x + k) % TP}, device_id_type=MESH)
    pl.semaphore_signal(barrier, inc=1, device_id={"grp": mate}, device_id_type=MESH)

    for copy in fetch[:4]:
        copy.wait()
    values = x_in[...].astype(jnp.float32)
    mean_square = jnp.mean(values * values, axis=-1, keepdims=True)
    nt[...] = (values * lax.rsqrt(mean_square + 1e-06)).astype(jnp.bfloat16)
    count = routes.shape[1]
    first = jax.nn.sigmoid(logits[0:1] - logits[1:2])
    second = jax.nn.sigmoid(logits[1:2] - logits[0:1])
    weight = first * (routes[0:1] == x).astype(jnp.float32) + second * (routes[1:2] == x).astype(jnp.float32)
    wt[...] = jnp.zeros_like(wt)
    wt[:, :count] = jnp.broadcast_to(weight, (wt.shape[0], count)).astype(jnp.bfloat16)
    scale[...] = jnp.broadcast_to(gain[...], (LANES, gain.shape[1])).T
    factor = scale[pl.ds(p * rows, rows), :][:, :1]
    ff = wp.shape[4] // 4
    part = rows // 2
    fetch[4].wait()
    fetch[5].wait()

    def pack(e):
        gate = raw_gate[e] * factor
        up = raw_up[e] * factor
        for j in range(2 * Q):
            span = slice(j * ff, (j + 1) * ff)
            quarters = [gate[:part, span], up[:part, span], gate[part:, span], up[part:, span]]
            wp[e, j // 2, j % 2] = jnp.concatenate(quarters, axis=1).astype(jnp.bfloat16)

    pack(opposite)
    pl.semaphore_wait(barrier, FS - 1 + TP - 1 + 1)

    def cols(i):
        return pl.ds(pl.multiple_of(i * fb, LANES), fb)

    def dcols(i):
        return pl.ds(pl.multiple_of(i * db, LANES), db)

    def ring(i, fo, side):
        return remote(tok.at[fo, :, cols(x)], tok.at[fo, :, cols(x)], rs.at[side, i], rr.at[side, i], fs=zside[side])

    def ring_w(i, fo, side):
        return remote(wall.at[fo], wall.at[fo], ws.at[side, i], wr.at[side, i], fs=zside[side])

    for side in (0, 1):
        remote(nt.at[:, cols(x)], tok.at[f, :, cols(x)], rs.at[side, 0], rr.at[side, 0], fs=zside[side]).start()
        remote(wt, wall.at[f], ws.at[side, 0], wr.at[side, 0], fs=zside[side]).start()

    def spot(n):
        return (seat + n) % Q

    def xw(n, side):
        return remote(wp.at[xside[side], spot(n)], xr.at[x, spot(n)], xw_s.at[side, n], xw_r.at[side, n], tp=xside[side])

    def xw_recv(n, side):
        held = xr.at[xside[1 - side], spot(n)]
        return remote(held, held, xw_s.at[side, n], xw_r.at[side, n], tp=xside[side])

    def first_leg(n):
        return remote(wp.at[opposite, spot(n)], stage.at[n], st_s.at[n], st_r.at[n], tp=xside[n % 2])

    def second_leg(n):
        return remote(stage.at[n], xr.at[xside[1 - n % 2], spot(n)], sf_s.at[n], sf_r.at[n], tp=xside[n % 2])

    def second_leg_recv(n):
        return remote(stage.at[n], xr.at[opposite, spot(n)], sf_s.at[n], sf_r.at[n], tp=xside[n % 2])

    def xd(k):
        return remote(dn.at[(x + k) % TP], ds.at[p, :, dcols(x)], xd_s.at[k - 1], xd_r.at[k - 1], tp=(x + k) % TP)

    def xd_recv(k):
        held = ds.at[p, :, dcols((x + TP - k) % TP)]
        return remote(held, held, xd_s.at[k - 1], xd_r.at[k - 1], tp=(x + k) % TP)

    def send_packed(k, _):
        @pl.when(k == 0)
        def _():
            first_leg(0).start()
            first_leg(1).start()

        e = jnp.where(k < 2, jnp.where(k == 0, xside[0], xside[1]), x)
        pack(e)

        @pl.when(k == 0)
        def _():
            for n in range(Q):
                xw(n, 0).start()

        @pl.when(k == 1)
        def _():
            for n in range(Q):
                xw(n, 1).start()
            for n in range(2, Q):
                first_leg(n).start()

        return 0

    lax.fori_loop(0, 3, send_packed, 0)
    fetch[6].wait()
    dn[...] = raw_down[...].astype(jnp.bfloat16)
    own_cross = remote(nt, tok.at[f], cc_s.at[Z - 1], cc_r.at[Z - 1], fs=other)
    own_cross.start()
    own_cross_w = remote(wt, wall.at[f], cw_s.at[Z - 1], cw_r.at[Z - 1], fs=other)
    own_cross_w.start()
    local = [
        pltpu.make_async_copy(wp.at[x], xr.at[x], loc.at[0]),
        pltpu.make_async_copy(dn.at[x], ds.at[p, :, dcols(x)], loc.at[1]),
        pltpu.make_async_copy(nt, tok.at[f], loc.at[2]),
        pltpu.make_async_copy(wt, wall.at[f], loc.at[3]),
    ]
    for copy in local:
        copy.start()

    def across(i, fo, side):
        return remote(
            tok.at[fo, :, cols(x)], tok.at[fo, :, cols(x)], xt_s.at[side, i], xt_r.at[side, i], tp=xside[side]
        )

    def across_recv(i, fo, side):
        held = tok.at[fo, :, cols(xside[1 - side])]
        return remote(held, held, xt_s.at[side, i], xt_r.at[side, i], tp=xside[side])

    def from_left(s):
        return ((z + Z - s) % Z) * 2 + c

    def from_right(s):
        return ((z + s) % Z) * 2 + c

    def origin(i):
        s = i // 2 + 1
        return jnp.where(i % 2 == 0, from_left(s), from_right(s))

    def ring_step(s):
        for side in (0, 1):
            if s < H or side == 0:
                fo = from_left(s) if side == 0 else from_right(s)
                ring(s - 1, fo, side).wait_recv()
                ring_w(s - 1, fo, side).wait_recv()
                if s < H - side:
                    ring(s, fo, side).start()
                    ring_w(s, fo, side).start()
                for way in (0, 1):
                    across(2 * s - 2 + side, fo, way).start()

    turns = ((1, 3), (2, 0))

    def za(n, u, cd):
        zc = ((zone + u) % TP) * Q + spot(n)
        return remote(
            xr.at[zc // Q, spot(n), cd], gu.at[f, p], za_s.at[n * TP + u, cd], za_r.at[n * TP + u, c], fs=zc * 2 + cd
        )

    def source(n, u):
        return ((zone + TP - u) % TP) * Q + (seat + Q - n) % Q

    def za_recv(n, u, cs):
        held = gu.at[2 * source(n, u) + cs, p]
        return remote(held, held, za_s.at[n * TP + u, cs], za_r.at[n * TP + u, cs], fs=other)

    def y_hand(n, u):
        held = gu.at[pl.ds(2 * source(n, u), 2), p]
        return remote(held, held, y_s.at[n * TP + u], y_r.at[n * TP + u], grp=mate)

    def y_recv(n, u):
        held = gu.at[pl.ds(2 * source(n, u), 2), 1 - p]
        return remote(held, held, y_s.at[n * TP + u], y_r.at[n * TP + u], grp=mate)

    own = pltpu.make_async_copy(xr.at[zone, seat, c], gu.at[f, p], loc.at[4])

    def issue(b):
        n = b // 2
        if b % 2 == 0:
            for side in (0, 1):
                xw_recv(n, side).wait_recv()
            second_leg_recv(n).wait_recv()
        for u in turns[b % 2]:
            if n == 0 and u == 0:
                za(0, 0, 1 - c).start()
                own.start()
            else:
                za(n, u, 0).start()
                za(n, u, 1).start()

    def accept(b):
        n = b // 2
        for u in turns[b % 2]:
            if n == 0 and u == 0:
                own.wait()
                za_recv(0, 0, 1 - c).wait_recv()
            else:
                za_recv(n, u, 0).wait_recv()
                za_recv(n, u, 1).wait_recv()
            y_hand(n, u).start()

    def onward(i, fo, side):
        held = tok.at[fo, pl.ds(side * half, half), cols(xside[1 - side])]
        return remote(held, held, xo_s.at[side, i], xo_r.at[side, i], tp=xside[side])

    def onward_recv(i, fo, side):
        held = tok.at[fo, pl.ds(side * half, half), cols(opposite)]
        return remote(held, held, xo_s.at[side, i], xo_r.at[side, i], tp=xside[side])

    def cross(i, fo):
        return remote(tok.at[fo], tok.at[fo], cc_s.at[i], cc_r.at[i], fs=other)

    def cross_w(i, fo):
        return remote(wall.at[fo], wall.at[fo], cw_s.at[i], cw_r.at[i], fs=other)

    def cross_recv(i, fo):
        return remote(tok.at[fo + 1 - 2 * c], tok.at[fo + 1 - 2 * c], cc_s.at[i], cc_r.at[i], fs=other)

    def cross_w_recv(i, fo):
        return remote(wall.at[fo + 1 - 2 * c], wall.at[fo + 1 - 2 * c], cw_s.at[i], cw_r.at[i], fs=other)

    def pass_on(i):
        fo = origin(i)
        for side in (0, 1):
            across_recv(i, fo, side).wait_recv()
            onward(i, fo, side).start()

    def finish(i):
        fo = origin(i)
        for side in (0, 1):
            onward_recv(i, fo, side).wait_recv()
        cross(i, fo).start()
        cross_w(i, fo).start()

    yd = remote(ds.at[p], ds.at[p], yd_s, yd_r, grp=mate)
    ring_step(1)
    for n in (0, 1):
        first_leg(n).wait_recv()
        second_leg(n).start()
    for n in range(2, Q):
        first_leg(n).wait_recv()
        second_leg(n).start()
    for k in (2, 1, 3):
        xd(k).start()
    ring_step(2)
    local[0].wait()
    issue(0)
    for s in range(3, H + 1):
        ring_step(s)
        issue(s - 2)
        if s == H:
            issue(s - 1)
        for i in (2 * s - 6, 2 * s - 5):
            pass_on(i)
        if s == 4:
            local[1].wait()
            for k in (2, 1, 3):
                xd_recv(k).wait_recv()
            yd.start()
        if s > 3:
            for i in (2 * s - 8, 2 * s - 7):
                finish(i)
            accept(s - 4)
    pass_on(2 * H - 4)
    pass_on(2 * H - 3)
    finish(2 * H - 6)
    finish(2 * H - 5)
    accept(H - 3)
    pass_on(2 * H - 2)
    finish(2 * H - 4)
    finish(2 * H - 3)
    accept(H - 2)
    finish(2 * H - 2)
    accept(H - 1)

    local[2].wait()
    local[3].wait()
    own_fo = f + 1 - 2 * c
    remote(nt, tok.at[own_fo], cc_s.at[Z - 1], cc_r.at[Z - 1], fs=other).wait_recv()
    remote(wt, wall.at[own_fo], cw_s.at[Z - 1], cw_r.at[Z - 1], fs=other).wait_recv()
    own_cross.wait_send()
    own_cross_w.wait_send()

    def drain(i, _):
        fo = origin(i)
        for side in (0, 1):
            across(i, fo, side).wait_send()
            onward(i, fo, side).wait_send()
        cross(i, fo).wait_send()
        cross_w(i, fo).wait_send()
        cross_recv(i, fo).wait_recv()
        cross_w_recv(i, fo).wait_recv()
        return 0

    lax.fori_loop(0, Z - 1, drain, 0)

    def ring_drain(s, _):
        ring(s, f, 0).wait_send()
        ring_w(s, f, 0).wait_send()

        @pl.when(s < H - 1)
        def _():
            ring(s, f, 1).wait_send()
            ring_w(s, f, 1).wait_send()

        return 0

    lax.fori_loop(0, H, ring_drain, 0)
    za(0, 0, 1 - c).wait_send()
    y_hand(0, 0).wait_send()
    y_recv(0, 0).wait_recv()

    def exchange_drain(v, _):
        n, u = v // TP, v % TP
        za(n, u, 0).wait_send()
        za(n, u, 1).wait_send()
        y_hand(n, u).wait_send()
        y_recv(n, u).wait_recv()
        return 0

    lax.fori_loop(1, Z, exchange_drain, 0)
    yd.wait_send()
    remote(ds.at[1 - p], ds.at[1 - p], yd_s, yd_r, grp=mate).wait_recv()
    for n in range(Q):
        first_leg(n).wait_send()
        second_leg(n).wait_send()
        for side in (0, 1):
            xw(n, side).wait_send()
    for k in range(1, TP):
        xd(k).wait_send()


def run_hand_over(FS, TP, tokens, routes, logits, gain, w_gate, w_up, w_down):
    Z = FS // 2
    Q = Z // TP
    _, rows, ff = w_gate.shape
    ff = ff // (2 * Q)
    half = rows // 2
    drows, db = w_down.shape[1] // 2, w_down.shape[2]
    vmem = pl.BlockSpec(memory_space=pltpu.VMEM)
    hbm = pl.BlockSpec(memory_space=pltpu.HBM)
    tile = (16, LANES)
    piece = (half // 2, 4 * ff)
    bf16 = jnp.bfloat16
    return pl.pallas_call(
        functools.partial(hand_over, FS, TP),
        out_shape=(
            jax.ShapeDtypeStruct((FS, 2) + piece, bf16),
            jax.ShapeDtypeStruct((2, drows, TP * db), bf16),
            jax.ShapeDtypeStruct((FS,) + tokens.shape, bf16),
            jax.ShapeDtypeStruct((FS,) + tile, bf16),
        ),
        in_specs=[hbm] * 7,
        out_specs=(vmem,) * 4,
        scratch_shapes=[
            pltpu.VMEM(tokens.shape, tokens.dtype),
            pltpu.VMEM(routes.shape, routes.dtype),
            pltpu.VMEM(logits.shape, logits.dtype),
            pltpu.VMEM(gain.shape, gain.dtype),
            pltpu.VMEM((TP, half, w_gate.shape[2]), jnp.float32),
            pltpu.VMEM((TP, half, w_gate.shape[2]), jnp.float32),
            pltpu.VMEM((TP, drows, db), jnp.float32),
            pltpu.VMEM((rows, LANES), jnp.float32),
            pltpu.VMEM((TP, Q, 2) + piece, bf16),
            pltpu.VMEM((TP, drows, db), bf16),
            pltpu.VMEM(tokens.shape, bf16),
            pltpu.VMEM(tile, bf16),
            pltpu.VMEM((TP, Q, 2) + piece, bf16),
            pltpu.VMEM((Q, 2) + piece, bf16),
            DMA((7,)), DMA((5,)),
            DMA((2, Q)), DMA((2, Q)), DMA((Q,)), DMA((Q,)), DMA((Q,)), DMA((Q,)),
            DMA((TP - 1,)), DMA((TP - 1,)),
            DMA((2, Z // 2)), DMA((2, Z // 2)), DMA((2, Z // 2)), DMA((2, Z // 2)),
            DMA((2, Z - 1)), DMA((2, Z - 1)), DMA((2, Z - 1)), DMA((2, Z - 1)),
            DMA((Z,)), DMA((Z,)), DMA((Z,)), DMA((Z,)),
            DMA((Z, 2)), DMA((Z, 2)),
            DMA((Z,)), DMA((Z,)), DMA, DMA,
        ],
        compiler_params=pltpu.CompilerParams(collective_id=0, has_side_effects=True, vmem_limit_bytes=16 << 20),
        cost_estimate=pl.CostEstimate(flops=10**9, bytes_accessed=30 << 20, transcendentals=0),
        name="hand_over",
    )(*[
        pltpu.with_memory_space_constraint(a, pltpu.HBM)
        for a in (tokens, routes, logits, gain, w_gate, w_up, w_down)
    ])


def unpack(block, gu, wg, wu, gate_out, up_out):
    part, ff = gu.shape[2], gu.shape[3] // 4
    pieces = block // (2 * part)

    def step(i, _):
        span = pl.ds(pl.multiple_of(i * block, block), block)
        for v in range(pieces):
            k = i * pieces + v
            piece = gu[k // 2, k % 2].astype(jnp.float32)
            for hh in (0, 1):
                at = pl.ds(pl.multiple_of(k * 2 * part + hh * part, part), part)
                wg[at, :] = piece[:, 2 * hh * ff : (2 * hh + 1) * ff].astype(jnp.bfloat16)
                wu[at, :] = piece[:, (2 * hh + 1) * ff : (2 * hh + 2) * ff].astype(jnp.bfloat16)
        for own, served in ((wg, gate_out), (wu, up_out)):
            served[:, span] = own[span, :].astype(jnp.float32).T.astype(jnp.bfloat16)
        return 0

    lax.fori_loop(0, wg.shape[0] // block, step, 0)


def run_unpack(gu):
    ff = gu.shape[3] // 4
    features = gu.shape[0] * gu.shape[1] * gu.shape[2] * 2
    vmem = pl.BlockSpec(memory_space=pltpu.VMEM)
    bf16 = jnp.bfloat16
    return pl.pallas_call(
        functools.partial(unpack, 256),
        out_shape=(
            jax.ShapeDtypeStruct((features, ff), bf16),
            jax.ShapeDtypeStruct((features, ff), bf16),
            jax.ShapeDtypeStruct((ff, features), bf16),
            jax.ShapeDtypeStruct((ff, features), bf16),
        ),
        in_specs=[vmem],
        out_specs=(vmem,) * 4,
        compiler_params=pltpu.CompilerParams(vmem_limit_bytes=8 << 20),
        cost_estimate=pl.CostEstimate(flops=10**9, bytes_accessed=16 << 20, transcendentals=0),
        name="unpack",
    )(gu)


def combine(FS, TP, L, wg, wu, tok, wall, wd, out, wdt, hs, part, prec, zs, zr, outt, turned, xd_s, xd_r, xo_s, xo_r, cc_s, cc_r, z_s, z_r, fin_s, fin_r):
    Z = FS // 2
    H = Z // 2
    x, f = lax.axis_index("tp"), lax.axis_index("fs")
    z, c = f // 2, f % 2
    other = f + 1 - 2 * c
    ff, block = hs.shape[2], hs.shape[3]
    half = ff // 2
    keep = part.shape[1] // 2
    xside = ((x + 1) % TP, (x + TP - 1) % TP)
    zside = (((z + 1) % Z) * 2 + c, ((z + Z - 1) % Z) * 2 + c)

    barrier = pltpu.get_barrier_semaphore()
    for k in xside:
        pl.semaphore_signal(barrier, inc=1, device_id={"tp": k}, device_id_type=MESH)
    for k in zside + (other,):
        pl.semaphore_signal(barrier, inc=1, device_id={"fs": k}, device_id_type=MESH)

    def away(i):
        return H - (i + 1) // 2

    def chip(i):
        return jnp.where(i % 2 == 0, (z + away(i)) % Z, (z + Z - away(i)) % Z)

    count, features = tok.shape[1], tok.shape[2]

    def make(i):
        rows = jnp.concatenate([tok[pl.ds(2 * chip(i + v), 2)].reshape(block, features) for v in (0, 1)], axis=0)
        gate = jnp.dot(rows, wg[...], preferred_element_type=jnp.float32)
        up = jnp.dot(rows, wu[...], preferred_element_type=jnp.float32)
        hidden = (jax.nn.silu(gate) * up).T
        for v in (0, 1):
            scale = [wall[2 * chip(i + v) + n, 0:1, :count] for n in (0, 1)]
            scale = jnp.concatenate(scale, axis=1).astype(jnp.float32)
            hs[i + v, x] = (hidden[:, v * block : (v + 1) * block] * scale).astype(jnp.bfloat16)

    def direct(i, side):
        return remote(hs.at[i, x], hs.at[i, x], xd_s.at[side, i], xd_r.at[side, i], tp=xside[side])

    def direct_recv(i, side):
        held = hs.at[i, xside[1 - side]]
        return remote(held, held, xd_s.at[side, i], xd_r.at[side, i], tp=xside[side])

    def onward(i, side):
        held = hs.at[i, xside[1 - side], pl.ds(side * half, half)]
        return remote(held, held, xo_s.at[side, i], xo_r.at[side, i], tp=xside[side])

    def onward_recv(i, side):
        held = hs.at[i, (x + 2) % TP, pl.ds(side * half, half)]
        return remote(held, held, xo_s.at[side, i], xo_r.at[side, i], tp=xside[side])

    def cross(j):
        return remote(part.at[j, pl.ds((1 - c) * keep, keep)], prec.at[j], cc_s.at[j], cc_r.at[j], fs=other)

    def walk(m, side):
        k = away(m) - 1
        return remote(zs.at[m], zr.at[side, k], z_s.at[m], z_r.at[side, k], fs=zside[side])

    def arrival(side, k):
        return remote(zs.at[0], zr.at[side, k], z_s.at[0], z_r.at[side, k], fs=zside[side])

    AHEAD = 4

    def begin(k, _):
        make(2 * k)

        @pl.when(k == 0)
        def _():
            pl.semaphore_wait(barrier, 5)

        @pl.when(2 * k < AHEAD)
        def _():
            for v in (0, 1):
                for side in (0, 1):
                    direct(2 * k + v, side).start()

        return 0

    lax.fori_loop(0, AHEAD // 2 + 1, begin, 0)
    for e in range(TP):
        wdt[:, e * ff : (e + 1) * ff] = wd[e].T.astype(jnp.bfloat16)

    def step(i, _):
        @pl.when(i + AHEAD < Z)
        def _():
            for side in (0, 1):
                direct(i + AHEAD, side).start()

        @pl.when(i < Z)
        def _():
            for side in (0, 1):
                direct_recv(i, side).wait_recv()
                onward(i, side).start()

        @pl.when((i % 2 == 0) & (i + AHEAD + 2 < Z))
        def _():
            make(i + AHEAD + 2)

        @pl.when((i >= L) & (i < Z + L))
        def _():
            j = i - L
            for side in (0, 1):
                onward_recv(j, side).wait_recv()
            rhs = hs[j].reshape(TP * ff, block)
            part[j] = jnp.dot(wdt[...], rhs, preferred_element_type=jnp.float32)
            cross(j).start()

        @pl.when(i > L)
        def _():
            m = i - L - 1
            k = away(m)
            cross(m).wait_recv()
            total = part[m, pl.ds(c * keep, keep)] + prec[m]

            @pl.when(m == 0)
            def _():
                zs[m] = total.astype(jnp.bfloat16)

            @pl.when(m == 1)
            def _():
                zs[m] = total.astype(jnp.bfloat16)

            for side in (0, 1):
                @pl.when((m >= 2) & (m < Z - 1) & (m % 2 == side))
                def _():
                    arrival(side, k).wait_recv()
                    zs[m] = (total + zr[side, k].astype(jnp.float32)).astype(jnp.bfloat16)

                @pl.when((m < Z - 1) & (m % 2 == side))
                def _():
                    walk(m, side).start()

            @pl.when(m == Z - 1)
            def _():
                arrival(0, 0).wait_recv()
                arrival(1, 0).wait_recv()
                both = zr[0, 0].astype(jnp.float32) + zr[1, 0].astype(jnp.float32)
                outt[pl.ds(c * keep, keep)] = (total + both).astype(jnp.bfloat16)

        return 0

    lax.fori_loop(0, Z + L + 1, step, 0)
    last = remote(outt.at[pl.ds(c * keep, keep)], outt.at[pl.ds(c * keep, keep)], fin_s, fin_r, fs=other)
    last.start()

    def drain(i, _):
        for side in (0, 1):
            direct(i, side).wait_send()
            onward(i, side).wait_send()
        cross(i).wait_send()

        @pl.when(i < Z - 1)
        def _():
            arrival_of = remote(zs.at[i], zr.at[0, 0], z_s.at[i], z_r.at[0, 0], fs=other)
            arrival_of.wait_send()

        return 0

    lax.fori_loop(0, Z, drain, 0)
    last.wait()
    turned[...] = outt[...].astype(jnp.float32).T
    rows = block // 2
    out[...] = turned[pl.ds(c * rows, rows)].astype(jnp.bfloat16)


def run_combine(FS, TP, wg, wu, tok, wall, wd):
    Z = FS // 2
    ff = wg.shape[1]
    block = 2 * tok.shape[1]
    feats = wd.shape[2]
    vmem = pl.BlockSpec(memory_space=pltpu.VMEM)
    return pl.pallas_call(
        functools.partial(combine, FS, TP, 2),
        out_shape=jax.ShapeDtypeStruct((block // 2, feats), jnp.bfloat16),
        in_specs=[vmem] * 5,
        out_specs=vmem,
        scratch_shapes=[
            pltpu.VMEM((feats, TP * ff), jnp.bfloat16),
            pltpu.VMEM((Z, TP, ff, block), jnp.bfloat16),
            pltpu.VMEM((Z, feats, block), jnp.float32),
            pltpu.VMEM((Z, feats // 2, block), jnp.float32),
            pltpu.VMEM((Z - 1, feats // 2, block), jnp.bfloat16),
            pltpu.VMEM((2, Z // 2, feats // 2, block), jnp.bfloat16),
            pltpu.VMEM((feats, block), jnp.bfloat16),
            pltpu.VMEM((block, feats), jnp.float32),
            DMA((2, Z)), DMA((2, Z)), DMA((2, Z)), DMA((2, Z)),
            DMA((Z,)), DMA((Z,)), DMA((Z - 1,)), DMA((2, Z // 2)), DMA, DMA,
        ],
        compiler_params=pltpu.CompilerParams(collective_id=1, has_side_effects=True, vmem_limit_bytes=20 << 20),
        cost_estimate=pl.CostEstimate(flops=10**9, bytes_accessed=30 << 20, transcendentals=0),
        name="combine",
    )(wg, wu, tok, wall, wd)


def body(FS, TP, tokens, routes, route_logits, gain, w_gate, w_up, w_down):
    gu, ds, tok, wall = run_hand_over(
        FS, TP, tokens, routes.T, route_logits.T, gain[None], w_gate, w_up, w_down
    )
    wg, wu, gate_t, up_t = run_unpack(gu)
    mixed = run_combine(FS, TP, wg, wu, tok, wall, w_down)
    return (gate_t.T[None], up_t.T[None], ds.reshape(1, 2 * ds.shape[1], -1), mixed)


def solution(mesh):
    return jax.shard_map(
        functools.partial(body, mesh.shape["fs"], mesh.shape["tp"]),
        mesh=mesh,
        in_specs=(
            P(("grp", "fs"), None),
            P(("grp", "fs"), None),
            P(("grp", "fs"), None),
            P("fs"),
            P(None, "fs", "tp"),
            P(None, "fs", "tp"),
            P(None, "fs", "tp"),
        ),
        out_specs=(
            P(("grp", "tp"), None, "fs"),
            P(("grp", "tp"), None, "fs"),
            P(("grp", "tp"), "fs", None),
            P(("grp", "fs"), "tp"),
        ),
        check_vma=False,
    )
```

```python
import functools

import jax
import jax.numpy as jnp
from jax import lax
from jax.experimental import pallas as pl
from jax.experimental.pallas import tpu as pltpu
from jax.sharding import PartitionSpec as P

MESH = pl.DeviceIdType.MESH
DMA = pltpu.SemaphoreType.DMA
LANES = 128


def remote(src, dst, send, recv, **where):
    return pltpu.make_async_remote_copy(
        src_ref=src, dst_ref=dst, send_sem=send, recv_sem=recv, device_id=where, device_id_type=MESH
    )


def hand_over(
    FS, TP, x_hbm, routes_hbm, logits_hbm, gain_hbm, w_gate, w_up, w_down, gu, ds, tok, wall,
    x_in, routes, logits, gain, raw_gate, raw_up, raw_down, scale, wp, dn, nt, wt, xr, stage, relay,
    in_s, loc, xw_s, xw_r, st_s, st_r, sf_s, sf_r, xd_s, xd_r, rs, rr, ws, wr, xt_s, xt_r, xo_s, xo_r,
    cc_s, cc_r, cw_s, cw_r, za_s, za_r, ra_s, ra_r, rb_s, y_s, y_r, yd_s, yd_r,
):
    Z = FS // 2
    H = Z // 2
    Q = Z // TP
    assert TP == 4 and Q * TP == Z and H == 2 * Q
    x, f, g = lax.axis_index("tp"), lax.axis_index("fs"), lax.axis_index("grp")
    z, c = f // 2, f % 2
    zone, seat = z // Q, z % Q
    p = g % 2
    mate = g + 1 - 2 * p
    fb = nt.shape[1] // TP
    half = nt.shape[0] // 2
    db = dn.shape[2]
    rows = raw_gate.shape[1]
    drows = raw_down.shape[1]
    other = f + 1 - 2 * c
    xside = ((x + 1) % TP, (x + TP - 1) % TP)
    zside = (((z + 1) % Z) * 2 + c, ((z + Z - 1) % Z) * 2 + c)
    opposite = (x + 2) % TP

    fetch = (
        pltpu.make_async_copy(x_hbm, x_in, in_s.at[3]),
        pltpu.make_async_copy(routes_hbm, routes, in_s.at[4]),
        pltpu.make_async_copy(logits_hbm, logits, in_s.at[5]),
        pltpu.make_async_copy(gain_hbm, gain, in_s.at[6]),
        pltpu.make_async_copy(w_gate.at[:, pl.ds(p * rows, rows)], raw_gate, in_s.at[0]),
        pltpu.make_async_copy(w_up.at[:, pl.ds(p * rows, rows)], raw_up, in_s.at[1]),
        pltpu.make_async_copy(w_down.at[:, pl.ds(p * drows, drows)], raw_down, in_s.at[2]),
    )
    for copy in fetch:
        copy.start()

    barrier = pltpu.get_barrier_semaphore()

    def greet(r, _):
        pl.semaphore_signal(barrier, inc=1, device_id={"fs": (f + r) % FS}, device_id_type=MESH)
        return 0

    lax.fori_loop(1, FS, greet, 0)
    for k in range(1, TP):
        pl.semaphore_signal(barrier, inc=1, device_id={"tp": (x + k) % TP}, device_id_type=MESH)
    pl.semaphore_signal(barrier, inc=1, device_id={"grp": mate}, device_id_type=MESH)

    for copy in fetch[:4]:
        copy.wait()
    values = x_in[...].astype(jnp.float32)
    mean_square = jnp.mean(values * values, axis=-1, keepdims=True)
    nt[...] = (values * lax.rsqrt(mean_square + 1e-06)).astype(jnp.bfloat16)
    count = routes.shape[1]
    first = jax.nn.sigmoid(logits[0:1] - logits[1:2])
    second = jax.nn.sigmoid(logits[1:2] - logits[0:1])
    weight = first * (routes[0:1] == x).astype(jnp.float32) + second * (routes[1:2] == x).astype(jnp.float32)
    wt[...] = jnp.zeros_like(wt)
    wt[:, :count] = jnp.broadcast_to(weight, (wt.shape[0], count)).astype(jnp.bfloat16)
    scale[...] = jnp.broadcast_to(gain[...], (LANES, gain.shape[1])).T
    factor = scale[pl.ds(p * rows, rows), :][:, :1]
    ff = wp.shape[4] // 4
    part = rows // 2
    fetch[4].wait()
    fetch[5].wait()

    def pack(e):
        gate = raw_gate[e] * factor
        up = raw_up[e] * factor
        for j in range(2 * Q):
            span = slice(j * ff, (j + 1) * ff)
            quarters = [gate[:part, span], up[:part, span], gate[part:, span], up[part:, span]]
            wp[e, j // 2, j % 2] = jnp.concatenate(quarters, axis=1).astype(jnp.bfloat16)

    pack(opposite)
    pl.semaphore_wait(barrier, FS - 1 + TP - 1 + 1)

    def cols(i):
        return pl.ds(pl.multiple_of(i * fb, LANES), fb)

    def dcols(i):
        return pl.ds(pl.multiple_of(i * db, LANES), db)

    def ring(i, fo, side):
        return remote(tok.at[fo, :, cols(x)], tok.at[fo, :, cols(x)], rs.at[side, i], rr.at[side, i], fs=zside[side])

    def ring_w(i, fo, side):
        return remote(wall.at[fo], wall.at[fo], ws.at[side, i], wr.at[side, i], fs=zside[side])

    for side in (0, 1):
        remote(nt.at[:, cols(x)], tok.at[f, :, cols(x)], rs.at[side, 0], rr.at[side, 0], fs=zside[side]).start()
        remote(wt, wall.at[f], ws.at[side, 0], wr.at[side, 0], fs=zside[side]).start()

    def spot(n):
        return (seat + n) % Q

    def xw(n, side):
        return remote(wp.at[xside[side], spot(n)], xr.at[x, spot(n)], xw_s.at[side, n], xw_r.at[side, n], tp=xside[side])

    def xw_recv(n, side):
        held = xr.at[xside[1 - side], spot(n)]
        return remote(held, held, xw_s.at[side, n], xw_r.at[side, n], tp=xside[side])

    def first_leg(n):
        return remote(wp.at[opposite, spot(n)], stage.at[n], st_s.at[n], st_r.at[n], tp=xside[n % 2])

    def second_leg(n):
        return remote(stage.at[n], xr.at[xside[1 - n % 2], spot(n)], sf_s.at[n], sf_r.at[n], tp=xside[n % 2])

    def second_leg_recv(n):
        return remote(stage.at[n], xr.at[opposite, spot(n)], sf_s.at[n], sf_r.at[n], tp=xside[n % 2])

    def xd(k):
        return remote(dn.at[(x + k) % TP], ds.at[p, :, dcols(x)], xd_s.at[k - 1], xd_r.at[k - 1], tp=(x + k) % TP)

    def xd_recv(k):
        held = ds.at[p, :, dcols((x + TP - k) % TP)]
        return remote(held, held, xd_s.at[k - 1], xd_r.at[k - 1], tp=(x + k) % TP)

    def send_packed(k, _):
        @pl.when(k == 0)
        def _():
            first_leg(0).start()
            first_leg(1).start()

        e = jnp.where(k < 2, jnp.where(k == 0, xside[0], xside[1]), x)
        pack(e)

        @pl.when(k == 0)
        def _():
            for n in range(Q):
                xw(n, 0).start()

        @pl.when(k == 1)
        def _():
            for n in range(Q):
                xw(n, 1).start()
            for n in range(2, Q):
                first_leg(n).start()

        return 0

    lax.fori_loop(0, 3, send_packed, 0)
    fetch[6].wait()
    dn[...] = raw_down[...].astype(jnp.bfloat16)
    own_cross = remote(nt, tok.at[f], cc_s.at[Z - 1], cc_r.at[Z - 1], fs=other)
    own_cross.start()
    own_cross_w = remote(wt, wall.at[f], cw_s.at[Z - 1], cw_r.at[Z - 1], fs=other)
    own_cross_w.start()
    local = [
        pltpu.make_async_copy(wp.at[x], xr.at[x], loc.at[0]),
        pltpu.make_async_copy(dn.at[x], ds.at[p, :, dcols(x)], loc.at[1]),
        pltpu.make_async_copy(nt, tok.at[f], loc.at[2]),
        pltpu.make_async_copy(wt, wall.at[f], loc.at[3]),
    ]
    for copy in local:
        copy.start()

    def across(i, fo, side):
        return remote(
            tok.at[fo, :, cols(x)], tok.at[fo, :, cols(x)], xt_s.at[side, i], xt_r.at[side, i], tp=xside[side]
        )

    def across_recv(i, fo, side):
        held = tok.at[fo, :, cols(xside[1 - side])]
        return remote(held, held, xt_s.at[side, i], xt_r.at[side, i], tp=xside[side])

    def from_left(s):
        return ((z + Z - s) % Z) * 2 + c

    def from_right(s):
        return ((z + s) % Z) * 2 + c

    def origin(i):
        s = i // 2 + 1
        return jnp.where(i % 2 == 0, from_left(s), from_right(s))

    def ring_step(s):
        for side in (0, 1):
            if s < H or side == 0:
                fo = from_left(s) if side == 0 else from_right(s)
                ring(s - 1, fo, side).wait_recv()
                ring_w(s - 1, fo, side).wait_recv()
                if s < H - side:
                    ring(s, fo, side).start()
                    ring_w(s, fo, side).start()
                for way in (0, 1):
                    across(2 * s - 2 + side, fo, way).start()

    turns = ((1, 3), (2, 0))

    def za(n, u, cd):
        zc = ((zone + u) % TP) * Q + spot(n)
        return remote(
            xr.at[zc // Q, spot(n), cd], gu.at[f, p], za_s.at[n * TP + u, cd], za_r.at[n * TP + u, c], fs=zc * 2 + cd
        )

    def source(n, u):
        return ((zone + TP - u) % TP) * Q + (seat + Q - n) % Q

    def za_recv(n, u, cs):
        held = gu.at[2 * source(n, u) + cs, p]
        return remote(held, held, za_s.at[n * TP + u, cs], za_r.at[n * TP + u, cs], fs=other)

    def half_way(side):
        return (z + Q) % Z if side == 0 else (z + Z - Q) % Z

    def relay_out(side):
        zc = (z + H) % Z
        piece = xr.at[zc // Q, seat, side]
        return remote(piece, relay.at[side], ra_s.at[side], ra_r.at[side], fs=half_way(side) * 2 + c)

    def relay_on(side):
        fo = half_way(1 - side) * 2 + c
        return remote(relay.at[side], gu.at[fo, p], rb_s.at[side], za_r.at[2, c], fs=half_way(side) * 2 + side)

    def y_hand(n, u):
        held = gu.at[pl.ds(2 * source(n, u), 2), p]
        return remote(held, held, y_s.at[n * TP + u], y_r.at[n * TP + u], grp=mate)

    def y_recv(n, u):
        held = gu.at[pl.ds(2 * source(n, u), 2), 1 - p]
        return remote(held, held, y_s.at[n * TP + u], y_r.at[n * TP + u], grp=mate)

    own = pltpu.make_async_copy(xr.at[zone, seat, c], gu.at[f, p], loc.at[4])

    def issue(b):
        n = b // 2
        if b % 2 == 0:
            for side in (0, 1):
                xw_recv(n, side).wait_recv()
            second_leg_recv(n).wait_recv()
        for u in turns[b % 2]:
            if n == 0 and u == 0:
                za(0, 0, 1 - c).start()
                own.start()
            elif n == 0 and u == 2:
                relay_out(0).start()
                relay_out(1).start()
            else:
                za(n, u, 0).start()
                za(n, u, 1).start()

    def accept(b):
        n = b // 2
        for u in turns[b % 2]:
            if n == 0 and u == 0:
                own.wait()
                za_recv(0, 0, 1 - c).wait_recv()
            else:
                za_recv(n, u, 0).wait_recv()
                za_recv(n, u, 1).wait_recv()
            y_hand(n, u).start()

    def onward(i, fo, side):
        held = tok.at[fo, pl.ds(side * half, half), cols(xside[1 - side])]
        return remote(held, held, xo_s.at[side, i], xo_r.at[side, i], tp=xside[side])

    def onward_recv(i, fo, side):
        held = tok.at[fo, pl.ds(side * half, half), cols(opposite)]
        return remote(held, held, xo_s.at[side, i], xo_r.at[side, i], tp=xside[side])

    def cross(i, fo):
        return remote(tok.at[fo], tok.at[fo], cc_s.at[i], cc_r.at[i], fs=other)

    def cross_w(i, fo):
        return remote(wall.at[fo], wall.at[fo], cw_s.at[i], cw_r.at[i], fs=other)

    def cross_recv(i, fo):
        return remote(tok.at[fo + 1 - 2 * c], tok.at[fo + 1 - 2 * c], cc_s.at[i], cc_r.at[i], fs=other)

    def cross_w_recv(i, fo):
        return remote(wall.at[fo + 1 - 2 * c], wall.at[fo + 1 - 2 * c], cw_s.at[i], cw_r.at[i], fs=other)

    def pass_on(i):
        fo = origin(i)
        for side in (0, 1):
            across_recv(i, fo, side).wait_recv()
            onward(i, fo, side).start()

    def finish(i):
        fo = origin(i)
        for side in (0, 1):
            onward_recv(i, fo, side).wait_recv()
        cross(i, fo).start()
        cross_w(i, fo).start()

    yd = remote(ds.at[p], ds.at[p], yd_s, yd_r, grp=mate)
    ring_step(1)
    for n in (0, 1):
        first_leg(n).wait_recv()
        second_leg(n).start()
    for n in range(2, Q):
        first_leg(n).wait_recv()
        second_leg(n).start()
    for k in (2, 1, 3):
        xd(k).start()
    local[0].wait()
    issue(0)
    for s in range(2, H + 1):
        ring_step(s)
        issue(s - 1)
        if s == 3:
            for side in (0, 1):
                relay_out(side).wait_recv()
                relay_on(side).start()
        if s > 2:
            for i in (2 * s - 6, 2 * s - 5):
                pass_on(i)
        if s == 4:
            local[1].wait()
            for k in (2, 1, 3):
                xd_recv(k).wait_recv()
            yd.start()
        if s > 3:
            for i in (2 * s - 8, 2 * s - 7):
                finish(i)
        if s > 2:
            accept(s - 3)
    pass_on(2 * H - 4)
    pass_on(2 * H - 3)
    finish(2 * H - 6)
    finish(2 * H - 5)
    accept(H - 2)
    pass_on(2 * H - 2)
    finish(2 * H - 4)
    finish(2 * H - 3)
    accept(H - 1)
    finish(2 * H - 2)

    local[2].wait()
    local[3].wait()
    own_fo = f + 1 - 2 * c
    remote(nt, tok.at[own_fo], cc_s.at[Z - 1], cc_r.at[Z - 1], fs=other).wait_recv()
    remote(wt, wall.at[own_fo], cw_s.at[Z - 1], cw_r.at[Z - 1], fs=other).wait_recv()
    own_cross.wait_send()
    own_cross_w.wait_send()

    def drain(i, _):
        fo = origin(i)
        for side in (0, 1):
            across(i, fo, side).wait_send()
            onward(i, fo, side).wait_send()
        cross(i, fo).wait_send()
        cross_w(i, fo).wait_send()
        cross_recv(i, fo).wait_recv()
        cross_w_recv(i, fo).wait_recv()
        return 0

    lax.fori_loop(0, Z - 1, drain, 0)

    def ring_drain(s, _):
        ring(s, f, 0).wait_send()
        ring_w(s, f, 0).wait_send()

        @pl.when(s < H - 1)
        def _():
            ring(s, f, 1).wait_send()
            ring_w(s, f, 1).wait_send()

        return 0

    lax.fori_loop(0, H, ring_drain, 0)
    za(0, 0, 1 - c).wait_send()
    y_hand(0, 0).wait_send()
    y_recv(0, 0).wait_recv()

    def exchange_drain(v, _):
        n, u = v // TP, v % TP
        @pl.when(v != 2)
        def _():
            za(n, u, 0).wait_send()
            za(n, u, 1).wait_send()

        y_hand(n, u).wait_send()
        y_recv(n, u).wait_recv()
        return 0

    lax.fori_loop(1, Z, exchange_drain, 0)
    for side in (0, 1):
        relay_out(side).wait_send()
        relay_on(side).wait_send()
    yd.wait_send()
    remote(ds.at[1 - p], ds.at[1 - p], yd_s, yd_r, grp=mate).wait_recv()
    for n in range(Q):
        first_leg(n).wait_send()
        second_leg(n).wait_send()
        for side in (0, 1):
            xw(n, side).wait_send()
    for k in range(1, TP):
        xd(k).wait_send()


def run_hand_over(FS, TP, tokens, routes, logits, gain, w_gate, w_up, w_down):
    Z = FS // 2
    Q = Z // TP
    _, rows, ff = w_gate.shape
    ff = ff // (2 * Q)
    half = rows // 2
    drows, db = w_down.shape[1] // 2, w_down.shape[2]
    vmem = pl.BlockSpec(memory_space=pltpu.VMEM)
    hbm = pl.BlockSpec(memory_space=pltpu.HBM)
    tile = (16, LANES)
    piece = (half // 2, 4 * ff)
    bf16 = jnp.bfloat16
    return pl.pallas_call(
        functools.partial(hand_over, FS, TP),
        out_shape=(
            jax.ShapeDtypeStruct((FS, 2) + piece, bf16),
            jax.ShapeDtypeStruct((2, drows, TP * db), bf16),
            jax.ShapeDtypeStruct((FS,) + tokens.shape, bf16),
            jax.ShapeDtypeStruct((FS,) + tile, bf16),
        ),
        in_specs=[hbm] * 7,
        out_specs=(vmem,) * 4,
        scratch_shapes=[
            pltpu.VMEM(tokens.shape, tokens.dtype),
            pltpu.VMEM(routes.shape, routes.dtype),
            pltpu.VMEM(logits.shape, logits.dtype),
            pltpu.VMEM(gain.shape, gain.dtype),
            pltpu.VMEM((TP, half, w_gate.shape[2]), jnp.float32),
            pltpu.VMEM((TP, half, w_gate.shape[2]), jnp.float32),
            pltpu.VMEM((TP, drows, db), jnp.float32),
            pltpu.VMEM((rows, LANES), jnp.float32),
            pltpu.VMEM((TP, Q, 2) + piece, bf16),
            pltpu.VMEM((TP, drows, db), bf16),
            pltpu.VMEM(tokens.shape, bf16),
            pltpu.VMEM(tile, bf16),
            pltpu.VMEM((TP, Q, 2) + piece, bf16),
            pltpu.VMEM((Q, 2) + piece, bf16),
            pltpu.VMEM((2,) + piece, bf16),
            DMA((7,)), DMA((5,)),
            DMA((2, Q)), DMA((2, Q)), DMA((Q,)), DMA((Q,)), DMA((Q,)), DMA((Q,)),
            DMA((TP - 1,)), DMA((TP - 1,)),
            DMA((2, Z // 2)), DMA((2, Z // 2)), DMA((2, Z // 2)), DMA((2, Z // 2)),
            DMA((2, Z - 1)), DMA((2, Z - 1)), DMA((2, Z - 1)), DMA((2, Z - 1)),
            DMA((Z,)), DMA((Z,)), DMA((Z,)), DMA((Z,)),
            DMA((Z, 2)), DMA((Z, 2)), DMA((2,)), DMA((2,)), DMA((2,)),
            DMA((Z,)), DMA((Z,)), DMA, DMA,
        ],
        compiler_params=pltpu.CompilerParams(collective_id=0, has_side_effects=True, vmem_limit_bytes=16 << 20),
        cost_estimate=pl.CostEstimate(flops=10**9, bytes_accessed=30 << 20, transcendentals=0),
        name="hand_over",
    )(*[
        pltpu.with_memory_space_constraint(a, pltpu.HBM)
        for a in (tokens, routes, logits, gain, w_gate, w_up, w_down)
    ])


def unpack(block, gu, ds, wg, wu, gate_out, up_out, down_out, sem):
    down = pltpu.make_async_copy(ds, down_out, sem)
    down.start()
    part, ff = gu.shape[2], gu.shape[3] // 4
    pieces = block // (2 * part)

    def step(i, _):
        span = pl.ds(pl.multiple_of(i * block, block), block)
        for v in range(pieces):
            k = i * pieces + v
            piece = gu[k // 2, k % 2].astype(jnp.float32)
            for hh in (0, 1):
                at = pl.ds(pl.multiple_of(k * 2 * part + hh * part, part), part)
                wg[at, :] = piece[:, 2 * hh * ff : (2 * hh + 1) * ff].astype(jnp.bfloat16)
                wu[at, :] = piece[:, (2 * hh + 1) * ff : (2 * hh + 2) * ff].astype(jnp.bfloat16)
        for own, served in ((wg, gate_out), (wu, up_out)):
            served[:, span] = own[span, :].astype(jnp.float32).T.astype(jnp.bfloat16)
        return 0

    lax.fori_loop(0, wg.shape[0] // block, step, 0)
    down.wait()


def run_unpack(gu, ds):
    ff = gu.shape[3] // 4
    features = gu.shape[0] * gu.shape[1] * gu.shape[2] * 2
    vmem = pl.BlockSpec(memory_space=pltpu.VMEM)
    bf16 = jnp.bfloat16
    return pl.pallas_call(
        functools.partial(unpack, 256),
        out_shape=(
            jax.ShapeDtypeStruct((features, ff), bf16),
            jax.ShapeDtypeStruct((features, ff), bf16),
            jax.ShapeDtypeStruct((ff, features), bf16),
            jax.ShapeDtypeStruct((ff, features), bf16),
            jax.ShapeDtypeStruct(ds.shape, bf16),
        ),
        in_specs=[vmem] * 2,
        out_specs=(vmem,) * 4 + (pl.BlockSpec(memory_space=pltpu.HBM),),
        scratch_shapes=[DMA],
        compiler_params=pltpu.CompilerParams(vmem_limit_bytes=8 << 20),
        cost_estimate=pl.CostEstimate(flops=10**9, bytes_accessed=16 << 20, transcendentals=0),
        name="unpack",
    )(gu, ds)


def combine(FS, TP, L, wg, wu, tok, wall, wd, out, wdt, hs, part, prec, zs, zr, outt, turned, xd_s, xd_r, xo_s, xo_r, cc_s, cc_r, z_s, z_r, fin_s, fin_r):
    Z = FS // 2
    H = Z // 2
    x, f = lax.axis_index("tp"), lax.axis_index("fs")
    z, c = f // 2, f % 2
    other = f + 1 - 2 * c
    ff, block = hs.shape[2], hs.shape[3]
    half = ff // 2
    keep = part.shape[1] // 2
    xside = ((x + 1) % TP, (x + TP - 1) % TP)
    zside = (((z + 1) % Z) * 2 + c, ((z + Z - 1) % Z) * 2 + c)

    barrier = pltpu.get_barrier_semaphore()
    for k in xside:
        pl.semaphore_signal(barrier, inc=1, device_id={"tp": k}, device_id_type=MESH)
    for k in zside + (other,):
        pl.semaphore_signal(barrier, inc=1, device_id={"fs": k}, device_id_type=MESH)

    def away(i):
        return H - (i + 1) // 2

    def chip(i):
        return jnp.where(i % 2 == 0, (z + away(i)) % Z, (z + Z - away(i)) % Z)

    count, features = tok.shape[1], tok.shape[2]

    def make(i):
        rows = jnp.concatenate([tok[pl.ds(2 * chip(i + v), 2)].reshape(block, features) for v in (0, 1)], axis=0)
        gate = jnp.dot(rows, wg[...], preferred_element_type=jnp.float32)
        up = jnp.dot(rows, wu[...], preferred_element_type=jnp.float32)
        hidden = (jax.nn.silu(gate) * up).T
        for v in (0, 1):
            scale = [wall[2 * chip(i + v) + n, 0:1, :count] for n in (0, 1)]
            scale = jnp.concatenate(scale, axis=1).astype(jnp.float32)
            hs[i + v, x] = (hidden[:, v * block : (v + 1) * block] * scale).astype(jnp.bfloat16)

    def direct(i, side):
        return remote(hs.at[i, x], hs.at[i, x], xd_s.at[side, i], xd_r.at[side, i], tp=xside[side])

    def direct_recv(i, side):
        held = hs.at[i, xside[1 - side]]
        return remote(held, held, xd_s.at[side, i], xd_r.at[side, i], tp=xside[side])

    def onward(i, side):
        held = hs.at[i, xside[1 - side], pl.ds(side * half, half)]
        return remote(held, held, xo_s.at[side, i], xo_r.at[side, i], tp=xside[side])

    def onward_recv(i, side):
        held = hs.at[i, (x + 2) % TP, pl.ds(side * half, half)]
        return remote(held, held, xo_s.at[side, i], xo_r.at[side, i], tp=xside[side])

    def cross(j):
        return remote(part.at[j, pl.ds((1 - c) * keep, keep)], prec.at[j], cc_s.at[j], cc_r.at[j], fs=other)

    def walk(m, side):
        k = away(m) - 1
        return remote(zs.at[m], zr.at[side, k], z_s.at[m], z_r.at[side, k], fs=zside[side])

    def arrival(side, k):
        return remote(zs.at[0], zr.at[side, k], z_s.at[0], z_r.at[side, k], fs=zside[side])

    AHEAD = 2

    def begin(k, _):
        make(2 * k)

        @pl.when(k == 0)
        def _():
            pl.semaphore_wait(barrier, 5)

        @pl.when(2 * k < AHEAD)
        def _():
            for v in (0, 1):
                for side in (0, 1):
                    direct(2 * k + v, side).start()

        return 0

    lax.fori_loop(0, AHEAD // 2 + 1, begin, 0)
    for e in range(TP):
        wdt[:, e * ff : (e + 1) * ff] = wd[e].T.astype(jnp.bfloat16)

    def step(i, _):
        @pl.when(i + AHEAD < Z)
        def _():
            for side in (0, 1):
                direct(i + AHEAD, side).start()

        @pl.when(i < Z)
        def _():
            for side in (0, 1):
                direct_recv(i, side).wait_recv()
                onward(i, side).start()

        @pl.when((i % 2 == 0) & (i + AHEAD + 2 < Z))
        def _():
            make(i + AHEAD + 2)

        @pl.when((i >= L) & (i < Z + L))
        def _():
            j = i - L
            for side in (0, 1):
                onward_recv(j, side).wait_recv()
            rhs = hs[j].reshape(TP * ff, block)
            part[j] = jnp.dot(wdt[...], rhs, preferred_element_type=jnp.float32)
            cross(j).start()

        @pl.when(i > L)
        def _():
            m = i - L - 1
            k = away(m)
            cross(m).wait_recv()
            total = part[m, pl.ds(c * keep, keep)] + prec[m]

            @pl.when(m == 0)
            def _():
                zs[m] = total.astype(jnp.bfloat16)

            @pl.when(m == 1)
            def _():
                zs[m] = total.astype(jnp.bfloat16)

            for side in (0, 1):
                @pl.when((m >= 2) & (m < Z - 1) & (m % 2 == side))
                def _():
                    arrival(side, k).wait_recv()
                    zs[m] = (total + zr[side, k].astype(jnp.float32)).astype(jnp.bfloat16)

                @pl.when((m < Z - 1) & (m % 2 == side))
                def _():
                    walk(m, side).start()

            @pl.when(m == Z - 1)
            def _():
                arrival(0, 0).wait_recv()
                arrival(1, 0).wait_recv()
                both = zr[0, 0].astype(jnp.float32) + zr[1, 0].astype(jnp.float32)
                outt[pl.ds(c * keep, keep)] = (total + both).astype(jnp.bfloat16)

        return 0

    lax.fori_loop(0, Z + L + 1, step, 0)
    last = remote(outt.at[pl.ds(c * keep, keep)], outt.at[pl.ds(c * keep, keep)], fin_s, fin_r, fs=other)
    last.start()

    def drain(i, _):
        for side in (0, 1):
            direct(i, side).wait_send()
            onward(i, side).wait_send()
        cross(i).wait_send()

        @pl.when(i < Z - 1)
        def _():
            arrival_of = remote(zs.at[i], zr.at[0, 0], z_s.at[i], z_r.at[0, 0], fs=other)
            arrival_of.wait_send()

        return 0

    lax.fori_loop(0, Z, drain, 0)
    last.wait()
    turned[...] = outt[...].astype(jnp.float32).T
    rows = block // 2
    out[...] = turned[pl.ds(c * rows, rows)].astype(jnp.bfloat16)


def run_combine(FS, TP, wg, wu, tok, wall, wd):
    Z = FS // 2
    ff = wg.shape[1]
    block = 2 * tok.shape[1]
    feats = wd.shape[2]
    vmem = pl.BlockSpec(memory_space=pltpu.VMEM)
    return pl.pallas_call(
        functools.partial(combine, FS, TP, 2),
        out_shape=jax.ShapeDtypeStruct((block // 2, feats), jnp.bfloat16),
        in_specs=[vmem] * 5,
        out_specs=vmem,
        scratch_shapes=[
            pltpu.VMEM((feats, TP * ff), jnp.bfloat16),
            pltpu.VMEM((Z, TP, ff, block), jnp.bfloat16),
            pltpu.VMEM((Z, feats, block), jnp.float32),
            pltpu.VMEM((Z, feats // 2, block), jnp.float32),
            pltpu.VMEM((Z - 1, feats // 2, block), jnp.bfloat16),
            pltpu.VMEM((2, Z // 2, feats // 2, block), jnp.bfloat16),
            pltpu.VMEM((feats, block), jnp.bfloat16),
            pltpu.VMEM((block, feats), jnp.float32),
            DMA((2, Z)), DMA((2, Z)), DMA((2, Z)), DMA((2, Z)),
            DMA((Z,)), DMA((Z,)), DMA((Z - 1,)), DMA((2, Z // 2)), DMA, DMA,
        ],
        compiler_params=pltpu.CompilerParams(collective_id=1, has_side_effects=True, vmem_limit_bytes=20 << 20),
        cost_estimate=pl.CostEstimate(flops=10**9, bytes_accessed=30 << 20, transcendentals=0),
        name="combine",
    )(wg, wu, tok, wall, wd)


def body(FS, TP, tokens, routes, route_logits, gain, w_gate, w_up, w_down):
    gu, ds, tok, wall = run_hand_over(
        FS, TP, tokens, routes.T, route_logits.T, gain[None], w_gate, w_up, w_down
    )
    wg, wu, gate_t, up_t, down = run_unpack(gu, ds)
    mixed = run_combine(FS, TP, wg, wu, tok, wall, w_down)
    return (gate_t.T[None], up_t.T[None], down.reshape(1, 2 * ds.shape[1], -1), mixed)


def solution(mesh):
    return jax.shard_map(
        functools.partial(body, mesh.shape["fs"], mesh.shape["tp"]),
        mesh=mesh,
        in_specs=(
            P(("grp", "fs"), None),
            P(("grp", "fs"), None),
            P(("grp", "fs"), None),
            P("fs"),
            P(None, "fs", "tp"),
            P(None, "fs", "tp"),
            P(None, "fs", "tp"),
        ),
        out_specs=(
            P(("grp", "tp"), None, "fs"),
            P(("grp", "tp"), None, "fs"),
            P(("grp", "tp"), "fs", None),
            P(("grp", "fs"), "tp"),
        ),
        check_vma=False,
    )
```

```python
import functools

import jax
import jax.numpy as jnp
from jax import lax
from jax.experimental import pallas as pl
from jax.experimental.pallas import tpu as pltpu
from jax.sharding import PartitionSpec as P

MESH = pl.DeviceIdType.MESH
DMA = pltpu.SemaphoreType.DMA
LANES = 128


def remote(src, dst, send, recv, **where):
    return pltpu.make_async_remote_copy(
        src_ref=src, dst_ref=dst, send_sem=send, recv_sem=recv, device_id=where, device_id_type=MESH
    )


def hand_over(
    FS, TP, x_hbm, routes_hbm, logits_hbm, gain_hbm, w_gate, w_up, w_down, gu, ds, tok, wall,
    x_in, routes, logits, gain, raw_gate, raw_up, raw_down, scale, wp, dn, nt, wt, xr, stage,
    in_s, loc, xw_s, xw_r, st_s, st_r, sf_s, sf_r, xd_s, xd_r, rs, rr, ws, wr, xt_s, xt_r, xo_s, xo_r,
    cc_s, cc_r, cw_s, cw_r, za_s, za_r, y_s, y_r, yd_s, yd_r,
):
    Z = FS // 2
    H = Z // 2
    Q = Z // TP
    assert TP == 4 and Q == 4 and Q * TP == Z
    x, f, g = lax.axis_index("tp"), lax.axis_index("fs"), lax.axis_index("grp")
    z, c = f // 2, f % 2
    zone, seat = z // Q, z % Q
    order = (0, 2, 1, 3)
    p = g % 2
    mate = g + 1 - 2 * p
    fb = nt.shape[1] // TP
    half = nt.shape[0] // 2
    db = dn.shape[2]
    rows = raw_gate.shape[1]
    drows = raw_down.shape[1]
    other = f + 1 - 2 * c
    xside = ((x + 1) % TP, (x + TP - 1) % TP)
    zside = (((z + 1) % Z) * 2 + c, ((z + Z - 1) % Z) * 2 + c)
    opposite = (x + 2) % TP

    fetch = (
        pltpu.make_async_copy(x_hbm, x_in, in_s.at[3]),
        pltpu.make_async_copy(routes_hbm, routes, in_s.at[4]),
        pltpu.make_async_copy(logits_hbm, logits, in_s.at[5]),
        pltpu.make_async_copy(gain_hbm, gain, in_s.at[6]),
        pltpu.make_async_copy(w_gate.at[:, pl.ds(p * rows, rows)], raw_gate, in_s.at[0]),
        pltpu.make_async_copy(w_up.at[:, pl.ds(p * rows, rows)], raw_up, in_s.at[1]),
        pltpu.make_async_copy(w_down.at[:, pl.ds(p * drows, drows)], raw_down, in_s.at[2]),
    )
    for copy in fetch:
        copy.start()

    barrier = pltpu.get_barrier_semaphore()

    def greet(r, _):
        pl.semaphore_signal(barrier, inc=1, device_id={"fs": (f + r) % FS}, device_id_type=MESH)
        return 0

    lax.fori_loop(1, FS, greet, 0)
    for k in range(1, TP):
        pl.semaphore_signal(barrier, inc=1, device_id={"tp": (x + k) % TP}, device_id_type=MESH)
    pl.semaphore_signal(barrier, inc=1, device_id={"grp": mate}, device_id_type=MESH)

    for copy in fetch[:4]:
        copy.wait()
    values = x_in[...].astype(jnp.float32)
    mean_square = jnp.mean(values * values, axis=-1, keepdims=True)
    nt[...] = (values * lax.rsqrt(mean_square + 1e-06)).astype(jnp.bfloat16)
    count = routes.shape[1]
    first = jax.nn.sigmoid(logits[0:1] - logits[1:2])
    second = jax.nn.sigmoid(logits[1:2] - logits[0:1])
    weight = first * (routes[0:1] == x).astype(jnp.float32) + second * (routes[1:2] == x).astype(jnp.float32)
    wt[...] = jnp.zeros_like(wt)
    wt[:, :count] = jnp.broadcast_to(weight, (wt.shape[0], count)).astype(jnp.bfloat16)
    scale[...] = jnp.broadcast_to(gain[...], (LANES, gain.shape[1])).T
    factor = scale[pl.ds(p * rows, rows), :][:, :1]
    ff = wp.shape[4] // 4
    part = rows // 2
    fetch[4].wait()
    fetch[5].wait()

    def pack(e):
        gate = raw_gate[e] * factor
        up = raw_up[e] * factor
        for j in range(2 * Q):
            span = slice(j * ff, (j + 1) * ff)
            quarters = [gate[:part, span], up[:part, span], gate[part:, span], up[part:, span]]
            wp[e, j // 2, j % 2] = jnp.concatenate(quarters, axis=1).astype(jnp.bfloat16)

    pack(opposite)
    pl.semaphore_wait(barrier, FS - 1 + TP - 1 + 1)

    def cols(i):
        return pl.ds(pl.multiple_of(i * fb, LANES), fb)

    def dcols(i):
        return pl.ds(pl.multiple_of(i * db, LANES), db)

    def ring(i, fo, side):
        return remote(tok.at[fo, :, cols(x)], tok.at[fo, :, cols(x)], rs.at[side, i], rr.at[side, i], fs=zside[side])

    def ring_w(i, fo, side):
        return remote(wall.at[fo], wall.at[fo], ws.at[side, i], wr.at[side, i], fs=zside[side])

    for side in (0, 1):
        remote(nt.at[:, cols(x)], tok.at[f, :, cols(x)], rs.at[side, 0], rr.at[side, 0], fs=zside[side]).start()
        remote(wt, wall.at[f], ws.at[side, 0], wr.at[side, 0], fs=zside[side]).start()

    def spot(n):
        return (seat + n) % Q

    def leg(n):
        return n // 2

    def xw(n, side):
        return remote(wp.at[xside[side], spot(n)], xr.at[x, spot(n)], xw_s.at[side, n], xw_r.at[side, n], tp=xside[side])

    def xw_recv(n, side):
        held = xr.at[xside[1 - side], spot(n)]
        return remote(held, held, xw_s.at[side, n], xw_r.at[side, n], tp=xside[side])

    def first_leg(n):
        return remote(wp.at[opposite, spot(n)], stage.at[n], st_s.at[n], st_r.at[n], tp=xside[leg(n)])

    def second_leg(n):
        return remote(stage.at[n], xr.at[xside[1 - leg(n)], spot(n)], sf_s.at[n], sf_r.at[n], tp=xside[leg(n)])

    def second_leg_recv(n):
        return remote(stage.at[n], xr.at[opposite, spot(n)], sf_s.at[n], sf_r.at[n], tp=xside[leg(n)])

    def xd(k):
        return remote(dn.at[(x + k) % TP], ds.at[p, :, dcols(x)], xd_s.at[k - 1], xd_r.at[k - 1], tp=(x + k) % TP)

    def xd_recv(k):
        held = ds.at[p, :, dcols((x + TP - k) % TP)]
        return remote(held, held, xd_s.at[k - 1], xd_r.at[k - 1], tp=(x + k) % TP)

    def send_packed(k, _):
        @pl.when(k == 0)
        def _():
            for n in order[:2]:
                first_leg(n).start()

        e = jnp.where(k < 2, jnp.where(k == 0, xside[0], xside[1]), x)
        pack(e)

        @pl.when(k == 0)
        def _():
            for n in order:
                xw(n, 0).start()

        @pl.when(k == 1)
        def _():
            for n in order:
                xw(n, 1).start()
            for n in order[2:]:
                first_leg(n).start()

        return 0

    lax.fori_loop(0, 3, send_packed, 0)
    fetch[6].wait()
    dn[...] = raw_down[...].astype(jnp.bfloat16)
    own_cross = remote(nt, tok.at[f], cc_s.at[Z - 1], cc_r.at[Z - 1], fs=other)
    own_cross.start()
    own_cross_w = remote(wt, wall.at[f], cw_s.at[Z - 1], cw_r.at[Z - 1], fs=other)
    own_cross_w.start()
    local = [
        pltpu.make_async_copy(wp.at[x], xr.at[x], loc.at[0]),
        pltpu.make_async_copy(dn.at[x], ds.at[p, :, dcols(x)], loc.at[1]),
        pltpu.make_async_copy(nt, tok.at[f], loc.at[2]),
        pltpu.make_async_copy(wt, wall.at[f], loc.at[3]),
    ]
    for copy in local:
        copy.start()

    def across(i, fo, side):
        return remote(
            tok.at[fo, :, cols(x)], tok.at[fo, :, cols(x)], xt_s.at[side, i], xt_r.at[side, i], tp=xside[side]
        )

    def across_recv(i, fo, side):
        held = tok.at[fo, :, cols(xside[1 - side])]
        return remote(held, held, xt_s.at[side, i], xt_r.at[side, i], tp=xside[side])

    def from_left(s):
        return ((z + Z - s) % Z) * 2 + c

    def from_right(s):
        return ((z + s) % Z) * 2 + c

    def origin(i):
        s = i // 2 + 1
        return jnp.where(i % 2 == 0, from_left(s), from_right(s))

    def ring_step(s):
        for side in (0, 1):
            if s < H or side == 0:
                fo = from_left(s) if side == 0 else from_right(s)
                ring(s - 1, fo, side).wait_recv()
                ring_w(s - 1, fo, side).wait_recv()
                if s < H - side:
                    ring(s, fo, side).start()
                    ring_w(s, fo, side).start()
                for way in (0, 1):
                    across(2 * s - 2 + side, fo, way).start()

    turns = (
        ((0, 1), (0, 3)), ((0, 2), (0, 0)), ((2, 1), (2, 2)), ((2, 0), (2, 3)),
        ((3, 1), (1, 2)), ((1, 1), (3, 2)), ((3, 0), (1, 3)), ((1, 0), (3, 3)),
    )
    needs = {0: (0,), 2: (2,), 4: (1, 3)}

    def za(n, u, cd):
        zc = (z + n + Q * u) % Z
        return remote(
            xr.at[zc // Q, spot(n), cd], gu.at[f, p], za_s.at[n * TP + u, cd], za_r.at[n * TP + u, c], fs=zc * 2 + cd
        )

    def source(n, u):
        return (z + Z - n - Q * u) % Z

    def za_recv(n, u, cs):
        held = gu.at[2 * source(n, u) + cs, p]
        return remote(held, held, za_s.at[n * TP + u, cs], za_r.at[n * TP + u, cs], fs=other)

    def y_hand(n, u):
        held = gu.at[pl.ds(2 * source(n, u), 2), p]
        return remote(held, held, y_s.at[n * TP + u], y_r.at[n * TP + u], grp=mate)

    def y_recv(n, u):
        held = gu.at[pl.ds(2 * source(n, u), 2), 1 - p]
        return remote(held, held, y_s.at[n * TP + u], y_r.at[n * TP + u], grp=mate)

    own = pltpu.make_async_copy(xr.at[zone, seat, c], gu.at[f, p], loc.at[4])

    def issue(b):
        for n in needs.get(b, ()):
            for side in (0, 1):
                xw_recv(n, side).wait_recv()
            second_leg_recv(n).wait_recv()
        for n, u in turns[b]:
            if n == 0 and u == 0:
                za(0, 0, 1 - c).start()
                own.start()
            else:
                za(n, u, 0).start()
                za(n, u, 1).start()

    def accept(b):
        for n, u in turns[b]:
            if n == 0 and u == 0:
                own.wait()
                za_recv(0, 0, 1 - c).wait_recv()
            else:
                za_recv(n, u, 0).wait_recv()
                za_recv(n, u, 1).wait_recv()
            y_hand(n, u).start()

    def onward(i, fo, side):
        held = tok.at[fo, pl.ds(side * half, half), cols(xside[1 - side])]
        return remote(held, held, xo_s.at[side, i], xo_r.at[side, i], tp=xside[side])

    def onward_recv(i, fo, side):
        held = tok.at[fo, pl.ds(side * half, half), cols(opposite)]
        return remote(held, held, xo_s.at[side, i], xo_r.at[side, i], tp=xside[side])

    def cross(i, fo):
        return remote(tok.at[fo], tok.at[fo], cc_s.at[i], cc_r.at[i], fs=other)

    def cross_w(i, fo):
        return remote(wall.at[fo], wall.at[fo], cw_s.at[i], cw_r.at[i], fs=other)

    def cross_recv(i, fo):
        return remote(tok.at[fo + 1 - 2 * c], tok.at[fo + 1 - 2 * c], cc_s.at[i], cc_r.at[i], fs=other)

    def cross_w_recv(i, fo):
        return remote(wall.at[fo + 1 - 2 * c], wall.at[fo + 1 - 2 * c], cw_s.at[i], cw_r.at[i], fs=other)

    def pass_on(i):
        fo = origin(i)
        for side in (0, 1):
            across_recv(i, fo, side).wait_recv()
            onward(i, fo, side).start()

    def finish(i):
        fo = origin(i)
        for side in (0, 1):
            onward_recv(i, fo, side).wait_recv()
        cross(i, fo).start()
        cross_w(i, fo).start()

    yd = remote(ds.at[p], ds.at[p], yd_s, yd_r, grp=mate)
    ring_step(1)
    for n in order:
        first_leg(n).wait_recv()
        second_leg(n).start()
    for k in (2, 1, 3):
        xd(k).start()
    ring_step(2)
    local[0].wait()
    issue(0)
    issue(1)
    for s in range(3, H + 1):
        ring_step(s)
        issue(s - 1)
        for i in (2 * s - 6, 2 * s - 5):
            pass_on(i)
        if s == 4:
            local[1].wait()
            for k in (2, 1, 3):
                xd_recv(k).wait_recv()
            yd.start()
        if s > 3:
            for i in (2 * s - 8, 2 * s - 7):
                finish(i)
            accept(s - 4)
    pass_on(2 * H - 4)
    pass_on(2 * H - 3)
    finish(2 * H - 6)
    finish(2 * H - 5)
    accept(H - 3)
    pass_on(2 * H - 2)
    finish(2 * H - 4)
    finish(2 * H - 3)
    accept(H - 2)
    finish(2 * H - 2)
    accept(H - 1)

    local[2].wait()
    local[3].wait()
    own_fo = f + 1 - 2 * c
    remote(nt, tok.at[own_fo], cc_s.at[Z - 1], cc_r.at[Z - 1], fs=other).wait_recv()
    remote(wt, wall.at[own_fo], cw_s.at[Z - 1], cw_r.at[Z - 1], fs=other).wait_recv()
    own_cross.wait_send()
    own_cross_w.wait_send()

    def drain(i, _):
        fo = origin(i)
        for side in (0, 1):
            across(i, fo, side).wait_send()
            onward(i, fo, side).wait_send()
        cross(i, fo).wait_send()
        cross_w(i, fo).wait_send()
        cross_recv(i, fo).wait_recv()
        cross_w_recv(i, fo).wait_recv()
        return 0

    lax.fori_loop(0, Z - 1, drain, 0)

    def ring_drain(s, _):
        ring(s, f, 0).wait_send()
        ring_w(s, f, 0).wait_send()

        @pl.when(s < H - 1)
        def _():
            ring(s, f, 1).wait_send()
            ring_w(s, f, 1).wait_send()

        return 0

    lax.fori_loop(0, H, ring_drain, 0)
    za(0, 0, 1 - c).wait_send()
    y_hand(0, 0).wait_send()
    y_recv(0, 0).wait_recv()

    def exchange_drain(v, _):
        n, u = v // TP, v % TP
        za(n, u, 0).wait_send()
        za(n, u, 1).wait_send()
        y_hand(n, u).wait_send()
        y_recv(n, u).wait_recv()
        return 0

    lax.fori_loop(1, Z, exchange_drain, 0)
    yd.wait_send()
    remote(ds.at[1 - p], ds.at[1 - p], yd_s, yd_r, grp=mate).wait_recv()
    for n in range(Q):
        first_leg(n).wait_send()
        second_leg(n).wait_send()
        for side in (0, 1):
            xw(n, side).wait_send()
    for k in range(1, TP):
        xd(k).wait_send()


def run_hand_over(FS, TP, tokens, routes, logits, gain, w_gate, w_up, w_down):
    Z = FS // 2
    Q = Z // TP
    _, rows, ff = w_gate.shape
    ff = ff // (2 * Q)
    half = rows // 2
    drows, db = w_down.shape[1] // 2, w_down.shape[2]
    vmem = pl.BlockSpec(memory_space=pltpu.VMEM)
    hbm = pl.BlockSpec(memory_space=pltpu.HBM)
    tile = (16, LANES)
    piece = (half // 2, 4 * ff)
    bf16 = jnp.bfloat16
    return pl.pallas_call(
        functools.partial(hand_over, FS, TP),
        out_shape=(
            jax.ShapeDtypeStruct((FS, 2) + piece, bf16),
            jax.ShapeDtypeStruct((2, drows, TP * db), bf16),
            jax.ShapeDtypeStruct((FS,) + tokens.shape, bf16),
            jax.ShapeDtypeStruct((FS,) + tile, bf16),
        ),
        in_specs=[hbm] * 7,
        out_specs=(vmem,) * 4,
        scratch_shapes=[
            pltpu.VMEM(tokens.shape, tokens.dtype),
            pltpu.VMEM(routes.shape, routes.dtype),
            pltpu.VMEM(logits.shape, logits.dtype),
            pltpu.VMEM(gain.shape, gain.dtype),
            pltpu.VMEM((TP, half, w_gate.shape[2]), jnp.float32),
            pltpu.VMEM((TP, half, w_gate.shape[2]), jnp.float32),
            pltpu.VMEM((TP, drows, db), jnp.float32),
            pltpu.VMEM((rows, LANES), jnp.float32),
            pltpu.VMEM((TP, Q, 2) + piece, bf16),
            pltpu.VMEM((TP, drows, db), bf16),
            pltpu.VMEM(tokens.shape, bf16),
            pltpu.VMEM(tile, bf16),
            pltpu.VMEM((TP, Q, 2) + piece, bf16),
            pltpu.VMEM((Q, 2) + piece, bf16),
            DMA((7,)), DMA((5,)),
            DMA((2, Q)), DMA((2, Q)), DMA((Q,)), DMA((Q,)), DMA((Q,)), DMA((Q,)),
            DMA((TP - 1,)), DMA((TP - 1,)),
            DMA((2, Z // 2)), DMA((2, Z // 2)), DMA((2, Z // 2)), DMA((2, Z // 2)),
            DMA((2, Z - 1)), DMA((2, Z - 1)), DMA((2, Z - 1)), DMA((2, Z - 1)),
            DMA((Z,)), DMA((Z,)), DMA((Z,)), DMA((Z,)),
            DMA((Z, 2)), DMA((Z, 2)),
            DMA((Z,)), DMA((Z,)), DMA, DMA,
        ],
        compiler_params=pltpu.CompilerParams(collective_id=0, has_side_effects=True, vmem_limit_bytes=16 << 20),
        cost_estimate=pl.CostEstimate(flops=10**9, bytes_accessed=30 << 20, transcendentals=0),
        name="hand_over",
    )(*[
        pltpu.with_memory_space_constraint(a, pltpu.HBM)
        for a in (tokens, routes, logits, gain, w_gate, w_up, w_down)
    ])


def unpack(block, gu, ds, wg, wu, gate_out, up_out, down_out, sem):
    down = pltpu.make_async_copy(ds, down_out, sem)
    down.start()
    part, ff = gu.shape[2], gu.shape[3] // 4
    pieces = block // (2 * part)

    def step(i, _):
        span = pl.ds(pl.multiple_of(i * block, block), block)
        for v in range(pieces):
            k = i * pieces + v
            piece = gu[k // 2, k % 2].astype(jnp.float32)
            for hh in (0, 1):
                at = pl.ds(pl.multiple_of(k * 2 * part + hh * part, part), part)
                wg[at, :] = piece[:, 2 * hh * ff : (2 * hh + 1) * ff].astype(jnp.bfloat16)
                wu[at, :] = piece[:, (2 * hh + 1) * ff : (2 * hh + 2) * ff].astype(jnp.bfloat16)
        for own, served in ((wg, gate_out), (wu, up_out)):
            served[:, span] = own[span, :].astype(jnp.float32).T.astype(jnp.bfloat16)
        return 0

    lax.fori_loop(0, wg.shape[0] // block, step, 0)
    down.wait()


def run_unpack(gu, ds):
    ff = gu.shape[3] // 4
    features = gu.shape[0] * gu.shape[1] * gu.shape[2] * 2
    vmem = pl.BlockSpec(memory_space=pltpu.VMEM)
    bf16 = jnp.bfloat16
    return pl.pallas_call(
        functools.partial(unpack, 256),
        out_shape=(
            jax.ShapeDtypeStruct((features, ff), bf16),
            jax.ShapeDtypeStruct((features, ff), bf16),
            jax.ShapeDtypeStruct((ff, features), bf16),
            jax.ShapeDtypeStruct((ff, features), bf16),
            jax.ShapeDtypeStruct(ds.shape, bf16),
        ),
        in_specs=[vmem] * 2,
        out_specs=(vmem,) * 4 + (pl.BlockSpec(memory_space=pltpu.HBM),),
        scratch_shapes=[DMA],
        compiler_params=pltpu.CompilerParams(vmem_limit_bytes=8 << 20),
        cost_estimate=pl.CostEstimate(flops=10**9, bytes_accessed=16 << 20, transcendentals=0),
        name="unpack",
    )(gu, ds)


def combine(FS, TP, L, wg, wu, tok, wall, wd, out, wdt, hs, part, prec, zs, zr, outt, turned, xd_s, xd_r, xo_s, xo_r, cc_s, cc_r, z_s, z_r, fin_s, fin_r):
    Z = FS // 2
    H = Z // 2
    x, f = lax.axis_index("tp"), lax.axis_index("fs")
    z, c = f // 2, f % 2
    other = f + 1 - 2 * c
    ff, block = hs.shape[2], hs.shape[3]
    half = ff // 2
    keep = part.shape[1] // 2
    xside = ((x + 1) % TP, (x + TP - 1) % TP)
    zside = (((z + 1) % Z) * 2 + c, ((z + Z - 1) % Z) * 2 + c)

    barrier = pltpu.get_barrier_semaphore()
    for k in xside:
        pl.semaphore_signal(barrier, inc=1, device_id={"tp": k}, device_id_type=MESH)
    for k in zside + (other,):
        pl.semaphore_signal(barrier, inc=1, device_id={"fs": k}, device_id_type=MESH)

    def away(i):
        return H - (i + 1) // 2

    def chip(i):
        return jnp.where(i % 2 == 0, (z + away(i)) % Z, (z + Z - away(i)) % Z)

    count, features = tok.shape[1], tok.shape[2]

    def make(i):
        rows = jnp.concatenate([tok[pl.ds(2 * chip(i + v), 2)].reshape(block, features) for v in (0, 1)], axis=0)
        gate = jnp.dot(rows, wg[...], preferred_element_type=jnp.float32)
        up = jnp.dot(rows, wu[...], preferred_element_type=jnp.float32)
        hidden = (jax.nn.silu(gate) * up).T
        for v in (0, 1):
            scale = [wall[2 * chip(i + v) + n, 0:1, :count] for n in (0, 1)]
            scale = jnp.concatenate(scale, axis=1).astype(jnp.float32)
            hs[i + v, x] = (hidden[:, v * block : (v + 1) * block] * scale).astype(jnp.bfloat16)

    def direct(i, side):
        return remote(hs.at[i, x], hs.at[i, x], xd_s.at[side, i], xd_r.at[side, i], tp=xside[side])

    def direct_recv(i, side):
        held = hs.at[i, xside[1 - side]]
        return remote(held, held, xd_s.at[side, i], xd_r.at[side, i], tp=xside[side])

    def onward(i, side):
        held = hs.at[i, xside[1 - side], pl.ds(side * half, half)]
        return remote(held, held, xo_s.at[side, i], xo_r.at[side, i], tp=xside[side])

    def onward_recv(i, side):
        held = hs.at[i, (x + 2) % TP, pl.ds(side * half, half)]
        return remote(held, held, xo_s.at[side, i], xo_r.at[side, i], tp=xside[side])

    def cross(j):
        return remote(part.at[j, pl.ds((1 - c) * keep, keep)], prec.at[j], cc_s.at[j], cc_r.at[j], fs=other)

    def walk(m, side):
        k = away(m) - 1
        return remote(zs.at[m], zr.at[side, k], z_s.at[m], z_r.at[side, k], fs=zside[side])

    def arrival(side, k):
        return remote(zs.at[0], zr.at[side, k], z_s.at[0], z_r.at[side, k], fs=zside[side])

    AHEAD = 2

    def begin(k, _):
        make(2 * k)

        @pl.when(k == 0)
        def _():
            pl.semaphore_wait(barrier, 5)

        @pl.when(2 * k < AHEAD)
        def _():
            for v in (0, 1):
                for side in (0, 1):
                    direct(2 * k + v, side).start()

        return 0

    lax.fori_loop(0, AHEAD // 2 + 1, begin, 0)
    for e in range(TP):
        wdt[:, e * ff : (e + 1) * ff] = wd[e].T.astype(jnp.bfloat16)

    def step(i, _):
        @pl.when(i + AHEAD < Z)
        def _():
            for side in (0, 1):
                direct(i + AHEAD, side).start()

        @pl.when(i < Z)
        def _():
            for side in (0, 1):
                direct_recv(i, side).wait_recv()
                onward(i, side).start()

        @pl.when((i % 2 == 0) & (i + AHEAD + 2 < Z))
        def _():
            make(i + AHEAD + 2)

        @pl.when((i >= L) & (i < Z + L))
        def _():
            j = i - L
            for side in (0, 1):
                onward_recv(j, side).wait_recv()
            rhs = hs[j].reshape(TP * ff, block)
            part[j] = jnp.dot(wdt[...], rhs, preferred_element_type=jnp.float32)
            cross(j).start()

        @pl.when(i > L)
        def _():
            m = i - L - 1
            k = away(m)
            cross(m).wait_recv()
            total = part[m, pl.ds(c * keep, keep)] + prec[m]

            @pl.when(m == 0)
            def _():
                zs[m] = total.astype(jnp.bfloat16)

            @pl.when(m == 1)
            def _():
                zs[m] = total.astype(jnp.bfloat16)

            for side in (0, 1):
                @pl.when((m >= 2) & (m < Z - 1) & (m % 2 == side))
                def _():
                    arrival(side, k).wait_recv()
                    zs[m] = (total + zr[side, k].astype(jnp.float32)).astype(jnp.bfloat16)

                @pl.when((m < Z - 1) & (m % 2 == side))
                def _():
                    walk(m, side).start()

            @pl.when(m == Z - 1)
            def _():
                arrival(0, 0).wait_recv()
                arrival(1, 0).wait_recv()
                both = zr[0, 0].astype(jnp.float32) + zr[1, 0].astype(jnp.float32)
                outt[pl.ds(c * keep, keep)] = (total + both).astype(jnp.bfloat16)

        return 0

    lax.fori_loop(0, Z + L + 1, step, 0)
    last = remote(outt.at[pl.ds(c * keep, keep)], outt.at[pl.ds(c * keep, keep)], fin_s, fin_r, fs=other)
    last.start()

    def drain(i, _):
        for side in (0, 1):
            direct(i, side).wait_send()
            onward(i, side).wait_send()
        cross(i).wait_send()

        @pl.when(i < Z - 1)
        def _():
            arrival_of = remote(zs.at[i], zr.at[0, 0], z_s.at[i], z_r.at[0, 0], fs=other)
            arrival_of.wait_send()

        return 0

    lax.fori_loop(0, Z, drain, 0)
    last.wait()
    turned[...] = outt[...].astype(jnp.float32).T
    rows = block // 2
    out[...] = turned[pl.ds(c * rows, rows)].astype(jnp.bfloat16)


def run_combine(FS, TP, wg, wu, tok, wall, wd):
    Z = FS // 2
    ff = wg.shape[1]
    block = 2 * tok.shape[1]
    feats = wd.shape[2]
    vmem = pl.BlockSpec(memory_space=pltpu.VMEM)
    return pl.pallas_call(
        functools.partial(combine, FS, TP, 2),
        out_shape=jax.ShapeDtypeStruct((block // 2, feats), jnp.bfloat16),
        in_specs=[vmem] * 5,
        out_specs=vmem,
        scratch_shapes=[
            pltpu.VMEM((feats, TP * ff), jnp.bfloat16),
            pltpu.VMEM((Z, TP, ff, block), jnp.bfloat16),
            pltpu.VMEM((Z, feats, block), jnp.float32),
            pltpu.VMEM((Z, feats // 2, block), jnp.float32),
            pltpu.VMEM((Z - 1, feats // 2, block), jnp.bfloat16),
            pltpu.VMEM((2, Z // 2, feats // 2, block), jnp.bfloat16),
            pltpu.VMEM((feats, block), jnp.bfloat16),
            pltpu.VMEM((block, feats), jnp.float32),
            DMA((2, Z)), DMA((2, Z)), DMA((2, Z)), DMA((2, Z)),
            DMA((Z,)), DMA((Z,)), DMA((Z - 1,)), DMA((2, Z // 2)), DMA, DMA,
        ],
        compiler_params=pltpu.CompilerParams(collective_id=1, has_side_effects=True, vmem_limit_bytes=20 << 20),
        cost_estimate=pl.CostEstimate(flops=10**9, bytes_accessed=30 << 20, transcendentals=0),
        name="combine",
    )(wg, wu, tok, wall, wd)


def body(FS, TP, tokens, routes, route_logits, gain, w_gate, w_up, w_down):
    gu, ds, tok, wall = run_hand_over(
        FS, TP, tokens, routes.T, route_logits.T, gain[None], w_gate, w_up, w_down
    )
    wg, wu, gate_t, up_t, down = run_unpack(gu, ds)
    mixed = run_combine(FS, TP, wg, wu, tok, wall, w_down)
    return (gate_t.T[None], up_t.T[None], down.reshape(1, 2 * ds.shape[1], -1), mixed)


def solution(mesh):
    return jax.shard_map(
        functools.partial(body, mesh.shape["fs"], mesh.shape["tp"]),
        mesh=mesh,
        in_specs=(
            P(("grp", "fs"), None),
            P(("grp", "fs"), None),
            P(("grp", "fs"), None),
            P("fs"),
            P(None, "fs", "tp"),
            P(None, "fs", "tp"),
            P(None, "fs", "tp"),
        ),
        out_specs=(
            P(("grp", "tp"), None, "fs"),
            P(("grp", "tp"), None, "fs"),
            P(("grp", "tp"), "fs", None),
            P(("grp", "fs"), "tp"),
        ),
        check_vma=False,
    )
```

```python
import functools

import jax
import jax.numpy as jnp
from jax import lax
from jax.experimental import pallas as pl
from jax.experimental.pallas import tpu as pltpu
from jax.sharding import PartitionSpec as P

MESH = pl.DeviceIdType.MESH
DMA = pltpu.SemaphoreType.DMA
LANES = 128


def remote(src, dst, send, recv, **where):
    return pltpu.make_async_remote_copy(
        src_ref=src, dst_ref=dst, send_sem=send, recv_sem=recv, device_id=where, device_id_type=MESH
    )


def hand_over(
    FS, TP, x_hbm, routes_hbm, logits_hbm, gain_hbm, w_gate, w_up, w_down, gu, ds, tok, wall,
    x_in, routes, logits, gain, raw_gate, raw_up, raw_down, scale, wp, dn, nt, wt, xr, stage,
    in_s, loc, xw_s, xw_r, st_s, st_r, sf_s, sf_r, xd_s, xd_r, rs, rr, ws, wr, xt_s, xt_r, xo_s, xo_r,
    cc_s, cc_r, cw_s, cw_r, za_s, za_r, y_s, y_r, yd_s, yd_r,
):
    Z = FS // 2
    H = Z // 2
    Q = Z // TP
    assert TP == 4 and Q == 4 and Q * TP == Z
    x, f, g = lax.axis_index("tp"), lax.axis_index("fs"), lax.axis_index("grp")
    z, c = f // 2, f % 2
    zone, seat = z // Q, z % Q
    order = (0, 2, 1, 3)
    p = g % 2
    mate = g + 1 - 2 * p
    fb = nt.shape[1] // TP
    half = nt.shape[0] // 2
    db = dn.shape[2]
    rows = raw_gate.shape[1]
    drows = raw_down.shape[1]
    other = f + 1 - 2 * c
    xside = ((x + 1) % TP, (x + TP - 1) % TP)
    zside = (((z + 1) % Z) * 2 + c, ((z + Z - 1) % Z) * 2 + c)
    opposite = (x + 2) % TP

    fetch = (
        pltpu.make_async_copy(x_hbm, x_in, in_s.at[3]),
        pltpu.make_async_copy(routes_hbm, routes, in_s.at[4]),
        pltpu.make_async_copy(logits_hbm, logits, in_s.at[5]),
        pltpu.make_async_copy(gain_hbm, gain, in_s.at[6]),
        pltpu.make_async_copy(w_gate.at[:, pl.ds(p * rows, rows)], raw_gate, in_s.at[0]),
        pltpu.make_async_copy(w_up.at[:, pl.ds(p * rows, rows)], raw_up, in_s.at[1]),
        pltpu.make_async_copy(w_down.at[:, pl.ds(p * drows, drows)], raw_down, in_s.at[2]),
    )
    for copy in fetch:
        copy.start()

    barrier = pltpu.get_barrier_semaphore()

    def greet(r, _):
        pl.semaphore_signal(barrier, inc=1, device_id={"fs": (f + r) % FS}, device_id_type=MESH)
        return 0

    lax.fori_loop(1, FS, greet, 0)
    for k in range(1, TP):
        pl.semaphore_signal(barrier, inc=1, device_id={"tp": (x + k) % TP}, device_id_type=MESH)
    pl.semaphore_signal(barrier, inc=1, device_id={"grp": mate}, device_id_type=MESH)

    for copy in fetch[:4]:
        copy.wait()
    values = x_in[...].astype(jnp.float32)
    mean_square = jnp.mean(values * values, axis=-1, keepdims=True)
    nt[...] = (values * lax.rsqrt(mean_square + 1e-06)).astype(jnp.bfloat16)
    count = routes.shape[1]
    first = jax.nn.sigmoid(logits[0:1] - logits[1:2])
    second = jax.nn.sigmoid(logits[1:2] - logits[0:1])
    weight = first * (routes[0:1] == x).astype(jnp.float32) + second * (routes[1:2] == x).astype(jnp.float32)
    wt[...] = jnp.zeros_like(wt)
    wt[:, :count] = jnp.broadcast_to(weight, (wt.shape[0], count)).astype(jnp.bfloat16)
    scale[...] = jnp.broadcast_to(gain[...], (LANES, gain.shape[1])).T
    factor = scale[pl.ds(p * rows, rows), :][:, :1]
    ff = wp.shape[4] // 4
    part = rows // 2
    fetch[4].wait()
    fetch[5].wait()

    def pack(e):
        gate = raw_gate[e] * factor
        up = raw_up[e] * factor
        for j in range(2 * Q):
            span = slice(j * ff, (j + 1) * ff)
            quarters = [gate[:part, span], up[:part, span], gate[part:, span], up[part:, span]]
            wp[e, j // 2, j % 2] = jnp.concatenate(quarters, axis=1).astype(jnp.bfloat16)

    pack(opposite)
    pl.semaphore_wait(barrier, FS - 1 + TP - 1 + 1)

    def cols(i):
        return pl.ds(pl.multiple_of(i * fb, LANES), fb)

    def dcols(i):
        return pl.ds(pl.multiple_of(i * db, LANES), db)

    def ring(i, fo, side):
        return remote(tok.at[fo, :, cols(x)], tok.at[fo, :, cols(x)], rs.at[side, i], rr.at[side, i], fs=zside[side])

    def ring_w(i, fo, side):
        return remote(wall.at[fo], wall.at[fo], ws.at[side, i], wr.at[side, i], fs=zside[side])

    for side in (0, 1):
        remote(nt.at[:, cols(x)], tok.at[f, :, cols(x)], rs.at[side, 0], rr.at[side, 0], fs=zside[side]).start()
        remote(wt, wall.at[f], ws.at[side, 0], wr.at[side, 0], fs=zside[side]).start()

    def spot(n):
        return (seat + n) % Q

    def leg(n):
        return n // 2

    def xw(n, side):
        return remote(wp.at[xside[side], spot(n)], xr.at[x, spot(n)], xw_s.at[side, n], xw_r.at[side, n], tp=xside[side])

    def xw_recv(n, side):
        held = xr.at[xside[1 - side], spot(n)]
        return remote(held, held, xw_s.at[side, n], xw_r.at[side, n], tp=xside[side])

    def first_leg(n):
        return remote(wp.at[opposite, spot(n)], stage.at[n], st_s.at[n], st_r.at[n], tp=xside[leg(n)])

    def second_leg(n):
        return remote(stage.at[n], xr.at[xside[1 - leg(n)], spot(n)], sf_s.at[n], sf_r.at[n], tp=xside[leg(n)])

    def second_leg_recv(n):
        return remote(stage.at[n], xr.at[opposite, spot(n)], sf_s.at[n], sf_r.at[n], tp=xside[leg(n)])

    def xd(k):
        return remote(dn.at[(x + k) % TP], ds.at[p, :, dcols(x)], xd_s.at[k - 1], xd_r.at[k - 1], tp=(x + k) % TP)

    def xd_recv(k):
        held = ds.at[p, :, dcols((x + TP - k) % TP)]
        return remote(held, held, xd_s.at[k - 1], xd_r.at[k - 1], tp=(x + k) % TP)

    def send_packed(k, _):
        @pl.when(k == 0)
        def _():
            for n in order[:2]:
                first_leg(n).start()

        e = jnp.where(k < 2, jnp.where(k == 0, xside[0], xside[1]), x)
        pack(e)

        @pl.when(k == 0)
        def _():
            for n in order:
                xw(n, 0).start()

        @pl.when(k == 1)
        def _():
            for n in order:
                xw(n, 1).start()
            for n in order[2:]:
                first_leg(n).start()

        return 0

    lax.fori_loop(0, 3, send_packed, 0)
    fetch[6].wait()
    dn[...] = raw_down[...].astype(jnp.bfloat16)
    own_cross = remote(nt, tok.at[f], cc_s.at[Z - 1], cc_r.at[Z - 1], fs=other)
    own_cross.start()
    own_cross_w = remote(wt, wall.at[f], cw_s.at[Z - 1], cw_r.at[Z - 1], fs=other)
    own_cross_w.start()
    local = [
        pltpu.make_async_copy(wp.at[x], xr.at[x], loc.at[0]),
        pltpu.make_async_copy(dn.at[x], ds.at[p, :, dcols(x)], loc.at[1]),
        pltpu.make_async_copy(nt, tok.at[f], loc.at[2]),
        pltpu.make_async_copy(wt, wall.at[f], loc.at[3]),
    ]
    for copy in local:
        copy.start()

    def across(i, fo, side):
        return remote(
            tok.at[fo, :, cols(x)], tok.at[fo, :, cols(x)], xt_s.at[side, i], xt_r.at[side, i], tp=xside[side]
        )

    def across_recv(i, fo, side):
        held = tok.at[fo, :, cols(xside[1 - side])]
        return remote(held, held, xt_s.at[side, i], xt_r.at[side, i], tp=xside[side])

    def from_left(s):
        return ((z + Z - s) % Z) * 2 + c

    def from_right(s):
        return ((z + s) % Z) * 2 + c

    def origin(i):
        s = i // 2 + 1
        return jnp.where(i % 2 == 0, from_left(s), from_right(s))

    def ring_step(s):
        for side in (0, 1):
            if s < H or side == 0:
                fo = from_left(s) if side == 0 else from_right(s)
                ring(s - 1, fo, side).wait_recv()
                ring_w(s - 1, fo, side).wait_recv()
                if s < H - side:
                    ring(s, fo, side).start()
                    ring_w(s, fo, side).start()
                for way in (0, 1):
                    across(2 * s - 2 + side, fo, way).start()

    turns = (
        ((0, 1), (0, 3)), ((0, 2), (0, 0)), ((2, 1), (2, 2)), ((2, 0), (2, 3)),
        ((3, 1), (1, 2)), ((1, 1), (3, 2)), ((3, 0), (1, 3)), ((1, 0), (3, 3)),
    )
    needs = {0: (0,), 2: (2,), 4: (1, 3)}

    def za(n, u, cd):
        zc = (z + n + Q * u) % Z
        return remote(
            xr.at[zc // Q, spot(n), cd], gu.at[f, p], za_s.at[n * TP + u, cd], za_r.at[n * TP + u, c], fs=zc * 2 + cd
        )

    def source(n, u):
        return (z + Z - n - Q * u) % Z

    def za_recv(n, u, cs):
        held = gu.at[2 * source(n, u) + cs, p]
        return remote(held, held, za_s.at[n * TP + u, cs], za_r.at[n * TP + u, cs], fs=other)

    def y_hand(n, u):
        held = gu.at[pl.ds(2 * source(n, u), 2), p]
        return remote(held, held, y_s.at[n * TP + u], y_r.at[n * TP + u], grp=mate)

    def y_recv(n, u):
        held = gu.at[pl.ds(2 * source(n, u), 2), 1 - p]
        return remote(held, held, y_s.at[n * TP + u], y_r.at[n * TP + u], grp=mate)

    own = pltpu.make_async_copy(xr.at[zone, seat, c], gu.at[f, p], loc.at[4])

    def issue(b):
        for n in needs.get(b, ()):
            for side in (0, 1):
                xw_recv(n, side).wait_recv()
            second_leg_recv(n).wait_recv()
        for n, u in turns[b]:
            if n == 0 and u == 0:
                za(0, 0, 1 - c).start()
                own.start()
            else:
                za(n, u, 0).start()
                za(n, u, 1).start()

    def accept(b):
        for n, u in turns[b]:
            if n == 0 and u == 0:
                own.wait()
                za_recv(0, 0, 1 - c).wait_recv()
            else:
                za_recv(n, u, 0).wait_recv()
                za_recv(n, u, 1).wait_recv()
            y_hand(n, u).start()

    def onward(i, fo, side):
        held = tok.at[fo, pl.ds(side * half, half), cols(xside[1 - side])]
        return remote(held, held, xo_s.at[side, i], xo_r.at[side, i], tp=xside[side])

    def onward_recv(i, fo, side):
        held = tok.at[fo, pl.ds(side * half, half), cols(opposite)]
        return remote(held, held, xo_s.at[side, i], xo_r.at[side, i], tp=xside[side])

    def cross(i, fo):
        return remote(tok.at[fo], tok.at[fo], cc_s.at[i], cc_r.at[i], fs=other)

    def cross_w(i, fo):
        return remote(wall.at[fo], wall.at[fo], cw_s.at[i], cw_r.at[i], fs=other)

    def cross_recv(i, fo):
        return remote(tok.at[fo + 1 - 2 * c], tok.at[fo + 1 - 2 * c], cc_s.at[i], cc_r.at[i], fs=other)

    def cross_w_recv(i, fo):
        return remote(wall.at[fo + 1 - 2 * c], wall.at[fo + 1 - 2 * c], cw_s.at[i], cw_r.at[i], fs=other)

    def pass_on(i):
        fo = origin(i)
        for side in (0, 1):
            across_recv(i, fo, side).wait_recv()
            onward(i, fo, side).start()

    def finish(i):
        fo = origin(i)
        for side in (0, 1):
            onward_recv(i, fo, side).wait_recv()
        cross(i, fo).start()
        cross_w(i, fo).start()

    yd = remote(ds.at[p], ds.at[p], yd_s, yd_r, grp=mate)
    ring_step(1)
    for n in order:
        first_leg(n).wait_recv()
        second_leg(n).start()
    for k in (2, 1, 3):
        xd(k).start()
    ring_step(2)
    local[0].wait()
    issue(0)
    issue(1)
    for s in range(3, H + 1):
        ring_step(s)
        issue(s - 1)
        for i in (2 * s - 6, 2 * s - 5):
            pass_on(i)
        if s == 4:
            local[1].wait()
            for k in (2, 1, 3):
                xd_recv(k).wait_recv()
            yd.start()
        if s > 3:
            for i in (2 * s - 8, 2 * s - 7):
                finish(i)
        accept(s - 3)
    pass_on(2 * H - 4)
    pass_on(2 * H - 3)
    finish(2 * H - 6)
    finish(2 * H - 5)
    pass_on(2 * H - 2)
    finish(2 * H - 4)
    finish(2 * H - 3)
    accept(H - 2)
    finish(2 * H - 2)
    accept(H - 1)

    local[2].wait()
    local[3].wait()
    own_fo = f + 1 - 2 * c
    remote(nt, tok.at[own_fo], cc_s.at[Z - 1], cc_r.at[Z - 1], fs=other).wait_recv()
    remote(wt, wall.at[own_fo], cw_s.at[Z - 1], cw_r.at[Z - 1], fs=other).wait_recv()
    own_cross.wait_send()
    own_cross_w.wait_send()

    def drain(i, _):
        fo = origin(i)
        for side in (0, 1):
            across(i, fo, side).wait_send()
            onward(i, fo, side).wait_send()
        cross(i, fo).wait_send()
        cross_w(i, fo).wait_send()
        cross_recv(i, fo).wait_recv()
        cross_w_recv(i, fo).wait_recv()
        return 0

    lax.fori_loop(0, Z - 1, drain, 0)

    def ring_drain(s, _):
        ring(s, f, 0).wait_send()
        ring_w(s, f, 0).wait_send()

        @pl.when(s < H - 1)
        def _():
            ring(s, f, 1).wait_send()
            ring_w(s, f, 1).wait_send()

        return 0

    lax.fori_loop(0, H, ring_drain, 0)
    za(0, 0, 1 - c).wait_send()
    y_hand(0, 0).wait_send()
    y_recv(0, 0).wait_recv()

    def exchange_drain(v, _):
        n, u = v // TP, v % TP
        za(n, u, 0).wait_send()
        za(n, u, 1).wait_send()
        y_hand(n, u).wait_send()
        y_recv(n, u).wait_recv()
        return 0

    lax.fori_loop(1, Z, exchange_drain, 0)
    yd.wait_send()
    remote(ds.at[1 - p], ds.at[1 - p], yd_s, yd_r, grp=mate).wait_recv()
    for n in range(Q):
        first_leg(n).wait_send()
        second_leg(n).wait_send()
        for side in (0, 1):
            xw(n, side).wait_send()
    for k in range(1, TP):
        xd(k).wait_send()


def run_hand_over(FS, TP, tokens, routes, logits, gain, w_gate, w_up, w_down):
    Z = FS // 2
    Q = Z // TP
    _, rows, ff = w_gate.shape
    ff = ff // (2 * Q)
    half = rows // 2
    drows, db = w_down.shape[1] // 2, w_down.shape[2]
    vmem = pl.BlockSpec(memory_space=pltpu.VMEM)
    hbm = pl.BlockSpec(memory_space=pltpu.HBM)
    tile = (16, LANES)
    piece = (half // 2, 4 * ff)
    bf16 = jnp.bfloat16
    return pl.pallas_call(
        functools.partial(hand_over, FS, TP),
        out_shape=(
            jax.ShapeDtypeStruct((FS, 2) + piece, bf16),
            jax.ShapeDtypeStruct((2, drows, TP * db), bf16),
            jax.ShapeDtypeStruct((FS,) + tokens.shape, bf16),
            jax.ShapeDtypeStruct((FS,) + tile, bf16),
        ),
        in_specs=[hbm] * 7,
        out_specs=(vmem,) * 4,
        scratch_shapes=[
            pltpu.VMEM(tokens.shape, tokens.dtype),
            pltpu.VMEM(routes.shape, routes.dtype),
            pltpu.VMEM(logits.shape, logits.dtype),
            pltpu.VMEM(gain.shape, gain.dtype),
            pltpu.VMEM((TP, half, w_gate.shape[2]), jnp.float32),
            pltpu.VMEM((TP, half, w_gate.shape[2]), jnp.float32),
            pltpu.VMEM((TP, drows, db), jnp.float32),
            pltpu.VMEM((rows, LANES), jnp.float32),
            pltpu.VMEM((TP, Q, 2) + piece, bf16),
            pltpu.VMEM((TP, drows, db), bf16),
            pltpu.VMEM(tokens.shape, bf16),
            pltpu.VMEM(tile, bf16),
            pltpu.VMEM((TP, Q, 2) + piece, bf16),
            pltpu.VMEM((Q, 2) + piece, bf16),
            DMA((7,)), DMA((5,)),
            DMA((2, Q)), DMA((2, Q)), DMA((Q,)), DMA((Q,)), DMA((Q,)), DMA((Q,)),
            DMA((TP - 1,)), DMA((TP - 1,)),
            DMA((2, Z // 2)), DMA((2, Z // 2)), DMA((2, Z // 2)), DMA((2, Z // 2)),
            DMA((2, Z - 1)), DMA((2, Z - 1)), DMA((2, Z - 1)), DMA((2, Z - 1)),
            DMA((Z,)), DMA((Z,)), DMA((Z,)), DMA((Z,)),
            DMA((Z, 2)), DMA((Z, 2)),
            DMA((Z,)), DMA((Z,)), DMA, DMA,
        ],
        compiler_params=pltpu.CompilerParams(collective_id=0, has_side_effects=True, vmem_limit_bytes=16 << 20),
        cost_estimate=pl.CostEstimate(flops=10**9, bytes_accessed=30 << 20, transcendentals=0),
        name="hand_over",
    )(*[
        pltpu.with_memory_space_constraint(a, pltpu.HBM)
        for a in (tokens, routes, logits, gain, w_gate, w_up, w_down)
    ])


def unpack(block, gu, ds, wg, wu, gate_out, up_out, down_out, gate_t, up_t, sem, sems):
    down = pltpu.make_async_copy(ds, down_out, sem)
    down.start()
    part, ff = gu.shape[2], gu.shape[3] // 4
    pieces = block // (2 * part)
    blocks = wg.shape[0] // block

    def served(i, n):
        span = pl.ds(pl.multiple_of(i * block, block), block)
        held, out = ((gate_t, gate_out), (up_t, up_out))[n]
        return pltpu.make_async_copy(held.at[:, span], out.at[:, span], sems.at[n, i])

    def step(i, _):
        span = pl.ds(pl.multiple_of(i * block, block), block)
        for v in range(pieces):
            k = i * pieces + v
            piece = gu[k // 2, k % 2].astype(jnp.float32)
            for hh in (0, 1):
                at = pl.ds(pl.multiple_of(k * 2 * part + hh * part, part), part)
                wg[at, :] = piece[:, 2 * hh * ff : (2 * hh + 1) * ff].astype(jnp.bfloat16)
                wu[at, :] = piece[:, (2 * hh + 1) * ff : (2 * hh + 2) * ff].astype(jnp.bfloat16)
        for n, (own, held) in enumerate(((wg, gate_t), (wu, up_t))):
            held[:, span] = own[span, :].astype(jnp.float32).T.astype(jnp.bfloat16)
            served(i, n).start()
        return 0

    lax.fori_loop(0, blocks, step, 0)
    down.wait()

    def drain(i, _):
        served(i, 0).wait()
        served(i, 1).wait()
        return 0

    lax.fori_loop(0, blocks, drain, 0)


def run_unpack(gu, ds):
    ff = gu.shape[3] // 4
    features = gu.shape[0] * gu.shape[1] * gu.shape[2] * 2
    vmem = pl.BlockSpec(memory_space=pltpu.VMEM)
    bf16 = jnp.bfloat16
    return pl.pallas_call(
        functools.partial(unpack, 256),
        out_shape=(
            jax.ShapeDtypeStruct((features, ff), bf16),
            jax.ShapeDtypeStruct((features, ff), bf16),
            jax.ShapeDtypeStruct((ff, features), bf16),
            jax.ShapeDtypeStruct((ff, features), bf16),
            jax.ShapeDtypeStruct(ds.shape, bf16),
        ),
        in_specs=[vmem] * 2,
        out_specs=(vmem,) * 2 + (pl.BlockSpec(memory_space=pltpu.HBM),) * 3,
        scratch_shapes=[
            pltpu.VMEM((ff, features), bf16), pltpu.VMEM((ff, features), bf16), DMA, DMA((2, features // 256)),
        ],
        compiler_params=pltpu.CompilerParams(vmem_limit_bytes=8 << 20),
        cost_estimate=pl.CostEstimate(flops=10**9, bytes_accessed=16 << 20, transcendentals=0),
        name="unpack",
    )(gu, ds)


def combine(FS, TP, L, wg, wu, tok, wall, wd, out, wdt, hs, part, prec, zs, zr, outt, turned, xd_s, xd_r, xo_s, xo_r, cc_s, cc_r, z_s, z_r, fin_s, fin_r):
    Z = FS // 2
    H = Z // 2
    x, f = lax.axis_index("tp"), lax.axis_index("fs")
    z, c = f // 2, f % 2
    other = f + 1 - 2 * c
    ff, block = hs.shape[2], hs.shape[3]
    half = ff // 2
    keep = part.shape[1] // 2
    xside = ((x + 1) % TP, (x + TP - 1) % TP)
    zside = (((z + 1) % Z) * 2 + c, ((z + Z - 1) % Z) * 2 + c)

    barrier = pltpu.get_barrier_semaphore()
    for k in xside:
        pl.semaphore_signal(barrier, inc=1, device_id={"tp": k}, device_id_type=MESH)
    for k in zside + (other,):
        pl.semaphore_signal(barrier, inc=1, device_id={"fs": k}, device_id_type=MESH)

    def away(i):
        return H - (i + 1) // 2

    def chip(i):
        return jnp.where(i % 2 == 0, (z + away(i)) % Z, (z + Z - away(i)) % Z)

    count, features = tok.shape[1], tok.shape[2]

    def make(i):
        rows = jnp.concatenate([tok[pl.ds(2 * chip(i + v), 2)].reshape(block, features) for v in (0, 1)], axis=0)
        gate = jnp.dot(rows, wg[...], preferred_element_type=jnp.float32)
        up = jnp.dot(rows, wu[...], preferred_element_type=jnp.float32)
        hidden = (jax.nn.silu(gate) * up).T
        for v in (0, 1):
            scale = [wall[2 * chip(i + v) + n, 0:1, :count] for n in (0, 1)]
            scale = jnp.concatenate(scale, axis=1).astype(jnp.float32)
            hs[i + v, x] = (hidden[:, v * block : (v + 1) * block] * scale).astype(jnp.bfloat16)

    def direct(i, side):
        return remote(hs.at[i, x], hs.at[i, x], xd_s.at[side, i], xd_r.at[side, i], tp=xside[side])

    def direct_recv(i, side):
        held = hs.at[i, xside[1 - side]]
        return remote(held, held, xd_s.at[side, i], xd_r.at[side, i], tp=xside[side])

    def onward(i, side):
        held = hs.at[i, xside[1 - side], pl.ds(side * half, half)]
        return remote(held, held, xo_s.at[side, i], xo_r.at[side, i], tp=xside[side])

    def onward_recv(i, side):
        held = hs.at[i, (x + 2) % TP, pl.ds(side * half, half)]
        return remote(held, held, xo_s.at[side, i], xo_r.at[side, i], tp=xside[side])

    def cross(j):
        return remote(part.at[j, pl.ds((1 - c) * keep, keep)], prec.at[j], cc_s.at[j], cc_r.at[j], fs=other)

    def walk(m, side):
        k = away(m) - 1
        return remote(zs.at[m], zr.at[side, k], z_s.at[m], z_r.at[side, k], fs=zside[side])

    def arrival(side, k):
        return remote(zs.at[0], zr.at[side, k], z_s.at[0], z_r.at[side, k], fs=zside[side])

    AHEAD = 2

    def begin(k, _):
        make(2 * k)

        @pl.when(k == 0)
        def _():
            pl.semaphore_wait(barrier, 5)

        @pl.when(2 * k < AHEAD)
        def _():
            for v in (0, 1):
                for side in (0, 1):
                    direct(2 * k + v, side).start()

        return 0

    lax.fori_loop(0, AHEAD // 2 + 1, begin, 0)
    for e in range(TP):
        wdt[:, e * ff : (e + 1) * ff] = wd[e].T.astype(jnp.bfloat16)

    def step(i, _):
        @pl.when(i + AHEAD < Z)
        def _():
            for side in (0, 1):
                direct(i + AHEAD, side).start()

        @pl.when(i < Z)
        def _():
            for side in (0, 1):
                direct_recv(i, side).wait_recv()
                onward(i, side).start()

        @pl.when((i % 2 == 0) & (i + AHEAD + 2 < Z))
        def _():
            make(i + AHEAD + 2)

        @pl.when((i >= L) & (i < Z + L))
        def _():
            j = i - L
            for side in (0, 1):
                onward_recv(j, side).wait_recv()
            rhs = hs[j].reshape(TP * ff, block)
            part[j] = jnp.dot(wdt[...], rhs, preferred_element_type=jnp.float32)
            cross(j).start()

        @pl.when(i > L)
        def _():
            m = i - L - 1
            k = away(m)
            cross(m).wait_recv()
            total = part[m, pl.ds(c * keep, keep)] + prec[m]

            @pl.when(m == 0)
            def _():
                zs[m] = total.astype(jnp.bfloat16)

            @pl.when(m == 1)
            def _():
                zs[m] = total.astype(jnp.bfloat16)

            for side in (0, 1):
                @pl.when((m >= 2) & (m < Z - 1) & (m % 2 == side))
                def _():
                    arrival(side, k).wait_recv()
                    zs[m] = (total + zr[side, k].astype(jnp.float32)).astype(jnp.bfloat16)

                @pl.when((m < Z - 1) & (m % 2 == side))
                def _():
                    walk(m, side).start()

            @pl.when(m == Z - 1)
            def _():
                arrival(0, 0).wait_recv()
                arrival(1, 0).wait_recv()
                both = zr[0, 0].astype(jnp.float32) + zr[1, 0].astype(jnp.float32)
                outt[pl.ds(c * keep, keep)] = (total + both).astype(jnp.bfloat16)

        return 0

    lax.fori_loop(0, Z + L + 1, step, 0)
    last = remote(outt.at[pl.ds(c * keep, keep)], outt.at[pl.ds(c * keep, keep)], fin_s, fin_r, fs=other)
    last.start()

    def drain(i, _):
        for side in (0, 1):
            direct(i, side).wait_send()
            onward(i, side).wait_send()
        cross(i).wait_send()

        @pl.when(i < Z - 1)
        def _():
            arrival_of = remote(zs.at[i], zr.at[0, 0], z_s.at[i], z_r.at[0, 0], fs=other)
            arrival_of.wait_send()

        return 0

    lax.fori_loop(0, Z, drain, 0)
    last.wait()
    turned[...] = outt[...].astype(jnp.float32).T
    rows = block // 2
    out[...] = turned[pl.ds(c * rows, rows)].astype(jnp.bfloat16)


def run_combine(FS, TP, wg, wu, tok, wall, wd):
    Z = FS // 2
    ff = wg.shape[1]
    block = 2 * tok.shape[1]
    feats = wd.shape[2]
    vmem = pl.BlockSpec(memory_space=pltpu.VMEM)
    return pl.pallas_call(
        functools.partial(combine, FS, TP, 2),
        out_shape=jax.ShapeDtypeStruct((block // 2, feats), jnp.bfloat16),
        in_specs=[vmem] * 5,
        out_specs=vmem,
        scratch_shapes=[
            pltpu.VMEM((feats, TP * ff), jnp.bfloat16),
            pltpu.VMEM((Z, TP, ff, block), jnp.bfloat16),
            pltpu.VMEM((Z, feats, block), jnp.float32),
            pltpu.VMEM((Z, feats // 2, block), jnp.float32),
            pltpu.VMEM((Z - 1, feats // 2, block), jnp.bfloat16),
            pltpu.VMEM((2, Z // 2, feats // 2, block), jnp.bfloat16),
            pltpu.VMEM((feats, block), jnp.bfloat16),
            pltpu.VMEM((block, feats), jnp.float32),
            DMA((2, Z)), DMA((2, Z)), DMA((2, Z)), DMA((2, Z)),
            DMA((Z,)), DMA((Z,)), DMA((Z - 1,)), DMA((2, Z // 2)), DMA, DMA,
        ],
        compiler_params=pltpu.CompilerParams(collective_id=1, has_side_effects=True, vmem_limit_bytes=20 << 20),
        cost_estimate=pl.CostEstimate(flops=10**9, bytes_accessed=30 << 20, transcendentals=0),
        name="combine",
    )(wg, wu, tok, wall, wd)


def body(FS, TP, tokens, routes, route_logits, gain, w_gate, w_up, w_down):
    gu, ds, tok, wall = run_hand_over(
        FS, TP, tokens, routes.T, route_logits.T, gain[None], w_gate, w_up, w_down
    )
    wg, wu, gate_t, up_t, down = run_unpack(gu, ds)
    mixed = run_combine(FS, TP, wg, wu, tok, wall, w_down)
    return (gate_t.T[None], up_t.T[None], down.reshape(1, 2 * ds.shape[1], -1), mixed)


def solution(mesh):
    return jax.shard_map(
        functools.partial(body, mesh.shape["fs"], mesh.shape["tp"]),
        mesh=mesh,
        in_specs=(
            P(("grp", "fs"), None),
            P(("grp", "fs"), None),
            P(("grp", "fs"), None),
            P("fs"),
            P(None, "fs", "tp"),
            P(None, "fs", "tp"),
            P(None, "fs", "tp"),
        ),
        out_specs=(
            P(("grp", "tp"), None, "fs"),
            P(("grp", "tp"), None, "fs"),
            P(("grp", "tp"), "fs", None),
            P(("grp", "fs"), "tp"),
        ),
        check_vma=False,
    )
```

```python
import functools

import jax
import jax.numpy as jnp
from jax import lax
from jax.experimental import pallas as pl
from jax.experimental.pallas import tpu as pltpu
from jax.sharding import PartitionSpec as P

MESH = pl.DeviceIdType.MESH
DMA = pltpu.SemaphoreType.DMA
LANES = 128


def remote(src, dst, send, recv, **where):
    return pltpu.make_async_remote_copy(
        src_ref=src, dst_ref=dst, send_sem=send, recv_sem=recv, device_id=where, device_id_type=MESH
    )


def hand_over(
    FS, TP, x_hbm, routes_hbm, logits_hbm, gain_hbm, w_gate, w_up, w_down, gu, ds, tok, wall,
    x_in, routes, logits, gain, raw_gate, raw_up, raw_down, scale, wp, dn, nt, wt, xr, stage,
    in_s, loc, xw_s, xw_r, st_s, st_r, sf_s, sf_r, xd_s, xd_r, rs, rr, ws, wr, xt_s, xt_r, xo_s, xo_r,
    cc_s, cc_r, cw_s, cw_r, za_s, za_r, y_s, y_r, yd_s, yd_r,
):
    Z = FS // 2
    H = Z // 2
    Q = Z // TP
    assert TP == 4 and Q == 4 and Q * TP == Z
    x, f, g = lax.axis_index("tp"), lax.axis_index("fs"), lax.axis_index("grp")
    z, c = f // 2, f % 2
    zone, seat = z // Q, z % Q
    order = (0, 2, 1, 3)
    p = g % 2
    mate = g + 1 - 2 * p
    fb = nt.shape[1] // TP
    half = nt.shape[0] // 2
    db = dn.shape[2]
    rows = raw_gate.shape[1]
    drows = raw_down.shape[1]
    other = f + 1 - 2 * c
    xside = ((x + 1) % TP, (x + TP - 1) % TP)
    zside = (((z + 1) % Z) * 2 + c, ((z + Z - 1) % Z) * 2 + c)
    opposite = (x + 2) % TP

    fetch = (
        pltpu.make_async_copy(x_hbm, x_in, in_s.at[3]),
        pltpu.make_async_copy(routes_hbm, routes, in_s.at[4]),
        pltpu.make_async_copy(logits_hbm, logits, in_s.at[5]),
        pltpu.make_async_copy(gain_hbm, gain, in_s.at[6]),
        pltpu.make_async_copy(w_gate.at[:, pl.ds(p * rows, rows)], raw_gate, in_s.at[0]),
        pltpu.make_async_copy(w_up.at[:, pl.ds(p * rows, rows)], raw_up, in_s.at[1]),
        pltpu.make_async_copy(w_down.at[:, pl.ds(p * drows, drows)], raw_down, in_s.at[2]),
    )
    for copy in fetch:
        copy.start()

    barrier = pltpu.get_barrier_semaphore()

    def greet(r, _):
        pl.semaphore_signal(barrier, inc=1, device_id={"fs": (f + r) % FS}, device_id_type=MESH)
        return 0

    lax.fori_loop(1, FS, greet, 0)
    for k in range(1, TP):
        pl.semaphore_signal(barrier, inc=1, device_id={"tp": (x + k) % TP}, device_id_type=MESH)
    pl.semaphore_signal(barrier, inc=1, device_id={"grp": mate}, device_id_type=MESH)

    for copy in fetch[:4]:
        copy.wait()
    values = x_in[...].astype(jnp.float32)
    mean_square = jnp.mean(values * values, axis=-1, keepdims=True)
    nt[...] = (values * lax.rsqrt(mean_square + 1e-06)).astype(jnp.bfloat16)
    count = routes.shape[1]
    first = jax.nn.sigmoid(logits[0:1] - logits[1:2])
    second = jax.nn.sigmoid(logits[1:2] - logits[0:1])
    weight = first * (routes[0:1] == x).astype(jnp.float32) + second * (routes[1:2] == x).astype(jnp.float32)
    wt[...] = jnp.zeros_like(wt)
    wt[:, :count] = jnp.broadcast_to(weight, (wt.shape[0], count)).astype(jnp.bfloat16)
    scale[...] = jnp.broadcast_to(gain[...], (LANES, gain.shape[1])).T
    factor = scale[pl.ds(p * rows, rows), :][:, :1]
    ff = wp.shape[4] // 4
    part = rows // 2
    fetch[4].wait()
    fetch[5].wait()

    def pack(e):
        gate = raw_gate[e] * factor
        up = raw_up[e] * factor
        for j in range(2 * Q):
            span = slice(j * ff, (j + 1) * ff)
            quarters = [gate[:part, span], up[:part, span], gate[part:, span], up[part:, span]]
            wp[e, j // 2, j % 2] = jnp.concatenate(quarters, axis=1).astype(jnp.bfloat16)

    pack(opposite)
    pl.semaphore_wait(barrier, FS - 1 + TP - 1 + 1)

    def cols(i):
        return pl.ds(pl.multiple_of(i * fb, LANES), fb)

    def dcols(i):
        return pl.ds(pl.multiple_of(i * db, LANES), db)

    def ring(i, fo, side):
        return remote(tok.at[fo, :, cols(x)], tok.at[fo, :, cols(x)], rs.at[side, i], rr.at[side, i], fs=zside[side])

    def ring_w(i, fo, side):
        return remote(wall.at[fo], wall.at[fo], ws.at[side, i], wr.at[side, i], fs=zside[side])

    for side in (0, 1):
        remote(nt.at[:, cols(x)], tok.at[f, :, cols(x)], rs.at[side, 0], rr.at[side, 0], fs=zside[side]).start()
        remote(wt, wall.at[f], ws.at[side, 0], wr.at[side, 0], fs=zside[side]).start()

    def spot(n):
        return (seat + n) % Q

    def leg(n):
        return n // 2

    def xw(n, side):
        return remote(wp.at[xside[side], spot(n)], xr.at[x, spot(n)], xw_s.at[side, n], xw_r.at[side, n], tp=xside[side])

    def xw_recv(n, side):
        held = xr.at[xside[1 - side], spot(n)]
        return remote(held, held, xw_s.at[side, n], xw_r.at[side, n], tp=xside[side])

    def first_leg(n):
        return remote(wp.at[opposite, spot(n)], stage.at[n], st_s.at[n], st_r.at[n], tp=xside[leg(n)])

    def second_leg(n):
        return remote(stage.at[n], xr.at[xside[1 - leg(n)], spot(n)], sf_s.at[n], sf_r.at[n], tp=xside[leg(n)])

    def second_leg_recv(n):
        return remote(stage.at[n], xr.at[opposite, spot(n)], sf_s.at[n], sf_r.at[n], tp=xside[leg(n)])

    def xd(k):
        return remote(dn.at[(x + k) % TP], ds.at[p, :, dcols(x)], xd_s.at[k - 1], xd_r.at[k - 1], tp=(x + k) % TP)

    def xd_recv(k):
        held = ds.at[p, :, dcols((x + TP - k) % TP)]
        return remote(held, held, xd_s.at[k - 1], xd_r.at[k - 1], tp=(x + k) % TP)

    def send_packed(k, _):
        @pl.when(k == 0)
        def _():
            for n in order[:2]:
                first_leg(n).start()

        e = jnp.where(k < 2, jnp.where(k == 0, xside[0], xside[1]), x)
        pack(e)

        @pl.when(k == 0)
        def _():
            for n in order:
                xw(n, 0).start()

        @pl.when(k == 1)
        def _():
            for n in order:
                xw(n, 1).start()
            for n in order[2:]:
                first_leg(n).start()

        return 0

    lax.fori_loop(0, 3, send_packed, 0)
    fetch[6].wait()
    dn[...] = raw_down[...].astype(jnp.bfloat16)
    own_cross = remote(nt, tok.at[f], cc_s.at[Z - 1], cc_r.at[Z - 1], fs=other)
    own_cross.start()
    own_cross_w = remote(wt, wall.at[f], cw_s.at[Z - 1], cw_r.at[Z - 1], fs=other)
    own_cross_w.start()
    local = [
        pltpu.make_async_copy(wp.at[x], xr.at[x], loc.at[0]),
        pltpu.make_async_copy(dn.at[x], ds.at[p, :, dcols(x)], loc.at[1]),
        pltpu.make_async_copy(nt, tok.at[f], loc.at[2]),
        pltpu.make_async_copy(wt, wall.at[f], loc.at[3]),
    ]
    for copy in local:
        copy.start()

    def across(i, fo, side):
        return remote(
            tok.at[fo, :, cols(x)], tok.at[fo, :, cols(x)], xt_s.at[side, i], xt_r.at[side, i], tp=xside[side]
        )

    def across_recv(i, fo, side):
        held = tok.at[fo, :, cols(xside[1 - side])]
        return remote(held, held, xt_s.at[side, i], xt_r.at[side, i], tp=xside[side])

    def from_left(s):
        return ((z + Z - s) % Z) * 2 + c

    def from_right(s):
        return ((z + s) % Z) * 2 + c

    def origin(i):
        s = i // 2 + 1
        return jnp.where(i % 2 == 0, from_left(s), from_right(s))

    def ring_step(s):
        for side in (0, 1):
            if s < H or side == 0:
                fo = from_left(s) if side == 0 else from_right(s)
                ring(s - 1, fo, side).wait_recv()
                ring_w(s - 1, fo, side).wait_recv()
                if s < H - side:
                    ring(s, fo, side).start()
                    ring_w(s, fo, side).start()
                for way in (0, 1):
                    across(2 * s - 2 + side, fo, way).start()

    turns = (
        ((0, 1), (0, 3)), ((0, 2), (0, 0)), ((2, 1), (2, 2)), ((2, 0), (2, 3)),
        ((3, 1), (1, 2)), ((1, 1), (3, 2)), ((3, 0), (1, 3)), ((1, 0), (3, 3)),
    )
    needs = {0: (0,), 2: (2,), 4: (1, 3)}

    def za(n, u, cd):
        zc = (z + n + Q * u) % Z
        return remote(
            xr.at[zc // Q, spot(n), cd], gu.at[f, p], za_s.at[n * TP + u, cd], za_r.at[n * TP + u, c], fs=zc * 2 + cd
        )

    def source(n, u):
        return (z + Z - n - Q * u) % Z

    def za_recv(n, u, cs):
        held = gu.at[2 * source(n, u) + cs, p]
        return remote(held, held, za_s.at[n * TP + u, cs], za_r.at[n * TP + u, cs], fs=other)

    def y_hand(n, u):
        held = gu.at[pl.ds(2 * source(n, u), 2), p]
        return remote(held, held, y_s.at[n * TP + u], y_r.at[n * TP + u], grp=mate)

    def y_recv(n, u):
        held = gu.at[pl.ds(2 * source(n, u), 2), 1 - p]
        return remote(held, held, y_s.at[n * TP + u], y_r.at[n * TP + u], grp=mate)

    own = pltpu.make_async_copy(xr.at[zone, seat, c], gu.at[f, p], loc.at[4])

    def issue(b):
        for n in needs.get(b, ()):
            for side in (0, 1):
                xw_recv(n, side).wait_recv()
            second_leg_recv(n).wait_recv()
        for n, u in turns[b]:
            if n == 0 and u == 0:
                za(0, 0, 1 - c).start()
                own.start()
            else:
                za(n, u, 0).start()
                za(n, u, 1).start()

    def accept(b):
        for n, u in turns[b]:
            if n == 0 and u == 0:
                own.wait()
                za_recv(0, 0, 1 - c).wait_recv()
            else:
                za_recv(n, u, 0).wait_recv()
                za_recv(n, u, 1).wait_recv()
            y_hand(n, u).start()

    def onward(i, fo, side):
        held = tok.at[fo, pl.ds(side * half, half), cols(xside[1 - side])]
        return remote(held, held, xo_s.at[side, i], xo_r.at[side, i], tp=xside[side])

    def onward_recv(i, fo, side):
        held = tok.at[fo, pl.ds(side * half, half), cols(opposite)]
        return remote(held, held, xo_s.at[side, i], xo_r.at[side, i], tp=xside[side])

    def cross(i, fo):
        return remote(tok.at[fo], tok.at[fo], cc_s.at[i], cc_r.at[i], fs=other)

    def cross_w(i, fo):
        return remote(wall.at[fo], wall.at[fo], cw_s.at[i], cw_r.at[i], fs=other)

    def cross_recv(i, fo):
        return remote(tok.at[fo + 1 - 2 * c], tok.at[fo + 1 - 2 * c], cc_s.at[i], cc_r.at[i], fs=other)

    def cross_w_recv(i, fo):
        return remote(wall.at[fo + 1 - 2 * c], wall.at[fo + 1 - 2 * c], cw_s.at[i], cw_r.at[i], fs=other)

    def pass_on(i):
        fo = origin(i)
        for side in (0, 1):
            across_recv(i, fo, side).wait_recv()
            onward(i, fo, side).start()

    def finish(i):
        fo = origin(i)
        for side in (0, 1):
            onward_recv(i, fo, side).wait_recv()
        cross(i, fo).start()
        cross_w(i, fo).start()

    yd = remote(ds.at[p], ds.at[p], yd_s, yd_r, grp=mate)
    ring_step(1)
    for n in order[:2]:
        first_leg(n).wait_recv()
        second_leg(n).start()
    local[0].wait()
    issue(0)
    ring_step(2)
    for n in order[2:]:
        first_leg(n).wait_recv()
        second_leg(n).start()
    for k in (2, 1, 3):
        xd(k).start()
    issue(1)
    for s in range(3, H + 1):
        ring_step(s)
        issue(s - 1)
        for i in (2 * s - 6, 2 * s - 5):
            pass_on(i)
        if s == 4:
            local[1].wait()
            for k in (2, 1, 3):
                xd_recv(k).wait_recv()
            yd.start()
        if s > 3:
            for i in (2 * s - 8, 2 * s - 7):
                finish(i)
        accept(s - 3)
    pass_on(2 * H - 4)
    pass_on(2 * H - 3)
    finish(2 * H - 6)
    finish(2 * H - 5)
    pass_on(2 * H - 2)
    finish(2 * H - 4)
    finish(2 * H - 3)
    accept(H - 2)
    finish(2 * H - 2)
    accept(H - 1)

    local[2].wait()
    local[3].wait()
    own_fo = f + 1 - 2 * c
    remote(nt, tok.at[own_fo], cc_s.at[Z - 1], cc_r.at[Z - 1], fs=other).wait_recv()
    remote(wt, wall.at[own_fo], cw_s.at[Z - 1], cw_r.at[Z - 1], fs=other).wait_recv()
    own_cross.wait_send()
    own_cross_w.wait_send()

    def drain(i, _):
        fo = origin(i)
        for side in (0, 1):
            across(i, fo, side).wait_send()
            onward(i, fo, side).wait_send()
        cross(i, fo).wait_send()
        cross_w(i, fo).wait_send()
        cross_recv(i, fo).wait_recv()
        cross_w_recv(i, fo).wait_recv()
        return 0

    lax.fori_loop(0, Z - 1, drain, 0)

    def ring_drain(s, _):
        ring(s, f, 0).wait_send()
        ring_w(s, f, 0).wait_send()

        @pl.when(s < H - 1)
        def _():
            ring(s, f, 1).wait_send()
            ring_w(s, f, 1).wait_send()

        return 0

    lax.fori_loop(0, H, ring_drain, 0)
    za(0, 0, 1 - c).wait_send()
    y_hand(0, 0).wait_send()
    y_recv(0, 0).wait_recv()

    def exchange_drain(v, _):
        n, u = v // TP, v % TP
        za(n, u, 0).wait_send()
        za(n, u, 1).wait_send()
        y_hand(n, u).wait_send()
        y_recv(n, u).wait_recv()
        return 0

    lax.fori_loop(1, Z, exchange_drain, 0)
    yd.wait_send()
    remote(ds.at[1 - p], ds.at[1 - p], yd_s, yd_r, grp=mate).wait_recv()
    for n in range(Q):
        first_leg(n).wait_send()
        second_leg(n).wait_send()
        for side in (0, 1):
            xw(n, side).wait_send()
    for k in range(1, TP):
        xd(k).wait_send()


def run_hand_over(FS, TP, tokens, routes, logits, gain, w_gate, w_up, w_down):
    Z = FS // 2
    Q = Z // TP
    _, rows, ff = w_gate.shape
    ff = ff // (2 * Q)
    half = rows // 2
    drows, db = w_down.shape[1] // 2, w_down.shape[2]
    vmem = pl.BlockSpec(memory_space=pltpu.VMEM)
    hbm = pl.BlockSpec(memory_space=pltpu.HBM)
    tile = (16, LANES)
    piece = (half // 2, 4 * ff)
    bf16 = jnp.bfloat16
    return pl.pallas_call(
        functools.partial(hand_over, FS, TP),
        out_shape=(
            jax.ShapeDtypeStruct((FS, 2) + piece, bf16),
            jax.ShapeDtypeStruct((2, drows, TP * db), bf16),
            jax.ShapeDtypeStruct((FS,) + tokens.shape, bf16),
            jax.ShapeDtypeStruct((FS,) + tile, bf16),
        ),
        in_specs=[hbm] * 7,
        out_specs=(vmem,) * 4,
        scratch_shapes=[
            pltpu.VMEM(tokens.shape, tokens.dtype),
            pltpu.VMEM(routes.shape, routes.dtype),
            pltpu.VMEM(logits.shape, logits.dtype),
            pltpu.VMEM(gain.shape, gain.dtype),
            pltpu.VMEM((TP, half, w_gate.shape[2]), jnp.float32),
            pltpu.VMEM((TP, half, w_gate.shape[2]), jnp.float32),
            pltpu.VMEM((TP, drows, db), jnp.float32),
            pltpu.VMEM((rows, LANES), jnp.float32),
            pltpu.VMEM((TP, Q, 2) + piece, bf16),
            pltpu.VMEM((TP, drows, db), bf16),
            pltpu.VMEM(tokens.shape, bf16),
            pltpu.VMEM(tile, bf16),
            pltpu.VMEM((TP, Q, 2) + piece, bf16),
            pltpu.VMEM((Q, 2) + piece, bf16),
            DMA((7,)), DMA((5,)),
            DMA((2, Q)), DMA((2, Q)), DMA((Q,)), DMA((Q,)), DMA((Q,)), DMA((Q,)),
            DMA((TP - 1,)), DMA((TP - 1,)),
            DMA((2, Z // 2)), DMA((2, Z // 2)), DMA((2, Z // 2)), DMA((2, Z // 2)),
            DMA((2, Z - 1)), DMA((2, Z - 1)), DMA((2, Z - 1)), DMA((2, Z - 1)),
            DMA((Z,)), DMA((Z,)), DMA((Z,)), DMA((Z,)),
            DMA((Z, 2)), DMA((Z, 2)),
            DMA((Z,)), DMA((Z,)), DMA, DMA,
        ],
        compiler_params=pltpu.CompilerParams(collective_id=0, has_side_effects=True, vmem_limit_bytes=16 << 20),
        cost_estimate=pl.CostEstimate(flops=10**9, bytes_accessed=30 << 20, transcendentals=0),
        name="hand_over",
    )(*[
        pltpu.with_memory_space_constraint(a, pltpu.HBM)
        for a in (tokens, routes, logits, gain, w_gate, w_up, w_down)
    ])


def unpack(block, gu, ds, wg, wu, gate_out, up_out, down_out, gate_t, up_t, sem, sems):
    down = pltpu.make_async_copy(ds, down_out, sem)
    down.start()
    part, ff = gu.shape[2], gu.shape[3] // 4
    pieces = block // (2 * part)
    blocks = wg.shape[0] // block

    def served(i, n):
        span = pl.ds(pl.multiple_of(i * block, block), block)
        held, out = ((gate_t, gate_out), (up_t, up_out))[n]
        return pltpu.make_async_copy(held.at[:, span], out.at[:, span], sems.at[n, i])

    def step(i, _):
        span = pl.ds(pl.multiple_of(i * block, block), block)
        for v in range(pieces):
            k = i * pieces + v
            piece = gu[k // 2, k % 2].astype(jnp.float32)
            for hh in (0, 1):
                at = pl.ds(pl.multiple_of(k * 2 * part + hh * part, part), part)
                wg[at, :] = piece[:, 2 * hh * ff : (2 * hh + 1) * ff].astype(jnp.bfloat16)
                wu[at, :] = piece[:, (2 * hh + 1) * ff : (2 * hh + 2) * ff].astype(jnp.bfloat16)
        for n, (own, held) in enumerate(((wg, gate_t), (wu, up_t))):
            held[:, span] = own[span, :].astype(jnp.float32).T.astype(jnp.bfloat16)
            served(i, n).start()
        return 0

    lax.fori_loop(0, blocks, step, 0)
    down.wait()

    def drain(i, _):
        served(i, 0).wait()
        served(i, 1).wait()
        return 0

    lax.fori_loop(0, blocks, drain, 0)


def run_unpack(gu, ds):
    ff = gu.shape[3] // 4
    features = gu.shape[0] * gu.shape[1] * gu.shape[2] * 2
    vmem = pl.BlockSpec(memory_space=pltpu.VMEM)
    bf16 = jnp.bfloat16
    return pl.pallas_call(
        functools.partial(unpack, 256),
        out_shape=(
            jax.ShapeDtypeStruct((features, ff), bf16),
            jax.ShapeDtypeStruct((features, ff), bf16),
            jax.ShapeDtypeStruct((ff, features), bf16),
            jax.ShapeDtypeStruct((ff, features), bf16),
            jax.ShapeDtypeStruct(ds.shape, bf16),
        ),
        in_specs=[vmem] * 2,
        out_specs=(vmem,) * 2 + (pl.BlockSpec(memory_space=pltpu.HBM),) * 3,
        scratch_shapes=[
            pltpu.VMEM((ff, features), bf16), pltpu.VMEM((ff, features), bf16), DMA, DMA((2, features // 256)),
        ],
        compiler_params=pltpu.CompilerParams(vmem_limit_bytes=8 << 20),
        cost_estimate=pl.CostEstimate(flops=10**9, bytes_accessed=16 << 20, transcendentals=0),
        name="unpack",
    )(gu, ds)


def combine(FS, TP, L, wg, wu, tok, wall, wd, out, wdt, hs, part, prec, zs, zr, outt, turned, xd_s, xd_r, xo_s, xo_r, cc_s, cc_r, z_s, z_r, fin_s, fin_r):
    Z = FS // 2
    H = Z // 2
    x, f = lax.axis_index("tp"), lax.axis_index("fs")
    z, c = f // 2, f % 2
    other = f + 1 - 2 * c
    ff, block = hs.shape[2], hs.shape[3]
    half = ff // 2
    keep = part.shape[1] // 2
    xside = ((x + 1) % TP, (x + TP - 1) % TP)
    zside = (((z + 1) % Z) * 2 + c, ((z + Z - 1) % Z) * 2 + c)

    barrier = pltpu.get_barrier_semaphore()
    for k in xside:
        pl.semaphore_signal(barrier, inc=1, device_id={"tp": k}, device_id_type=MESH)
    for k in zside + (other,):
        pl.semaphore_signal(barrier, inc=1, device_id={"fs": k}, device_id_type=MESH)

    def away(i):
        return H - (i + 1) // 2

    def chip(i):
        return jnp.where(i % 2 == 0, (z + away(i)) % Z, (z + Z - away(i)) % Z)

    count, features = tok.shape[1], tok.shape[2]

    def make(i):
        rows = jnp.concatenate([tok[pl.ds(2 * chip(i + v), 2)].reshape(block, features) for v in (0, 1)], axis=0)
        gate = jnp.dot(rows, wg[...], preferred_element_type=jnp.float32)
        up = jnp.dot(rows, wu[...], preferred_element_type=jnp.float32)
        hidden = (jax.nn.silu(gate) * up).T
        for v in (0, 1):
            scale = [wall[2 * chip(i + v) + n, 0:1, :count] for n in (0, 1)]
            scale = jnp.concatenate(scale, axis=1).astype(jnp.float32)
            hs[i + v, x] = (hidden[:, v * block : (v + 1) * block] * scale).astype(jnp.bfloat16)

    def direct(i, side):
        return remote(hs.at[i, x], hs.at[i, x], xd_s.at[side, i], xd_r.at[side, i], tp=xside[side])

    def direct_recv(i, side):
        held = hs.at[i, xside[1 - side]]
        return remote(held, held, xd_s.at[side, i], xd_r.at[side, i], tp=xside[side])

    def onward(i, side):
        held = hs.at[i, xside[1 - side], pl.ds(side * half, half)]
        return remote(held, held, xo_s.at[side, i], xo_r.at[side, i], tp=xside[side])

    def onward_recv(i, side):
        held = hs.at[i, (x + 2) % TP, pl.ds(side * half, half)]
        return remote(held, held, xo_s.at[side, i], xo_r.at[side, i], tp=xside[side])

    def cross(j):
        return remote(part.at[j, pl.ds((1 - c) * keep, keep)], prec.at[j], cc_s.at[j], cc_r.at[j], fs=other)

    def walk(m, side):
        k = away(m) - 1
        return remote(zs.at[m], zr.at[side, k], z_s.at[m], z_r.at[side, k], fs=zside[side])

    def arrival(side, k):
        return remote(zs.at[0], zr.at[side, k], z_s.at[0], z_r.at[side, k], fs=zside[side])

    AHEAD = 2

    def begin(k, _):
        make(2 * k)

        @pl.when(k == 0)
        def _():
            pl.semaphore_wait(barrier, 5)

        @pl.when(2 * k < AHEAD)
        def _():
            for v in (0, 1):
                for side in (0, 1):
                    direct(2 * k + v, side).start()

        return 0

    lax.fori_loop(0, AHEAD // 2 + 1, begin, 0)
    for e in range(TP):
        wdt[:, e * ff : (e + 1) * ff] = wd[e].T.astype(jnp.bfloat16)

    def step(i, _):
        @pl.when(i + AHEAD < Z)
        def _():
            for side in (0, 1):
                direct(i + AHEAD, side).start()

        @pl.when(i < Z)
        def _():
            for side in (0, 1):
                direct_recv(i, side).wait_recv()
                onward(i, side).start()

        @pl.when((i % 2 == 0) & (i + AHEAD + 2 < Z))
        def _():
            make(i + AHEAD + 2)

        @pl.when((i >= L) & (i < Z + L))
        def _():
            j = i - L
            for side in (0, 1):
                onward_recv(j, side).wait_recv()
            rhs = hs[j].reshape(TP * ff, block)
            part[j] = jnp.dot(wdt[...], rhs, preferred_element_type=jnp.float32)
            cross(j).start()

        @pl.when(i > L)
        def _():
            m = i - L - 1
            k = away(m)
            cross(m).wait_recv()
            total = part[m, pl.ds(c * keep, keep)] + prec[m]

            @pl.when(m == 0)
            def _():
                zs[m] = total.astype(jnp.bfloat16)

            @pl.when(m == 1)
            def _():
                zs[m] = total.astype(jnp.bfloat16)

            for side in (0, 1):
                @pl.when((m >= 2) & (m < Z - 1) & (m % 2 == side))
                def _():
                    arrival(side, k).wait_recv()
                    zs[m] = (total + zr[side, k].astype(jnp.float32)).astype(jnp.bfloat16)

                @pl.when((m < Z - 1) & (m % 2 == side))
                def _():
                    walk(m, side).start()

            @pl.when(m == Z - 1)
            def _():
                arrival(0, 0).wait_recv()
                arrival(1, 0).wait_recv()
                both = zr[0, 0].astype(jnp.float32) + zr[1, 0].astype(jnp.float32)
                outt[pl.ds(c * keep, keep)] = (total + both).astype(jnp.bfloat16)

        return 0

    lax.fori_loop(0, Z + L + 1, step, 0)
    last = remote(outt.at[pl.ds(c * keep, keep)], outt.at[pl.ds(c * keep, keep)], fin_s, fin_r, fs=other)
    last.start()

    def drain(i, _):
        for side in (0, 1):
            direct(i, side).wait_send()
            onward(i, side).wait_send()
        cross(i).wait_send()

        @pl.when(i < Z - 1)
        def _():
            arrival_of = remote(zs.at[i], zr.at[0, 0], z_s.at[i], z_r.at[0, 0], fs=other)
            arrival_of.wait_send()

        return 0

    lax.fori_loop(0, Z, drain, 0)
    last.wait()
    turned[...] = outt[...].astype(jnp.float32).T
    rows = block // 2
    out[...] = turned[pl.ds(c * rows, rows)].astype(jnp.bfloat16)


def run_combine(FS, TP, wg, wu, tok, wall, wd):
    Z = FS // 2
    ff = wg.shape[1]
    block = 2 * tok.shape[1]
    feats = wd.shape[2]
    vmem = pl.BlockSpec(memory_space=pltpu.VMEM)
    return pl.pallas_call(
        functools.partial(combine, FS, TP, 2),
        out_shape=jax.ShapeDtypeStruct((block // 2, feats), jnp.bfloat16),
        in_specs=[vmem] * 5,
        out_specs=vmem,
        scratch_shapes=[
            pltpu.VMEM((feats, TP * ff), jnp.bfloat16),
            pltpu.VMEM((Z, TP, ff, block), jnp.bfloat16),
            pltpu.VMEM((Z, feats, block), jnp.float32),
            pltpu.VMEM((Z, feats // 2, block), jnp.float32),
            pltpu.VMEM((Z - 1, feats // 2, block), jnp.bfloat16),
            pltpu.VMEM((2, Z // 2, feats // 2, block), jnp.bfloat16),
            pltpu.VMEM((feats, block), jnp.bfloat16),
            pltpu.VMEM((block, feats), jnp.float32),
            DMA((2, Z)), DMA((2, Z)), DMA((2, Z)), DMA((2, Z)),
            DMA((Z,)), DMA((Z,)), DMA((Z - 1,)), DMA((2, Z // 2)), DMA, DMA,
        ],
        compiler_params=pltpu.CompilerParams(collective_id=1, has_side_effects=True, vmem_limit_bytes=20 << 20),
        cost_estimate=pl.CostEstimate(flops=10**9, bytes_accessed=30 << 20, transcendentals=0),
        name="combine",
    )(wg, wu, tok, wall, wd)


def body(FS, TP, tokens, routes, route_logits, gain, w_gate, w_up, w_down):
    gu, ds, tok, wall = run_hand_over(
        FS, TP, tokens, routes.T, route_logits.T, gain[None], w_gate, w_up, w_down
    )
    wg, wu, gate_t, up_t, down = run_unpack(gu, ds)
    mixed = run_combine(FS, TP, wg, wu, tok, wall, w_down)
    return (gate_t.T[None], up_t.T[None], down.reshape(1, 2 * ds.shape[1], -1), mixed)


def solution(mesh):
    return jax.shard_map(
        functools.partial(body, mesh.shape["fs"], mesh.shape["tp"]),
        mesh=mesh,
        in_specs=(
            P(("grp", "fs"), None),
            P(("grp", "fs"), None),
            P(("grp", "fs"), None),
            P("fs"),
            P(None, "fs", "tp"),
            P(None, "fs", "tp"),
            P(None, "fs", "tp"),
        ),
        out_specs=(
            P(("grp", "tp"), None, "fs"),
            P(("grp", "tp"), None, "fs"),
            P(("grp", "tp"), "fs", None),
            P(("grp", "fs"), "tp"),
        ),
        check_vma=False,
    )
```

```python
import functools

import jax
import jax.numpy as jnp
from jax import lax
from jax.experimental import pallas as pl
from jax.experimental.pallas import tpu as pltpu
from jax.sharding import PartitionSpec as P

MESH = pl.DeviceIdType.MESH
DMA = pltpu.SemaphoreType.DMA
LANES = 128


def remote(src, dst, send, recv, **where):
    return pltpu.make_async_remote_copy(
        src_ref=src, dst_ref=dst, send_sem=send, recv_sem=recv, device_id=where, device_id_type=MESH
    )


def hand_over(
    FS, TP, x_hbm, routes_hbm, logits_hbm, gain_hbm, w_gate, w_up, w_down, gu, ds, tok, wall,
    x_in, routes, logits, gain, raw_gate, raw_up, raw_down, scale, wp, dn, nt, wt, xr, stage,
    in_s, loc, xw_s, xw_r, st_s, st_r, sf_s, sf_r, xd_s, xd_r, rs, rr, ws, wr, xt_s, xt_r, xo_s, xo_r,
    cc_s, cc_r, cw_s, cw_r, za_s, za_r, y_s, y_r, yd_s, yd_r,
):
    Z = FS // 2
    H = Z // 2
    Q = Z // TP
    assert TP == 4 and Q == 4 and Q * TP == Z
    x, f, g = lax.axis_index("tp"), lax.axis_index("fs"), lax.axis_index("grp")
    z, c = f // 2, f % 2
    zone, seat = z // Q, z % Q
    order = (0, 2, 1, 3)
    p = g % 2
    mate = g + 1 - 2 * p
    fb = nt.shape[1] // TP
    half = nt.shape[0] // 2
    db = dn.shape[2]
    rows = raw_gate.shape[1]
    drows = raw_down.shape[1]
    other = f + 1 - 2 * c
    xside = ((x + 1) % TP, (x + TP - 1) % TP)
    zside = (((z + 1) % Z) * 2 + c, ((z + Z - 1) % Z) * 2 + c)
    opposite = (x + 2) % TP

    fetch = (
        pltpu.make_async_copy(x_hbm, x_in, in_s.at[3]),
        pltpu.make_async_copy(routes_hbm, routes, in_s.at[4]),
        pltpu.make_async_copy(logits_hbm, logits, in_s.at[5]),
        pltpu.make_async_copy(gain_hbm, gain, in_s.at[6]),
        pltpu.make_async_copy(w_gate.at[:, pl.ds(p * rows, rows)], raw_gate, in_s.at[0]),
        pltpu.make_async_copy(w_up.at[:, pl.ds(p * rows, rows)], raw_up, in_s.at[1]),
        pltpu.make_async_copy(w_down.at[:, pl.ds(p * drows, drows)], raw_down, in_s.at[2]),
    )
    for copy in fetch:
        copy.start()

    barrier = pltpu.get_barrier_semaphore()

    def greet(r, _):
        pl.semaphore_signal(barrier, inc=1, device_id={"fs": (f + r) % FS}, device_id_type=MESH)
        return 0

    lax.fori_loop(1, FS, greet, 0)
    for k in range(1, TP):
        pl.semaphore_signal(barrier, inc=1, device_id={"tp": (x + k) % TP}, device_id_type=MESH)
    pl.semaphore_signal(barrier, inc=1, device_id={"grp": mate}, device_id_type=MESH)

    for copy in fetch[:4]:
        copy.wait()
    values = x_in[...].astype(jnp.float32)
    mean_square = jnp.mean(values * values, axis=-1, keepdims=True)
    nt[...] = (values * lax.rsqrt(mean_square + 1e-06)).astype(jnp.bfloat16)
    count = routes.shape[1]
    first = jax.nn.sigmoid(logits[0:1] - logits[1:2])
    second = jax.nn.sigmoid(logits[1:2] - logits[0:1])
    weight = first * (routes[0:1] == x).astype(jnp.float32) + second * (routes[1:2] == x).astype(jnp.float32)
    wt[...] = jnp.zeros_like(wt)
    wt[:, :count] = jnp.broadcast_to(weight, (wt.shape[0], count)).astype(jnp.bfloat16)
    scale[...] = jnp.broadcast_to(gain[...], (LANES, gain.shape[1])).T
    factor = scale[pl.ds(p * rows, rows), :][:, :1]
    ff = wp.shape[4] // 4
    part = rows // 2
    fetch[4].wait()
    fetch[5].wait()

    def pack(e):
        gate = raw_gate[e] * factor
        up = raw_up[e] * factor
        for j in range(2 * Q):
            span = slice(j * ff, (j + 1) * ff)
            quarters = [gate[:part, span], up[:part, span], gate[part:, span], up[part:, span]]
            wp[e, j // 2, j % 2] = jnp.concatenate(quarters, axis=1).astype(jnp.bfloat16)

    pack(opposite)
    pl.semaphore_wait(barrier, FS - 1 + TP - 1 + 1)

    def cols(i):
        return pl.ds(pl.multiple_of(i * fb, LANES), fb)

    def dcols(i):
        return pl.ds(pl.multiple_of(i * db, LANES), db)

    def ring(i, fo, side):
        return remote(tok.at[fo, :, cols(x)], tok.at[fo, :, cols(x)], rs.at[side, i], rr.at[side, i], fs=zside[side])

    def ring_w(i, fo, side):
        return remote(wall.at[fo], wall.at[fo], ws.at[side, i], wr.at[side, i], fs=zside[side])

    for side in (0, 1):
        remote(nt.at[:, cols(x)], tok.at[f, :, cols(x)], rs.at[side, 0], rr.at[side, 0], fs=zside[side]).start()
        remote(wt, wall.at[f], ws.at[side, 0], wr.at[side, 0], fs=zside[side]).start()

    def spot(n):
        return (seat + n) % Q

    def leg(n):
        return n // 2

    def xw(n, side):
        return remote(wp.at[xside[side], spot(n)], xr.at[x, spot(n)], xw_s.at[side, n], xw_r.at[side, n], tp=xside[side])

    def xw_recv(n, side):
        held = xr.at[xside[1 - side], spot(n)]
        return remote(held, held, xw_s.at[side, n], xw_r.at[side, n], tp=xside[side])

    def first_leg(n):
        return remote(wp.at[opposite, spot(n)], stage.at[n], st_s.at[n], st_r.at[n], tp=xside[leg(n)])

    def second_leg(n):
        return remote(stage.at[n], xr.at[xside[1 - leg(n)], spot(n)], sf_s.at[n], sf_r.at[n], tp=xside[leg(n)])

    def second_leg_recv(n):
        return remote(stage.at[n], xr.at[opposite, spot(n)], sf_s.at[n], sf_r.at[n], tp=xside[leg(n)])

    def xd(k):
        return remote(dn.at[(x + k) % TP], ds.at[p, :, dcols(x)], xd_s.at[k - 1], xd_r.at[k - 1], tp=(x + k) % TP)

    def xd_recv(k):
        held = ds.at[p, :, dcols((x + TP - k) % TP)]
        return remote(held, held, xd_s.at[k - 1], xd_r.at[k - 1], tp=(x + k) % TP)

    def send_packed(k, _):
        @pl.when(k == 0)
        def _():
            for n in order[:2]:
                first_leg(n).start()

        e = jnp.where(k < 2, jnp.where(k == 0, xside[0], xside[1]), x)
        pack(e)

        @pl.when(k == 0)
        def _():
            for n in order:
                xw(n, 0).start()

        @pl.when(k == 1)
        def _():
            for n in order:
                xw(n, 1).start()
            for n in order[2:]:
                first_leg(n).start()

        return 0

    lax.fori_loop(0, 3, send_packed, 0)
    fetch[6].wait()
    dn[...] = raw_down[...].astype(jnp.bfloat16)
    own_cross = remote(nt, tok.at[f], cc_s.at[Z - 1], cc_r.at[Z - 1], fs=other)
    own_cross.start()
    own_cross_w = remote(wt, wall.at[f], cw_s.at[Z - 1], cw_r.at[Z - 1], fs=other)
    own_cross_w.start()
    local = [
        pltpu.make_async_copy(wp.at[x], xr.at[x], loc.at[0]),
        pltpu.make_async_copy(dn.at[x], ds.at[p, :, dcols(x)], loc.at[1]),
        pltpu.make_async_copy(nt, tok.at[f], loc.at[2]),
        pltpu.make_async_copy(wt, wall.at[f], loc.at[3]),
    ]
    for copy in local:
        copy.start()

    def across(i, fo, side):
        return remote(
            tok.at[fo, :, cols(x)], tok.at[fo, :, cols(x)], xt_s.at[side, i], xt_r.at[side, i], tp=xside[side]
        )

    def across_recv(i, fo, side):
        held = tok.at[fo, :, cols(xside[1 - side])]
        return remote(held, held, xt_s.at[side, i], xt_r.at[side, i], tp=xside[side])

    def from_left(s):
        return ((z + Z - s) % Z) * 2 + c

    def from_right(s):
        return ((z + s) % Z) * 2 + c

    def origin(i):
        s = i // 2 + 1
        return jnp.where(i % 2 == 0, from_left(s), from_right(s))

    def ring_step(s):
        for side in (0, 1):
            if s < H or side == 0:
                fo = from_left(s) if side == 0 else from_right(s)
                ring(s - 1, fo, side).wait_recv()
                ring_w(s - 1, fo, side).wait_recv()
                if s < H - side:
                    ring(s, fo, side).start()
                    ring_w(s, fo, side).start()
                for way in (0, 1):
                    across(2 * s - 2 + side, fo, way).start()

    turns = (
        ((0, 1), (0, 3)), ((0, 2), (0, 0)), ((2, 1), (2, 2)), ((2, 0), (2, 3)),
        ((3, 1), (1, 2)), ((1, 1), (3, 2)), ((3, 0), (1, 3)), ((1, 0), (3, 3)),
    )
    needs = {0: (0,), 2: (2,), 4: (1, 3)}

    def za(n, u, cd):
        zc = (z + n + Q * u) % Z
        return remote(
            xr.at[zc // Q, spot(n), cd], gu.at[f, p], za_s.at[n * TP + u, cd], za_r.at[n * TP + u, c], fs=zc * 2 + cd
        )

    def source(n, u):
        return (z + Z - n - Q * u) % Z

    def za_recv(n, u, cs):
        held = gu.at[2 * source(n, u) + cs, p]
        return remote(held, held, za_s.at[n * TP + u, cs], za_r.at[n * TP + u, cs], fs=other)

    def y_hand(n, u):
        held = gu.at[pl.ds(2 * source(n, u), 2), p]
        return remote(held, held, y_s.at[n * TP + u], y_r.at[n * TP + u], grp=mate)

    def y_recv(n, u):
        held = gu.at[pl.ds(2 * source(n, u), 2), 1 - p]
        return remote(held, held, y_s.at[n * TP + u], y_r.at[n * TP + u], grp=mate)

    own = pltpu.make_async_copy(xr.at[zone, seat, c], gu.at[f, p], loc.at[4])

    def issue(b):
        for n in needs.get(b, ()):
            for side in (0, 1):
                xw_recv(n, side).wait_recv()
            second_leg_recv(n).wait_recv()
        for n, u in turns[b]:
            if n == 0 and u == 0:
                za(0, 0, 1 - c).start()
                own.start()
            else:
                za(n, u, 0).start()
                za(n, u, 1).start()

    def accept(b):
        for n, u in turns[b]:
            if n == 0 and u == 0:
                own.wait()
                za_recv(0, 0, 1 - c).wait_recv()
            else:
                za_recv(n, u, 0).wait_recv()
                za_recv(n, u, 1).wait_recv()
            y_hand(n, u).start()

    def onward(i, fo, side):
        held = tok.at[fo, pl.ds(side * half, half), cols(xside[1 - side])]
        return remote(held, held, xo_s.at[side, i], xo_r.at[side, i], tp=xside[side])

    def onward_recv(i, fo, side):
        held = tok.at[fo, pl.ds(side * half, half), cols(opposite)]
        return remote(held, held, xo_s.at[side, i], xo_r.at[side, i], tp=xside[side])

    def cross(i, fo):
        return remote(tok.at[fo], tok.at[fo], cc_s.at[i], cc_r.at[i], fs=other)

    def cross_w(i, fo):
        return remote(wall.at[fo], wall.at[fo], cw_s.at[i], cw_r.at[i], fs=other)

    def cross_recv(i, fo):
        return remote(tok.at[fo + 1 - 2 * c], tok.at[fo + 1 - 2 * c], cc_s.at[i], cc_r.at[i], fs=other)

    def cross_w_recv(i, fo):
        return remote(wall.at[fo + 1 - 2 * c], wall.at[fo + 1 - 2 * c], cw_s.at[i], cw_r.at[i], fs=other)

    def pass_on(i):
        fo = origin(i)
        for side in (0, 1):
            across_recv(i, fo, side).wait_recv()
            onward(i, fo, side).start()

    def finish(i):
        fo = origin(i)
        for side in (0, 1):
            onward_recv(i, fo, side).wait_recv()
        cross(i, fo).start()
        cross_w(i, fo).start()

    yd = remote(ds.at[p], ds.at[p], yd_s, yd_r, grp=mate)
    ring_step(1)
    for n in order:
        first_leg(n).wait_recv()
        second_leg(n).start()
    for k in (2, 1, 3):
        xd(k).start()
    ring_step(2)
    local[0].wait()
    issue(0)
    issue(1)
    for s in range(3, H + 1):
        ring_step(s)
        issue(s - 1)
        for i in (2 * s - 6, 2 * s - 5):
            pass_on(i)
        if s == 4:
            local[1].wait()
            for k in (2, 1, 3):
                xd_recv(k).wait_recv()
            yd.start()
        if s > 3:
            for i in (2 * s - 8, 2 * s - 7):
                finish(i)
        accept(s - 3)
    pass_on(2 * H - 4)
    pass_on(2 * H - 3)
    finish(2 * H - 6)
    finish(2 * H - 5)
    pass_on(2 * H - 2)
    finish(2 * H - 4)
    finish(2 * H - 3)
    accept(H - 2)
    finish(2 * H - 2)
    accept(H - 1)

    local[2].wait()
    local[3].wait()
    own_fo = f + 1 - 2 * c
    remote(nt, tok.at[own_fo], cc_s.at[Z - 1], cc_r.at[Z - 1], fs=other).wait_recv()
    remote(wt, wall.at[own_fo], cw_s.at[Z - 1], cw_r.at[Z - 1], fs=other).wait_recv()
    own_cross.wait_send()
    own_cross_w.wait_send()

    def drain(i, _):
        fo = origin(i)
        for side in (0, 1):
            across(i, fo, side).wait_send()
            onward(i, fo, side).wait_send()
        cross(i, fo).wait_send()
        cross_w(i, fo).wait_send()
        cross_recv(i, fo).wait_recv()
        cross_w_recv(i, fo).wait_recv()
        return 0

    lax.fori_loop(0, Z - 1, drain, 0)

    def ring_drain(s, _):
        ring(s, f, 0).wait_send()
        ring_w(s, f, 0).wait_send()

        @pl.when(s < H - 1)
        def _():
            ring(s, f, 1).wait_send()
            ring_w(s, f, 1).wait_send()

        return 0

    lax.fori_loop(0, H, ring_drain, 0)
    za(0, 0, 1 - c).wait_send()
    y_hand(0, 0).wait_send()
    y_recv(0, 0).wait_recv()

    def exchange_drain(v, _):
        n, u = v // TP, v % TP
        za(n, u, 0).wait_send()
        za(n, u, 1).wait_send()
        y_hand(n, u).wait_send()
        y_recv(n, u).wait_recv()
        return 0

    lax.fori_loop(1, Z, exchange_drain, 0)
    yd.wait_send()
    remote(ds.at[1 - p], ds.at[1 - p], yd_s, yd_r, grp=mate).wait_recv()
    for n in range(Q):
        first_leg(n).wait_send()
        second_leg(n).wait_send()
        for side in (0, 1):
            xw(n, side).wait_send()
    for k in range(1, TP):
        xd(k).wait_send()


def run_hand_over(FS, TP, tokens, routes, logits, gain, w_gate, w_up, w_down):
    Z = FS // 2
    Q = Z // TP
    _, rows, ff = w_gate.shape
    ff = ff // (2 * Q)
    half = rows // 2
    drows, db = w_down.shape[1] // 2, w_down.shape[2]
    vmem = pl.BlockSpec(memory_space=pltpu.VMEM)
    hbm = pl.BlockSpec(memory_space=pltpu.HBM)
    tile = (16, LANES)
    piece = (half // 2, 4 * ff)
    bf16 = jnp.bfloat16
    return pl.pallas_call(
        functools.partial(hand_over, FS, TP),
        out_shape=(
            jax.ShapeDtypeStruct((FS, 2) + piece, bf16),
            jax.ShapeDtypeStruct((2, drows, TP * db), bf16),
            jax.ShapeDtypeStruct((FS,) + tokens.shape, bf16),
            jax.ShapeDtypeStruct((FS,) + tile, bf16),
        ),
        in_specs=[hbm] * 7,
        out_specs=(vmem,) * 4,
        scratch_shapes=[
            pltpu.VMEM(tokens.shape, tokens.dtype),
            pltpu.VMEM(routes.shape, routes.dtype),
            pltpu.VMEM(logits.shape, logits.dtype),
            pltpu.VMEM(gain.shape, gain.dtype),
            pltpu.VMEM((TP, half, w_gate.shape[2]), jnp.float32),
            pltpu.VMEM((TP, half, w_gate.shape[2]), jnp.float32),
            pltpu.VMEM((TP, drows, db), jnp.float32),
            pltpu.VMEM((rows, LANES), jnp.float32),
            pltpu.VMEM((TP, Q, 2) + piece, bf16),
            pltpu.VMEM((TP, drows, db), bf16),
            pltpu.VMEM(tokens.shape, bf16),
            pltpu.VMEM(tile, bf16),
            pltpu.VMEM((TP, Q, 2) + piece, bf16),
            pltpu.VMEM((Q, 2) + piece, bf16),
            DMA((7,)), DMA((5,)),
            DMA((2, Q)), DMA((2, Q)), DMA((Q,)), DMA((Q,)), DMA((Q,)), DMA((Q,)),
            DMA((TP - 1,)), DMA((TP - 1,)),
            DMA((2, Z // 2)), DMA((2, Z // 2)), DMA((2, Z // 2)), DMA((2, Z // 2)),
            DMA((2, Z - 1)), DMA((2, Z - 1)), DMA((2, Z - 1)), DMA((2, Z - 1)),
            DMA((Z,)), DMA((Z,)), DMA((Z,)), DMA((Z,)),
            DMA((Z, 2)), DMA((Z, 2)),
            DMA((Z,)), DMA((Z,)), DMA, DMA,
        ],
        compiler_params=pltpu.CompilerParams(collective_id=0, has_side_effects=True, vmem_limit_bytes=16 << 20),
        cost_estimate=pl.CostEstimate(flops=10**9, bytes_accessed=30 << 20, transcendentals=0),
        name="hand_over",
    )(*[
        pltpu.with_memory_space_constraint(a, pltpu.HBM)
        for a in (tokens, routes, logits, gain, w_gate, w_up, w_down)
    ])


def unpack(block, gu, ds, wg, wu, gate_out, up_out, down_out, gate_t, up_t, sem, sems):
    down = pltpu.make_async_copy(ds, down_out, sem)
    down.start()
    part, ff = gu.shape[2], gu.shape[3] // 4
    pieces = block // (2 * part)
    blocks = wg.shape[0] // block

    def served(i, n):
        span = pl.ds(pl.multiple_of(i * block, block), block)
        held, out = ((gate_t, gate_out), (up_t, up_out))[n]
        return pltpu.make_async_copy(held.at[:, span], out.at[:, span], sems.at[n, i])

    def step(i, _):
        span = pl.ds(pl.multiple_of(i * block, block), block)
        for v in range(pieces):
            k = i * pieces + v
            piece = gu[k // 2, k % 2].astype(jnp.float32)
            for hh in (0, 1):
                at = pl.ds(pl.multiple_of(k * 2 * part + hh * part, part), part)
                wg[at, :] = piece[:, 2 * hh * ff : (2 * hh + 1) * ff].astype(jnp.bfloat16)
                wu[at, :] = piece[:, (2 * hh + 1) * ff : (2 * hh + 2) * ff].astype(jnp.bfloat16)
        for n, (own, held) in enumerate(((wg, gate_t), (wu, up_t))):
            held[:, span] = own[span, :].astype(jnp.float32).T.astype(jnp.bfloat16)
            served(i, n).start()
        return 0

    lax.fori_loop(0, blocks, step, 0)
    down.wait()

    def drain(i, _):
        served(i, 0).wait()
        served(i, 1).wait()
        return 0

    lax.fori_loop(0, blocks, drain, 0)


def run_unpack(gu, ds):
    ff = gu.shape[3] // 4
    features = gu.shape[0] * gu.shape[1] * gu.shape[2] * 2
    vmem = pl.BlockSpec(memory_space=pltpu.VMEM)
    bf16 = jnp.bfloat16
    return pl.pallas_call(
        functools.partial(unpack, 256),
        out_shape=(
            jax.ShapeDtypeStruct((features, ff), bf16),
            jax.ShapeDtypeStruct((features, ff), bf16),
            jax.ShapeDtypeStruct((ff, features), bf16),
            jax.ShapeDtypeStruct((ff, features), bf16),
            jax.ShapeDtypeStruct(ds.shape, bf16),
        ),
        in_specs=[vmem] * 2,
        out_specs=(vmem,) * 2 + (pl.BlockSpec(memory_space=pltpu.HBM),) * 3,
        scratch_shapes=[
            pltpu.VMEM((ff, features), bf16), pltpu.VMEM((ff, features), bf16), DMA, DMA((2, features // 256)),
        ],
        compiler_params=pltpu.CompilerParams(vmem_limit_bytes=8 << 20),
        cost_estimate=pl.CostEstimate(flops=10**9, bytes_accessed=16 << 20, transcendentals=0),
        name="unpack",
    )(gu, ds)


def combine(FS, TP, L, wg, wu, tok, wall, wd, out, wdt, hs, part, prec, zs, zr, outt, turned, xd_s, xd_r, xo_s, xo_r, cc_s, cc_r, z_s, z_r, fin_s, fin_r):
    Z = FS // 2
    H = Z // 2
    x, f = lax.axis_index("tp"), lax.axis_index("fs")
    z, c = f // 2, f % 2
    other = f + 1 - 2 * c
    ff, block = hs.shape[2], hs.shape[3]
    half = ff // 2
    keep = part.shape[1] // 2
    xside = ((x + 1) % TP, (x + TP - 1) % TP)
    zside = (((z + 1) % Z) * 2 + c, ((z + Z - 1) % Z) * 2 + c)

    barrier = pltpu.get_barrier_semaphore()
    for k in xside:
        pl.semaphore_signal(barrier, inc=1, device_id={"tp": k}, device_id_type=MESH)
    for k in zside + (other,):
        pl.semaphore_signal(barrier, inc=1, device_id={"fs": k}, device_id_type=MESH)

    def away(i):
        return H - (i + 1) // 2

    def chip(i):
        return jnp.where(i % 2 == 0, (z + away(i)) % Z, (z + Z - away(i)) % Z)

    count, features = tok.shape[1], tok.shape[2]

    def make(i):
        rows = jnp.concatenate([tok[pl.ds(2 * chip(i + v), 2)].reshape(block, features) for v in (0, 1)], axis=0)
        gate = jnp.dot(rows, wg[...], preferred_element_type=jnp.float32)
        up = jnp.dot(rows, wu[...], preferred_element_type=jnp.float32)
        hidden = (jax.nn.silu(gate) * up).T
        for v in (0, 1):
            scale = [wall[2 * chip(i + v) + n, 0:1, :count] for n in (0, 1)]
            scale = jnp.concatenate(scale, axis=1).astype(jnp.float32)
            hs[i + v, x] = (hidden[:, v * block : (v + 1) * block] * scale).astype(jnp.bfloat16)

    def direct(i, side):
        return remote(hs.at[i, x], hs.at[i, x], xd_s.at[side, i], xd_r.at[side, i], tp=xside[side])

    def direct_recv(i, side):
        held = hs.at[i, xside[1 - side]]
        return remote(held, held, xd_s.at[side, i], xd_r.at[side, i], tp=xside[side])

    def onward(i, side):
        held = hs.at[i, xside[1 - side], pl.ds(side * half, half)]
        return remote(held, held, xo_s.at[side, i], xo_r.at[side, i], tp=xside[side])

    def onward_recv(i, side):
        held = hs.at[i, (x + 2) % TP, pl.ds(side * half, half)]
        return remote(held, held, xo_s.at[side, i], xo_r.at[side, i], tp=xside[side])

    def cross(j):
        return remote(part.at[j, pl.ds((1 - c) * keep, keep)], prec.at[j], cc_s.at[j], cc_r.at[j], fs=other)

    def walk(m, side):
        k = away(m) - 1
        return remote(zs.at[m], zr.at[side, k], z_s.at[m], z_r.at[side, k], fs=zside[side])

    def arrival(side, k):
        return remote(zs.at[0], zr.at[side, k], z_s.at[0], z_r.at[side, k], fs=zside[side])

    AHEAD = 2

    def begin(k, _):
        make(2 * k)

        @pl.when(k == 0)
        def _():
            pl.semaphore_wait(barrier, 5)

        @pl.when(2 * k < AHEAD)
        def _():
            for v in (0, 1):
                for side in (0, 1):
                    direct(2 * k + v, side).start()

        return 0

    lax.fori_loop(0, AHEAD // 2 + 1, begin, 0)
    for e in range(TP):
        wdt[:, e * ff : (e + 1) * ff] = wd[e].T.astype(jnp.bfloat16)

    def step(i, _):
        @pl.when(i + AHEAD < Z)
        def _():
            for side in (0, 1):
                direct(i + AHEAD, side).start()

        @pl.when(i < Z)
        def _():
            for side in (0, 1):
                direct_recv(i, side).wait_recv()
                onward(i, side).start()

        @pl.when((i % 2 == 0) & (i + AHEAD + 2 < Z))
        def _():
            make(i + AHEAD + 2)

        @pl.when((i >= L) & (i < Z + L))
        def _():
            j = i - L
            for side in (0, 1):
                onward_recv(j, side).wait_recv()
            rhs = hs[j].reshape(TP * ff, block)
            part[j] = jnp.dot(wdt[...], rhs, preferred_element_type=jnp.float32)
            cross(j).start()

        @pl.when(i > L)
        def _():
            m = i - L - 1
            k = away(m)
            cross(m).wait_recv()
            total = part[m, pl.ds(c * keep, keep)] + prec[m]

            @pl.when(m == 0)
            def _():
                zs[m] = total.astype(jnp.bfloat16)

            @pl.when(m == 1)
            def _():
                zs[m] = total.astype(jnp.bfloat16)

            for side in (0, 1):
                @pl.when((m >= 2) & (m < Z - 1) & (m % 2 == side))
                def _():
                    arrival(side, k).wait_recv()
                    zs[m] = (total + zr[side, k].astype(jnp.float32)).astype(jnp.bfloat16)

                @pl.when((m < Z - 1) & (m % 2 == side))
                def _():
                    walk(m, side).start()

            @pl.when(m == Z - 1)
            def _():
                arrival(0, 0).wait_recv()
                arrival(1, 0).wait_recv()
                both = zr[0, 0].astype(jnp.float32) + zr[1, 0].astype(jnp.float32)
                outt[pl.ds(c * keep, keep)] = (total + both).astype(jnp.bfloat16)

        return 0

    lax.fori_loop(0, Z + L + 1, step, 0)
    last = remote(outt.at[pl.ds(c * keep, keep)], outt.at[pl.ds(c * keep, keep)], fin_s, fin_r, fs=other)
    last.start()

    def drain(i, _):
        for side in (0, 1):
            direct(i, side).wait_send()
            onward(i, side).wait_send()
        cross(i).wait_send()

        @pl.when(i < Z - 1)
        def _():
            arrival_of = remote(zs.at[i], zr.at[0, 0], z_s.at[i], z_r.at[0, 0], fs=other)
            arrival_of.wait_send()

        return 0

    lax.fori_loop(0, Z, drain, 0)
    last.wait()
    turned[...] = outt[...].astype(jnp.float32).T
    rows = block // 2
    out[...] = turned[pl.ds(c * rows, rows)].astype(jnp.bfloat16)


def run_combine(FS, TP, wg, wu, tok, wall, wd):
    Z = FS // 2
    ff = wg.shape[1]
    block = 2 * tok.shape[1]
    feats = wd.shape[2]
    vmem = pl.BlockSpec(memory_space=pltpu.VMEM)
    return pl.pallas_call(
        functools.partial(combine, FS, TP, 3),
        out_shape=jax.ShapeDtypeStruct((block // 2, feats), jnp.bfloat16),
        in_specs=[vmem] * 5,
        out_specs=vmem,
        scratch_shapes=[
            pltpu.VMEM((feats, TP * ff), jnp.bfloat16),
            pltpu.VMEM((Z, TP, ff, block), jnp.bfloat16),
            pltpu.VMEM((Z, feats, block), jnp.float32),
            pltpu.VMEM((Z, feats // 2, block), jnp.float32),
            pltpu.VMEM((Z - 1, feats // 2, block), jnp.bfloat16),
            pltpu.VMEM((2, Z // 2, feats // 2, block), jnp.bfloat16),
            pltpu.VMEM((feats, block), jnp.bfloat16),
            pltpu.VMEM((block, feats), jnp.float32),
            DMA((2, Z)), DMA((2, Z)), DMA((2, Z)), DMA((2, Z)),
            DMA((Z,)), DMA((Z,)), DMA((Z - 1,)), DMA((2, Z // 2)), DMA, DMA,
        ],
        compiler_params=pltpu.CompilerParams(collective_id=1, has_side_effects=True, vmem_limit_bytes=20 << 20),
        cost_estimate=pl.CostEstimate(flops=10**9, bytes_accessed=30 << 20, transcendentals=0),
        name="combine",
    )(wg, wu, tok, wall, wd)


def body(FS, TP, tokens, routes, route_logits, gain, w_gate, w_up, w_down):
    gu, ds, tok, wall = run_hand_over(
        FS, TP, tokens, routes.T, route_logits.T, gain[None], w_gate, w_up, w_down
    )
    wg, wu, gate_t, up_t, down = run_unpack(gu, ds)
    mixed = run_combine(FS, TP, wg, wu, tok, wall, w_down)
    return (gate_t.T[None], up_t.T[None], down.reshape(1, 2 * ds.shape[1], -1), mixed)


def solution(mesh):
    return jax.shard_map(
        functools.partial(body, mesh.shape["fs"], mesh.shape["tp"]),
        mesh=mesh,
        in_specs=(
            P(("grp", "fs"), None),
            P(("grp", "fs"), None),
            P(("grp", "fs"), None),
            P("fs"),
            P(None, "fs", "tp"),
            P(None, "fs", "tp"),
            P(None, "fs", "tp"),
        ),
        out_specs=(
            P(("grp", "tp"), None, "fs"),
            P(("grp", "tp"), None, "fs"),
            P(("grp", "tp"), "fs", None),
            P(("grp", "fs"), "tp"),
        ),
        check_vma=False,
    )
```
